256 devices in a mesh: sp: 64 (over z, y, core), tp: 4 (over x).
Axes of the slice: x: 4, y: 4, z: 8, core: 2. Of those that a mesh axis runs over, the one named last changes fastest.
Arguments:
- out_cotangent: bfloat16 [8192, 2048], P('sp'), may hold values from -16 to 16
- routes: int32 [8192, 2], P('sp'), may hold values from 0 to 63, all different within a row; in each aligned block of 128 rows (0 to 127, 128 to 255, ...) at most 6 rows name the same one
- route_weights: float32 [8192, 2], P('sp'), may hold values from 0.3 to 1.5
- expert_rows: bfloat16 [64, 384, 2048], P('sp', None, 'tp'), may hold values from -6 to 6
- w_gate: bfloat16 [64, 2048, 1024], P('sp', None, 'tp'), may hold values from -0.125 to 0.125
- w_up: bfloat16 [64, 2048, 1024], P('sp', None, 'tp'), may hold values from -0.125 to 0.125
- w_down: bfloat16 [64, 1024, 2048], P('sp', 'tp'), may hold values from -0.1875 to 0.1875
- out_weight: bfloat16 [2048, 4096], P('sp', 'tp'), may hold values from -0.09375 to 0.09375
- values: bfloat16 [8192, 4096], P('sp', 'tp'), may hold values from -0.25 to 0.25
- keys: bfloat16 [8192, 1024], P('sp', 'tp'), may hold values from -0.5 to 0.5
- queries: bfloat16 [8192, 1024], P('sp', 'tp'), may hold values from -6 to 6
- log_decay: float32 [8192, 64], P('sp', 'tp'), may hold values from -1 to 0
- gate_input: bfloat16 [8192, 4096], P('sp', 'tp'), may hold values from -6 to 6
Outputs:
- grad_w_gate: bfloat16 [64, 2048, 1024], P('sp', None, 'tp')
- grad_w_up: bfloat16 [64, 2048, 1024], P('sp', None, 'tp')
- grad_w_down: bfloat16 [64, 1024, 2048], P('sp', 'tp')
- grad_out_weight: float32 [2048, 4096], P('sp', 'tp')
- grad_residual: float32 [8192, 2048], P('sp', 'tp')
- grad_values: float32 [8192, 4096], P('sp', 'tp')
- grad_keys: float32 [8192, 1024], P('sp', 'tp')
- grad_queries: float32 [8192, 1024], P('sp', 'tp')
- grad_decay: float32 [8192, 64], P('sp', 'tp')
- grad_gate: float32 [8192, 4096], P('sp', 'tp')
The draws below stay inside these ranges and needn't reach their ends.
Inputs may be any that keep to these rules, and one draw needn't show every extreme that they name: `routes`: in each aligned block of 128 tokens no expert is named by more than 6 pairs, a bound that some block reaches.
All inputs are finite; a program needn't handle non-finite values.
Results may differ from the reference program's by a relative error of at most 0.0062.
Values may be sent and summed in bfloat16 or wider, within the bound.
A program may use at most 128 MiB of HBM per device.

```python
import math
import jax
import jax.numpy as jnp
import numpy as np
from jax import lax

D = 2048
MIXER_HEADS = 64
HEAD_DIM = 64
GROUPS = 8
STATE = 128
INNER = 4096
EXPERT_FF = 1024
EXPERTS = 64
TOP = 2
TOK_DEV = 128
SPAN = 128
SEQUENCE_TOKENS = 8192
CAP = 6
SLOTS = 384
N_SP = 64


def draw_log_decay(key, part):
    parallel_flows = jax.random.split(jax.random.fold_in(key, 11), 6)
    quick_decay_heads = (jax.random.randint(parallel_flows[0], (MIXER_HEADS,), 0, 2) == 1).astype(jnp.float32)
    fast_rate = jax.random.uniform(parallel_flows[1], (MIXER_HEADS,), jnp.float32, 1.0 / 90.0, 1.0 / 30.0)
    slow_rate = 0.4 / SEQUENCE_TOKENS
    base_rate = quick_decay_heads * fast_rate + (1.0 - quick_decay_heads) * slow_rate
    device_count = SEQUENCE_TOKENS // TOK_DEV
    device_scale = jnp.exp(jax.random.uniform(parallel_flows[2], (device_count,), jnp.float32, -0.7, 0.7))
    position_scale = jnp.repeat(device_scale, TOK_DEV)
    rough = jax.random.uniform(parallel_flows[3], (SEQUENCE_TOKENS, MIXER_HEADS), jnp.float32, 0.4, 1.6)
    decay_rates = base_rate[None, :] * position_scale[:, None] * rough
    spike_position = jax.random.randint(parallel_flows[4], (2,), 0, SEQUENCE_TOKENS)
    spike_length = jnp.log(jax.random.uniform(parallel_flows[5], (2, MIXER_HEADS), jnp.float32, 0.5, 0.8))
    spike_matches = (jnp.arange(SEQUENCE_TOKENS)[:, None] == spike_position[None, :]).astype(jnp.float32)
    spike_groups = jnp.dot(spike_matches, spike_length) * (1.0 - quick_decay_heads)[None, :]
    return (spike_groups - decay_rates).astype(jnp.float32)


def with_spikes(entries, stream_key, source, target, blocks, factor):
    def block_of(axis_at):
        return (jnp.arange(entries.shape[axis_at]) // (entries.shape[axis_at] // blocks)).reshape((-1,) + (1,) * (entries.ndim - 1 - axis_at))

    near = jax.random.permutation(stream_key, blocks)[block_of(target)]
    other_side = (block_of(target) + blocks // 2) % blocks
    return jnp.where((block_of(source) == near) | (block_of(source) == other_side), factor * entries, entries)


def levels(own_key, dims, cuts, low, largest):
    def one(axis_at, parts):
        draws = jax.random.uniform(jax.random.fold_in(jax.random.fold_in(own_key, 6), axis_at), (parts,), jnp.float32, low / len(cuts), largest / len(cuts))
        return jnp.repeat(jnp.exp(draws), dims[axis_at] // parts).reshape((-1,) + (1,) * (len(dims) - axis_at - 1))

    gain = one(*cuts[0])
    for cut in cuts[1:]:
        gain = gain * one(*cut)
    return gain


def routed_block(stream_key, own, number, rows, count, top, bound, skew):
    order = jax.random.permutation(stream_key, count)
    heavy_load, ordinary = shares(count, rows * top, bound, skew, True), shares(count, rows * top, bound, skew, False)
    places = jnp.arange(count)

    def named(tallies, rotation):
        used = int((tallies > 0).sum())
        fixed = max(1, used // 4)
        shifted = fixed + (places - fixed + rotation * (used - fixed)) % max(1, count - fixed)
        return jnp.zeros((count,), jnp.int32).at[order[jnp.where(places < fixed, places, shifted)]].set(jnp.asarray(tallies, jnp.int32))

    tallies = jnp.where(number % 4 == 0, named(heavy_load, number // 4), named(ordinary, number - number // 4 - 1))
    mixed = jax.random.permutation(jax.random.fold_in(own, 3), count)
    giver, taker = mixed[0:count // 2 * 2:2], mixed[1:count // 2 * 2:2]
    margin = jnp.minimum(tallies[giver] - 1, bound - tallies[taker]) // 2
    margin = jnp.where((giver == order[0]) | (taker == order[0]) | (tallies[taker] == 0), 0, jnp.maximum(margin, 0))
    shifted = jax.random.randint(jax.random.fold_in(own, 4), (count // 2,), 0, 1 << 20) % (margin + 1)
    tallies = tallies.at[giver].add(-shifted).at[taker].add(shifted)
    labels = jnp.searchsorted(jnp.cumsum(tallies), jnp.arange(rows * top), side="right").astype(jnp.int32)
    table = labels.reshape(top, rows).T
    table = table[jax.random.permutation(jax.random.fold_in(own, 1), rows)]
    rotation = jax.random.randint(jax.random.fold_in(own, 2), (rows, 1), 0, top)
    return jnp.take_along_axis(table, (jnp.arange(top)[None, :] + rotation) % top, axis=1)


def shares(count, total, reach, skew, full):
    portions = [(1 << 20) // math.isqrt(rank ** skew) + 1 for rank in range(1, count + 1)]
    largest = reach if full else min(reach, max(-(-total // count), total * portions[0] // sum(portions)))
    least = 1 if total - largest >= count - 1 else 0
    given, spare = [largest] + [least] * (count - 1), total - largest - least * (count - 1)
    while spare > 0:
        free = [i for i in range(1, count) if given[i] < largest] or [i for i in range(1, count) if given[i] < reach]
        mass, budget = sum([portions[i] for i in free]), spare
        for i in free:
            addition = min(reach - given[i], max(1, budget * portions[i] // mass), spare)
            given[i] = given[i] + addition
            spare = spare - addition
    return np.array(given)


def bell_draw(own_key, shape, deviation, limit, shards=(), kind=jnp.bfloat16):
    result = jax.random.normal(own_key, shape, jnp.float32) * deviation
    if len(shards) > 0:
        result = levels(own_key, shape, shards, -0.22, 0.18) * result
    return jnp.clip(result, min=-limit, max=limit).astype(kind)


def heavy_noise(key, shape, width, bound, cuts, heavy, kind=jnp.bfloat16):
    array = width * jax.random.normal(key, shape, jnp.float32)
    if cuts:
        array = array * levels(key, shape, cuts, -0.22, 0.18)
    return jnp.clip(with_spikes(array, jax.random.fold_in(key, 3), *heavy), -bound, bound).astype(kind)


def setup_inputs(seed: int = 0) -> dict:
    seeds = jax.random.split(jax.random.key(seed), 14)
    out_cotangent = heavy_noise(seeds[0], (SEQUENCE_TOKENS, D), 1.0, 16.0, ((0, 64),), (0, 1, 64, 4.0))
    routes_keys = jax.random.split(jax.random.fold_in(seeds[1], 1), SEQUENCE_TOKENS // TOK_DEV)
    routes_turns = jax.random.permutation(jax.random.fold_in(seeds[1], 3), SEQUENCE_TOKENS // TOK_DEV)
    routes = jax.vmap(lambda own, number: routed_block(jax.random.fold_in(seeds[1], 2), own, number, TOK_DEV, EXPERTS, TOP, CAP, 2))(routes_keys, routes_turns).reshape((SEQUENCE_TOKENS, TOP))
    route_weights = jnp.clip(0.3 + 1.2 * jax.random.uniform(seeds[2], (SEQUENCE_TOKENS, TOP), jnp.float32) ** levels(seeds[2], (SEQUENCE_TOKENS, TOP), ((0, 64),), -0.2, 0.2), 0.3, 1.5)
    expert_rows = bell_draw(seeds[3], (EXPERTS, SLOTS, D), 1.0, 6.0, ((0, 64), (2, 4)))
    w_gate = bell_draw(seeds[4], (EXPERTS, D, EXPERT_FF), D ** -0.5, 0.125, ((0, 64), (2, 4)))
    w_up = bell_draw(seeds[5], (EXPERTS, D, EXPERT_FF), D ** -0.5, 0.125, ((0, 64), (2, 4)))
    w_down = bell_draw(seeds[6], (EXPERTS, EXPERT_FF, D), EXPERT_FF ** -0.5, 0.1875, ((0, 64), (1, 4)))
    out_weight = bell_draw(seeds[7], (D, INNER), INNER ** -0.5, 0.09375, ((0, 64), (1, 4)))
    values = bell_draw(seeds[8], (SEQUENCE_TOKENS, INNER), (SEQUENCE_TOKENS // 16) ** -0.5, 0.25, ((0, 64), (1, 4)))
    keys = bell_draw(seeds[9], (SEQUENCE_TOKENS, GROUPS * STATE), STATE ** -0.5, 0.5, ((0, 64), (1, 4)))
    queries = bell_draw(seeds[10], (SEQUENCE_TOKENS, GROUPS * STATE), 1.0, 6.0, ((0, 64), (1, 4)))
    log_decay = draw_log_decay(jax.random.fold_in(seeds[13], 71), 0)
    gate_input = bell_draw(seeds[12], (SEQUENCE_TOKENS, INNER), 1.0, 6.0, ((0, 64), (1, 4)))
    return {"out_cotangent": out_cotangent, "routes": routes, "route_weights": route_weights, "expert_rows": expert_rows, "w_gate": w_gate, "w_up": w_up, "w_down": w_down, "out_weight": out_weight, "values": values, "keys": keys, "queries": queries, "log_decay": log_decay, "gate_input": gate_input}


HIGHEST = lax.Precision.HIGHEST

def block_step(state_now, block_input):
    values_blk, keys_blk, queries_blk, decay_blk = block_input
    span_len, head_count, head_dim = values_blk.shape
    groups = keys_blk.shape[1]
    state_dim = keys_blk.shape[2]
    repeat = head_count // groups
    cumulative = jnp.cumsum(decay_blk, axis=0)
    lower_mask = jnp.arange(span_len)[:, None] >= jnp.arange(span_len)[None, :]
    segment = cumulative[:, None, :] - cumulative[None, :, :]
    weights = jnp.exp(jnp.where(lower_mask[:, :, None], segment, -jnp.inf)).reshape(span_len, span_len, groups, repeat)
    inner_prod = jnp.einsum('tgn,sgn->tsg', queries_blk, keys_blk, precision=HIGHEST)
    grouped = values_blk.reshape(span_len, groups, repeat, head_dim)
    combined = inner_prod[:, :, :, None] * weights
    within = jnp.einsum('tsgr,sgrp->tgrp', combined, grouped, precision=HIGHEST)
    carried = jnp.einsum('tgn,grpn->tgrp', queries_blk, state_now.reshape(groups, repeat, head_dim, state_dim), precision=HIGHEST)
    carried = carried * jnp.exp(cumulative).reshape(span_len, groups, repeat)[..., None]
    to_end = jnp.exp(cumulative[-1][None, :] - cumulative).reshape(span_len, groups, repeat)
    added_state = jnp.einsum('sgn,sgrp->grpn', keys_blk, grouped * to_end[..., None], precision=HIGHEST)
    new_state = state_now * jnp.exp(cumulative[-1])[:, None, None] + added_state.reshape(head_count, head_dim, state_dim)
    return (new_state, (within + carried).reshape(span_len, head_count * head_dim))

def mixer_scan(value_f, key_f, query_f, decay_f, start_state):
    row_count = value_f.shape[0]
    head_count = decay_f.shape[1]
    groups = key_f.shape[1] // STATE
    head_dim = value_f.shape[1] // head_count
    span_len = min(SPAN, row_count)
    blocks = row_count // span_len
    value_b = value_f.reshape(blocks, span_len, head_count, head_dim)
    key_b = key_f.reshape(blocks, span_len, groups, STATE)
    query_b = query_f.reshape(blocks, span_len, groups, STATE)
    decay_b = decay_f.reshape(blocks, span_len, head_count)
    end_state, outputs = lax.scan(block_step, start_state, (value_b, key_b, query_b, decay_b))
    return (outputs.reshape(row_count, head_count * head_dim), end_state)

def expert_backward(expert_item):
    saved, grads_in, gate_w, up_w, down_w = expert_item
    gate_pre = jnp.dot(saved, gate_w, preferred_element_type=jnp.float32)
    up_pre = jnp.dot(saved, up_w, preferred_element_type=jnp.float32)
    sigmoid_gate = jax.nn.sigmoid(gate_pre)
    activated = gate_pre * sigmoid_gate
    hidden = (activated * up_pre).astype(jnp.bfloat16)
    hidden_grad = jnp.dot(grads_in, down_w.T, preferred_element_type=jnp.float32)
    slope = sigmoid_gate * (1.0 + gate_pre * (1.0 - sigmoid_gate))
    gate_grad = (hidden_grad * up_pre * slope).astype(jnp.bfloat16)
    up_grad = (hidden_grad * activated).astype(jnp.bfloat16)
    grad_down = jnp.dot(hidden.T, grads_in, preferred_element_type=jnp.float32).astype(jnp.bfloat16)
    grad_gate_w = jnp.dot(saved.T, gate_grad, preferred_element_type=jnp.float32).astype(jnp.bfloat16)
    grad_up_w = jnp.dot(saved.T, up_grad, preferred_element_type=jnp.float32).astype(jnp.bfloat16)
    row_value = jnp.dot(gate_grad, gate_w.T, preferred_element_type=jnp.float32) + jnp.dot(up_grad, up_w.T, preferred_element_type=jnp.float32)
    row_grad = row_value.astype(jnp.bfloat16)
    return (grad_gate_w, grad_up_w, grad_down, row_grad)

def reference(out_cotangent, routes, route_weights, expert_rows, w_gate, w_up, w_down, out_weight, values, keys, queries, log_decay, gate_input):
    model_width = out_cotangent.shape[1]
    pair_count = TOK_DEV * TOP
    flat_routes = routes.reshape(N_SP, pair_count)
    expert_ids = jnp.arange(EXPERTS, dtype=jnp.int32)
    onehot = (flat_routes[:, :, None] == expert_ids[None, None, :]).astype(jnp.int32)
    pair_rank = lax.optimization_barrier(jnp.sum(jnp.cumsum(onehot, axis=1) * onehot, axis=2)) - 1
    pair_slot = (jnp.arange(N_SP, dtype=jnp.int32)[:, None] * CAP + pair_rank).astype(jnp.int32)
    scaled = (route_weights[:, :, None] * out_cotangent[:, None, :].astype(jnp.float32)).astype(jnp.bfloat16)
    scaled = scaled.reshape(N_SP, pair_count, model_width)
    dispatched = jnp.zeros((EXPERTS, SLOTS, model_width), jnp.bfloat16).at[flat_routes, pair_slot].set(scaled)
    grad_w_gate, grad_w_up, grad_w_down, row_grads = lax.map(expert_backward, (expert_rows, dispatched, w_gate, w_up, w_down))
    returned = row_grads[flat_routes, pair_slot].reshape(SEQUENCE_TOKENS, TOP, model_width)
    grad_residual = out_cotangent.astype(jnp.float32) + lax.optimization_barrier(jnp.sum(returned.astype(jnp.float32), axis=1))
    residual_low = grad_residual.astype(jnp.bfloat16)
    zero_state = jnp.zeros((MIXER_HEADS, HEAD_DIM, STATE), jnp.float32)

    def forward(value_f, key_f, query_f, decay_f):
        return mixer_scan(value_f, key_f, query_f, decay_f, zero_state)[0]
    mixer_y, pull_back = jax.vjp(forward, values.astype(jnp.float32), keys.astype(jnp.float32), queries.astype(jnp.float32), log_decay)
    gate_f = gate_input.astype(jnp.float32)
    sigmoid_gate = jax.nn.sigmoid(gate_f)
    activated = gate_f * sigmoid_gate
    slope = sigmoid_gate * (1.0 + gate_f * (1.0 - sigmoid_gate))
    mixed = (mixer_y * activated).astype(jnp.bfloat16)
    mixed_grad = jnp.dot(residual_low, out_weight, preferred_element_type=jnp.float32)
    grad_out_weight = jnp.dot(residual_low.T, mixed, preferred_element_type=jnp.float32)
    grad_gate = mixed_grad * mixer_y * slope
    y_grad = mixed_grad * activated
    grad_values, grad_keys, grad_queries, grad_decay = pull_back(y_grad)
    return (grad_w_gate, grad_w_up, grad_w_down, grad_out_weight, grad_residual, grad_values, grad_keys, grad_queries, grad_decay, grad_gate)
```

```python
import jax
import jax.numpy as jnp
from jax import lax
from jax.experimental import pallas as pl
from jax.experimental.pallas import tpu as pltpu
from jax.sharding import PartitionSpec as P

MESH = pl.DeviceIdType.MESH
F32, BF16 = jnp.float32, jnp.bfloat16
HIGHEST = lax.Precision.HIGHEST

BUFFERS = dict(
    cot=((128, 512), BF16),
    routes=((2, 128), jnp.int32),
    route_weights=((2, 128), F32),
    w_gate=((2048, 256), BF16),
    w_up=((2048, 256), BF16),
    w_down=((256, 2048), BF16),
    out_weight=((32, 1024), BF16),
    v=((128, 1024), BF16),
    k=((128, 256), BF16),
    q=((128, 256), BF16),
    log_decay=((16, 128), F32),
    gate=((128, 1024), BF16),
    pack_out=((64, 8, 384), BF16),
    pack_in=((64, 8, 384), BF16),
    ret_out=((64, 8, 384), BF16),
    ret_in=((64, 8, 384), BF16),
    hit_a=((2, 128, 512), BF16),
    hit_b=((2, 3, 128, 512), BF16),
    sel_a=((384, 512), BF16),
    sel_b=((3, 384, 512), BF16),
    arr=((4, 384, 512), BF16),
    full=((4, 384, 512), BF16),
    gate_pre=((384, 256), F32),
    up_pre=((384, 256), F32),
    hidden_grad=((384, 256), F32),
    hidden=((384, 256), BF16),
    gate_grad=((384, 256), BF16),
    up_grad=((384, 256), BF16),
    rs_opp=((384, 512), BF16),
    rs_right=((384, 512), BF16),
    rs_left=((384, 512), BF16),
    rs_half_l=((192, 512), BF16),
    rs_half_r=((192, 512), BF16),
    rs_in_l=((384, 512), BF16),
    rs_in_r=((384, 512), BF16),
    rs_own=((384, 512), F32),
    rs_own_l=((384, 512), F32),
    resid=((4, 128, 512), BF16),
    res_t=((8, 8, 32, 128), BF16),
    res_in=((8, 8, 32, 128), BF16),
    weight=((8, 8, 32, 1024), BF16),
    mixed=((8, 128, 1024), BF16),
    gow_part=((8, 32, 1024), F32),
    gow_out=((8, 32, 1024), BF16),
    gow_in=((8, 32, 1024), BF16),
    c_exp=((128, 1024), F32),
    to_end=((128, 1024), F32),
    from_start=((128, 1024), F32),
    c_row=((16, 128), F32),
    c_col=((128, 128), F32),
    v_end=((2, 128, 1024), BF16),
    qk=((2, 128, 128), F32),
    decay=((8, 128, 256), F32),
    score=((2, 8, 128, 256), BF16),
    y=((128, 1024), F32),
    carried=((128, 1024), F32),
    dy=((128, 1024), F32),
    dy_start=((2, 128, 1024), BF16),
    dv=((128, 1024), F32),
    dqk=((2, 128, 128), F32),
    row_col=((128, 128), F32),
    dq=((128, 256), F32),
    log_out=((8, 8, 128), F32),
    log_in=((8, 8, 128), F32),
    log_run=((8, 128), F32),
    log_z=((8, 8, 128), F32),
    log_before=((8, 8, 128), F32),
    before=((8, 128, 128), F32),
    f_own=((8, 128, 128), F32),
    f_in=((8, 128, 128), F32),
    f_run=((128, 128), F32),
    f_z=((8, 128, 128), F32),
    f_back=((8, 128, 128), F32),
    state=((8, 128, 128), F32),
    b_own=((8, 128, 128), F32),
    b_in=((8, 128, 128), F32),
    b_run=((128, 128), BF16),
    b_z=((8, 128, 128), BF16),
    b_back=((8, 128, 128), F32),
    dstate=((8, 128, 128), F32),
)
CHANNELS = dict(
    rows=6,
    arrived=6,
    residual=6,
    dispatch=1,
    back=1,
    scatter=6,
    weight_z=1,
    weight_y=6,
    weight_c=1,
    mixed_y=6,
    mixed_c=1,
    gow_j=1,
    gow_z=1,
    f_j=1,
    f_jlog=1,
    f_z=1,
    f_zlog=1,
    f_back=1,
    b_j=1,
    b_z=1,
    b_back=1,
)
INPUTS = dict(
    h_cot=((128, 2048), BF16),
    h_routes=((2, 128), jnp.int32),
    h_route_weights=((2, 128), F32),
    h_rows=((384, 512), BF16),
    h_w_gate=((2048, 256), BF16),
    h_w_up=((2048, 256), BF16),
    h_w_down=((256, 2048), BF16),
    h_out_weight=((32, 1024), BF16),
    h_v=((128, 1024), BF16),
    h_k=((128, 256), BF16),
    h_q=((128, 256), BF16),
    h_log_decay=((16, 128), F32),
    h_gate=((128, 1024), BF16),
)
OUTPUTS = dict(
    g_gate=((2048, 256), BF16),
    g_up=((2048, 256), BF16),
    g_down=((256, 2048), BF16),
    g_out=((32, 1024), F32),
    g_res=((128, 512), F32),
    g_v=((128, 1024), F32),
    g_k=((128, 256), F32),
    g_q=((128, 256), F32),
    g_decay=((16, 128), F32),
    g_gate_in=((128, 1024), F32),
)


class Refs:
    pass


def dot(a, b, ca=1, cb=0, precision=None):
    return lax.dot_general(
        a, b, (((ca,), (cb,)), ((), ())), precision=precision, preferred_element_type=F32
    )


def iota(shape, dim):
    return lax.broadcasted_iota(jnp.int32, shape, dim)


def hot(cond, dtype=BF16):
    return jnp.where(cond, 1.0, 0.0).astype(dtype)


def split(x):
    high = x.astype(BF16)
    return high, (x - high.astype(F32)).astype(BF16)


def fine_dot(a, b, ca=1, cb=0):
    high, low = split(a)
    return dot(high, b, ca, cb) + dot(low, b, ca, cb)


def sigmoid(x):
    return 1.0 / (1.0 + jnp.exp(-x))


def publish(*refs):
    n = len(OUTPUTS)
    sources, targets, held, sems = refs[:n], refs[n : 2 * n], refs[2 * n : 3 * n], refs[3 * n]
    loads = [pltpu.make_async_copy(sources[i], held[i], sems.at[0, i]) for i in range(n)]
    stores = [pltpu.make_async_copy(held[i], targets[i], sems.at[1, i]) for i in range(n)]
    for load in loads:
        load.start()
    for load, store in zip(loads, stores):
        load.wait()
        store.start()
    for store in stores:
        store.wait()


def kernel(*refs):
    r, c, local, result = Refs(), Refs(), Refs(), Refs()
    names = list(INPUTS) + list(OUTPUTS) + list(BUFFERS)
    for name, ref in zip(names, refs):
        setattr(r, name, ref)
    at = len(names)
    for name in OUTPUTS:
        setattr(r, name.replace("g_", "o_", 1), refs[at])
        at += 1
    for name in CHANNELS:
        setattr(c, name, (refs[at], refs[at + 1]))
        at += 2
    in_sems, out_sems = refs[at], refs[at + 1]
    for i, name in enumerate(INPUTS):
        setattr(local, name[2:], in_sems.at[i])
    for i, name in enumerate(OUTPUTS):
        setattr(result, name[2:], out_sems.at[i])

    me, tx = lax.axis_index("sp"), lax.axis_index("tp")
    z, j = me // 8, me % 8
    partner = j + 1 - 2 * (j % 2)
    right, left, opp = (tx + 1) % 4, (tx + 3) % 4, (tx + 2) % 4
    column = pl.multiple_of(tx * 512, 512)

    barrier = pltpu.get_barrier_semaphore()

    @pl.loop(1, 64)
    def _(d):
        peer = (me + d) % 64
        pl.semaphore_signal(barrier, inc=1, device_id=(peer, tx), device_id_type=MESH)

    for side in (right, left):
        pl.semaphore_signal(barrier, inc=1, device_id=(me, side), device_id_type=MESH)

    loads = dict(
        routes=(r.h_routes, r.routes),
        route_weights=(r.h_route_weights, r.route_weights),
        cot=(r.h_cot.at[:, pl.ds(column, 512)], r.cot),
        rows=(r.h_rows, r.full.at[tx]),
        log_decay=(r.h_log_decay, r.log_decay),
        k=(r.h_k, r.k),
        v=(r.h_v, r.v),
        out_weight=(r.h_out_weight, r.out_weight),
        q=(r.h_q, r.q),
        w_gate=(r.h_w_gate, r.w_gate),
        w_up=(r.h_w_up, r.w_up),
        w_down=(r.h_w_down, r.w_down),
        gate=(r.h_gate, r.gate),
    )
    for name, (source, target) in loads.items():
        pltpu.make_async_copy(source, target, getattr(local, name)).start()

    def loaded(target, sem):
        pltpu.make_async_copy(target, target, sem).wait()

    def store(source, target, sem):
        pltpu.make_async_copy(source, target, sem).start()

    def send(src, dst, channel, n, sp, tp):
        out_sem, in_sem = channel
        pltpu.make_async_remote_copy(
            src_ref=src,
            dst_ref=dst,
            send_sem=out_sem.at[n],
            recv_sem=in_sem.at[n],
            device_id=(sp, tp),
            device_id_type=MESH,
        ).start()

    def got(ref, channel, n=0):
        pltpu.make_async_copy(ref, ref, channel[1].at[n]).wait()

    def sent(ref, channel, n=0):
        pltpu.make_async_copy(ref, ref, channel[0].at[n]).wait()

    class Ring:
        def __init__(self, piece, channel, members, targets):
            self.piece, self.channel = piece, channel
            self.mine, self.right, self.left, self.opp = members
            self.to_right, self.to_left = targets

        def go(self, n, h, sem, target):
            part = self.piece(n, h)
            send(part, part, self.channel, sem, *target)

        def start(self):
            self.go(self.mine, 0, 0, self.to_right)
            self.go(self.mine, 1, 2, self.to_left)
            self.go(self.mine, 1, 1, self.to_right)
            self.go(self.mine, 0, 3, self.to_left)

        def step(self):
            got(self.piece(self.left, 0), self.channel, 0)
            self.go(self.left, 0, 4, self.to_right)
            got(self.piece(self.right, 1), self.channel, 2)
            self.go(self.right, 1, 5, self.to_left)

        def near(self):
            got(self.piece(self.left, 1), self.channel, 1)
            got(self.piece(self.right, 0), self.channel, 3)

        def far(self):
            got(self.piece(self.opp, 0), self.channel, 4)
            got(self.piece(self.opp, 1), self.channel, 5)

        def sent(self):
            for sem, n, h in ((0, self.mine, 0), (1, self.mine, 1), (2, self.mine, 1), (3, self.mine, 0)):
                sent(self.piece(n, h), self.channel, sem)
            sent(self.piece(self.left, 0), self.channel, 4)
            sent(self.piece(self.right, 1), self.channel, 5)

    def tp_ring(buf, channel):
        half = buf.shape[1] // 2
        piece = lambda n, h: buf.at[n, pl.ds(h * half, half)]
        return Ring(piece, channel, (tx, right, left, opp), ((me, right), (me, left)))

    def y_ring(piece, channel):
        members = (j, (j + 2) % 8, (j + 6) % 8, (j + 4) % 8)
        return Ring(piece, channel, members, ((z * 8 + members[1], tx), (z * 8 + members[2], tx)))

    rows_ring = tp_ring(r.full, c.rows)
    arrived_ring = tp_ring(r.arr, c.arrived)
    residual_ring = tp_ring(r.resid, c.residual)
    weight_ring = y_ring(lambda n, h: r.weight.at[pl.ds(4 * h, 4), n], c.weight_y)
    mixed_ring = y_ring(lambda n, h: r.mixed.at[n, pl.ds(64 * h, 64)], c.mixed_y)

    def share(ring, channel, *members):
        for n in members:
            for h in range(2):
                part = ring.piece(n, h)
                send(part, part, channel, 0, z * 8 + partner, tx)

    def to_all(out, into, channel):
        @pl.loop(1, 64)
        def _(d):
            peer = (me + d) % 64
            send(out.at[peer], into.at[me], channel, 0, peer, tx)

        into[me] = out[me]

    def to_group(out, into, channel):
        @pl.loop(1, 8)
        def _(d):
            peer = (j + d) % 8
            send(out.at[peer], into.at[j], channel, 0, z * 8 + peer, tx)

        into[j] = out[j]

    def to_planes(src, into, channel):
        @pl.loop(1, 8)
        def _(d):
            send(src, into.at[z], channel, 0, ((z + d) % 8) * 8 + j, tx)

    eye = hot(iota((128, 128), 0) == iota((128, 128), 1), F32)
    loaded(r.routes, local.routes)
    loaded(r.route_weights, local.route_weights)
    routes = dot(eye, r.routes[...].astype(F32), 1, 1, precision=HIGHEST)
    route_weights = dot(eye, r.route_weights[...], 1, 1, precision=HIGHEST)
    expert = iota((128, 64), 1).astype(F32)
    route = [routes[:, 0:1], routes[:, 1:2]]
    named = [hot(route[n] == expert, F32) for n in range(2)]
    strict = iota((128, 128), 0) > iota((128, 128), 1)
    earlier = dot(hot(strict), (named[0] + named[1]).astype(BF16))
    slot = iota((128, 512), 1).astype(F32)
    loaded(r.cot, local.cot)
    cot = r.cot[...].astype(F32)
    scaled = []
    for n in range(2):
        rank = jnp.sum(named[n] * earlier, axis=1, keepdims=True)
        upper = jnp.where(rank >= 3.0, 1.0, 0.0)
        base = route[n] * 8.0
        r.hit_a[n] = hot(slot == base + rank)
        for m in range(3):
            place = jnp.where(rank - 3.0 * upper == float(m), base + 6.0 + upper, -1.0)
            r.hit_b[n, m] = hot(slot == place)
        scaled.append((route_weights[:, n : n + 1] * cot).astype(BF16))
    for m in range(3):
        lanes = slice(m * 128, (m + 1) * 128)
        total = dot(r.hit_a[0], scaled[0][:, lanes], 0, 0)
        total = total + dot(r.hit_a[1], scaled[1][:, lanes], 0, 0)
        total = total + dot(r.hit_b[0, m], scaled[0][:, 384:512], 0, 0)
        total = total + dot(r.hit_b[1, m], scaled[1][:, 384:512], 0, 0)
        r.pack_out[:, :, lanes] = total.reshape(64, 8, 128).astype(BF16)
    pl.semaphore_wait(barrier, 65)
    to_all(r.pack_out, r.pack_in, c.dispatch)
    loaded(r.full.at[tx], local.rows)
    rows_ring.start()

    loaded(r.out_weight, local.out_weight)

    @pl.loop(1, 8)
    def _(d):
        send(r.out_weight, r.weight.at[z, j], c.weight_z, 0, ((z + d) % 8) * 8 + j, tx)

    r.weight[z, j] = r.out_weight[...]

    row, col = iota((128, 128), 0), iota((128, 128), 1)
    tri = hot(row >= col, F32)
    head_of = iota((16, 1024), 1) // 64 == iota((16, 1024), 0)
    loaded(r.log_decay, local.log_decay)
    loaded(r.v, local.v)
    loaded(r.k, local.k)
    log_decay = r.log_decay[...]
    cumulative = dot(tri, log_decay, 1, 1, precision=HIGHEST)
    r.c_col[...] = dot(cumulative, hot(iota((16, 128), 0) == iota((16, 128), 1), F32), precision=HIGHEST)
    r.c_row[...] = dot(log_decay, tri, 1, 1, precision=HIGHEST)
    r.c_exp[...] = dot(cumulative, hot(head_of, F32), precision=HIGHEST)
    c_exp = r.c_exp[...]
    r.from_start[...] = jnp.exp(c_exp)
    r.to_end[...] = jnp.exp(r.c_exp[127:128, :] - c_exp)
    r.v_end[0], r.v_end[1] = split(r.v[...].astype(F32) * r.to_end[...])
    for g in range(2):
        wide, k = slice(g * 512, (g + 1) * 512), r.k[:, g * 128 : (g + 1) * 128]
        own = dot(r.v_end[0, :, wide], k, 0, 0) + dot(r.v_end[1, :, wide], k, 0, 0)
        r.f_own[g * 4 : (g + 1) * 4] = own.reshape(4, 128, 128)
    total = dot(log_decay, jnp.ones((128, 128), F32), precision=HIGHEST)
    spread = hot(iota((64, 16), 0) // 4 == iota((64, 16), 1), F32)
    r.log_out[...] = dot(spread, total, precision=HIGHEST).reshape(8, 8, 128)
    to_group(r.f_own, r.f_in, c.f_j)
    to_group(r.log_out, r.log_in, c.f_jlog)

    place, packed = iota((384, 512), 0), iota((384, 512), 1)
    source, rank = place // 6, place % 6
    r.sel_a[...] = hot(packed == source * 8 + rank)
    for m in range(3):
        r.sel_b[m] = hot((packed == source * 8 + 6 + rank // 3) & (rank % 3 == m))

    lower = row >= col
    first = col < 64
    loaded(r.q, local.q)
    for g in range(2):
        r.qk[g] = dot(r.q[:, g * 128 : (g + 1) * 128], r.k[:, g * 128 : (g + 1) * 128], 1, 1)

    def masked_values(p):
        vp = r.v[:, pl.ds(pl.multiple_of(p * 128, 128), 128)].astype(F32)
        return jnp.concatenate(
            [jnp.where(first, vp, 0.0).astype(BF16), jnp.where(first, 0.0, vp).astype(BF16)], axis=0
        )

    @pl.loop(0, 8)
    def _(p):
        off = pl.multiple_of(p * 128, 128)
        qk = r.qk[p // 4]
        c_pair = r.c_exp[:, pl.ds(off, 128)]
        for n in range(2):
            down = jnp.minimum(c_pair[:, 64 * n : 64 * n + 1] - r.c_row[pl.ds(2 * p + n, 1), :], 0.0)
            decay = jnp.where(lower, jnp.exp(down), 0.0)
            r.decay[p, :, n * 128 : (n + 1) * 128] = decay
            lanes = slice(n * 128, (n + 1) * 128)
            r.score[0, p, :, lanes], r.score[1, p, :, lanes] = split(qk * decay)
        values = masked_values(p)
        r.y[:, pl.ds(off, 128)] = dot(r.score[0, p], values) + dot(r.score[1, p], values)

    rows_ring.step()

    def factor(log):
        e = jnp.exp(log)
        return jnp.concatenate(
            [jnp.broadcast_to(e[0:1], (64, 128)), jnp.broadcast_to(e[4:5], (64, 128))], axis=0
        )

    def carry_group(states, run_ref, reverse):
        run, log = jnp.zeros((128, 128), F32), jnp.zeros((8, 128), F32)
        for i in reversed(range(8)) if reverse else range(8):
            r.before[i] = run
            r.log_before[i] = log
            run = factor(r.log_in[i]) * run + states[i].astype(F32)
            log = log + r.log_in[i]
        run_ref[...] = run.astype(run_ref.dtype)
        return log

    def carry_planes(planes, back, reverse):
        run = jnp.zeros((128, 128), F32)
        for i in reversed(range(8)) if reverse else range(8):
            passed = i > z if reverse else i < z
            run = jnp.where(passed, factor(r.log_z[i]) * run + planes[i].astype(F32), run)
        for i in range(8):
            back[i] = r.before[i] + factor(r.log_before[i]) * run

    got(r.f_in.at[pl.ds(0, 7)], c.f_j)
    got(r.log_in.at[pl.ds(0, 7)], c.f_jlog)
    r.log_run[...] = carry_group(r.f_in, r.f_run, False)
    r.log_z[z] = r.log_run[...]
    r.f_z[z] = r.f_run[...]
    to_planes(r.f_run, r.f_z, c.f_z)
    to_planes(r.log_run, r.log_z, c.f_zlog)

    got(r.pack_in.at[pl.ds(0, 63)], c.dispatch)
    packed_in = r.pack_in[...].reshape(512, 384)
    r.arr[tx, :, 0:384] = dot(r.sel_a[...], packed_in).astype(BF16)
    tail = dot(r.sel_b[0], packed_in[:, 0:128])
    tail = tail + dot(r.sel_b[1], packed_in[:, 128:256])
    tail = tail + dot(r.sel_b[2], packed_in[:, 256:384])
    r.arr[tx, :, 384:512] = tail.astype(BF16)
    arrived_ring.start()

    rows_ring.near()
    rows_ring.far()
    loaded(r.w_gate, local.w_gate)
    loaded(r.w_up, local.w_up)
    loaded(r.w_down, local.w_down)
    gate_pre, up_pre = jnp.zeros((384, 256), F32), jnp.zeros((384, 256), F32)
    for t in range(4):
        gate_pre = gate_pre + dot(r.full[t], r.w_gate[t * 512 : (t + 1) * 512, :])
    r.gate_pre[...] = gate_pre
    for t in range(4):
        up_pre = up_pre + dot(r.full[t], r.w_up[t * 512 : (t + 1) * 512, :])
    r.up_pre[...] = up_pre
    gate_pre = r.gate_pre[...]
    r.hidden[...] = (gate_pre * sigmoid(gate_pre) * up_pre).astype(BF16)

    def hidden_part(t):
        return dot(r.arr[t], r.w_down[:, pl.ds(pl.multiple_of(t * 512, 512), 512)], 1, 1)

    r.hidden_grad[...] = hidden_part(tx)
    arrived_ring.step()
    arrived_ring.near()
    r.hidden_grad[...] += hidden_part(left)
    r.hidden_grad[...] += hidden_part(right)

    arrived_ring.far()
    hidden_grad = r.hidden_grad[...] + hidden_part(opp)
    gate_pre = r.gate_pre[...]
    gate_sig = sigmoid(gate_pre)
    slope = gate_sig * (1.0 + gate_pre * (1.0 - gate_sig))
    r.gate_grad[...] = (hidden_grad * r.up_pre[...] * slope).astype(BF16)
    r.up_grad[...] = (hidden_grad * (gate_pre * gate_sig)).astype(BF16)

    def row_part(t):
        rows = pl.ds(pl.multiple_of(t * 512, 512), 512)
        part = dot(r.gate_grad[...], r.w_gate[rows, :], 1, 1)
        return part + dot(r.up_grad[...], r.w_up[rows, :], 1, 1)

    top, bottom = pl.ds(0, 192), pl.ds(192, 192)
    r.rs_opp[...] = row_part(opp).astype(BF16)
    send(r.rs_opp.at[top], r.rs_half_l, c.scatter, 0, me, right)
    send(r.rs_opp.at[bottom], r.rs_half_r, c.scatter, 1, me, left)
    r.rs_own[...] = row_part(right)
    r.rs_right[bottom] = r.rs_own[bottom].astype(BF16)
    send(r.rs_right.at[bottom], r.rs_in_l.at[bottom], c.scatter, 2, me, right)
    r.rs_own_l[...] = row_part(left)
    r.rs_left[top] = r.rs_own_l[top].astype(BF16)
    send(r.rs_left.at[top], r.rs_in_r.at[top], c.scatter, 3, me, left)

    got(r.weight.at[pl.ds(0, 7), 0], c.weight_z)
    weight_ring.start()
    share(weight_ring, c.weight_c, j)

    got(r.rs_half_l, c.scatter, 0)
    r.rs_right[top] = (r.rs_own[top] + r.rs_half_l[...].astype(F32)).astype(BF16)
    send(r.rs_right.at[top], r.rs_in_l.at[top], c.scatter, 4, me, right)
    got(r.rs_half_r, c.scatter, 1)
    r.rs_left[bottom] = (r.rs_own_l[bottom] + r.rs_half_r[...].astype(F32)).astype(BF16)
    send(r.rs_left.at[bottom], r.rs_in_r.at[bottom], c.scatter, 5, me, left)
    r.rs_own[...] = row_part(tx)

    got(r.f_z.at[pl.ds(0, 7)], c.f_z)
    got(r.log_z.at[pl.ds(0, 7)], c.f_zlog)
    carry_planes(r.f_z, r.f_back, False)
    to_group(r.f_back, r.state, c.f_back)

    @pl.loop(0, 4)
    def _(t):
        rows = pl.ds(pl.multiple_of(t * 512, 512), 512)
        r.o_gate[rows, :] = dot(r.full[t], r.gate_grad[...], 0, 0).astype(BF16)
        r.o_up[rows, :] = dot(r.full[t], r.up_grad[...], 0, 0).astype(BF16)
        r.o_down[:, rows] = dot(r.hidden[...], r.arr[t], 0, 0).astype(BF16)

    store(r.o_gate, r.g_gate, result.gate)
    store(r.o_up, r.g_up, result.up)
    store(r.o_down, r.g_down, result.down)
    weight_ring.step()

    got(r.rs_in_l.at[bottom], c.scatter, 2)
    got(r.rs_in_l.at[top], c.scatter, 4)
    got(r.rs_in_r.at[top], c.scatter, 3)
    got(r.rs_in_r.at[bottom], c.scatter, 5)
    summed = r.rs_own[...] + r.rs_in_l[...].astype(F32) + r.rs_in_r[...].astype(F32)
    summed = summed.astype(BF16)
    for m in range(3):
        lanes = slice(m * 128, (m + 1) * 128)
        total = dot(r.sel_a[...], summed[:, lanes], 0, 0)
        total = total + dot(r.sel_b[m], summed[:, 384:512], 0, 0)
        r.ret_out[:, :, lanes] = total.reshape(64, 8, 128).astype(BF16)
    to_all(r.ret_out, r.ret_in, c.back)

    got(r.state.at[pl.ds(0, 7)], c.f_back)
    for g in range(2):
        lanes = slice(g * 512, (g + 1) * 512)
        high, low = split(r.state[g * 4 : (g + 1) * 4].reshape(512, 128))
        q = r.q[:, g * 128 : (g + 1) * 128]
        r.carried[:, lanes] = (dot(q, high, 1, 1) + dot(q, low, 1, 1)) * r.from_start[:, lanes]
    y = r.y[...] + r.carried[...]
    r.y[...] = y
    loaded(r.gate, local.gate)
    gate = r.gate[...].astype(F32)
    r.mixed[j] = (y * (gate * sigmoid(gate))).astype(BF16)
    mixed_ring.start()
    share(mixed_ring, c.mixed_c, j)
    weight_ring.near()
    weight_ring.far()
    share(weight_ring, c.weight_c, weight_ring.left, weight_ring.right, weight_ring.opp)
    mixed_ring.step()

    got(r.ret_in.at[pl.ds(0, 63)], c.back)
    packed_back = r.ret_in[...].reshape(512, 384)
    picked = dot(r.hit_a[0] + r.hit_a[1], packed_back)
    tail = dot(r.hit_b[0, 0] + r.hit_b[1, 0], packed_back[:, 0:128])
    tail = tail + dot(r.hit_b[0, 1] + r.hit_b[1, 1], packed_back[:, 128:256])
    tail = tail + dot(r.hit_b[0, 2] + r.hit_b[1, 2], packed_back[:, 256:384])
    picked = jnp.concatenate([picked, tail], axis=1)
    residual = r.cot[...].astype(F32) + picked
    r.resid[tx] = residual.astype(BF16)
    residual_ring.start()
    r.o_res[...] = residual
    store(r.o_res, r.g_res, result.res)
    residual_ring.step()
    got(r.weight.at[:, pl.ds(0, 4)], c.weight_c)
    residual_ring.near()
    residual_ring.far()

    @pl.loop(0, 4)
    def _(n):
        lanes = pl.ds(pl.multiple_of(n * 256, 256), 256)
        grad = jnp.zeros((128, 256), F32)
        for t in range(4):
            w = r.weight[2 * t : 2 * t + 2, :, :, lanes].reshape(512, 256)
            grad = grad + dot(r.resid[t], w)
        gate = r.gate[:, lanes].astype(F32)
        sig = sigmoid(gate)
        r.o_gate_in[:, lanes] = grad * r.y[:, lanes] * (sig * (1.0 + gate * (1.0 - sig)))
        dy = grad * (gate * sig)
        r.dy[:, lanes] = dy
        r.dy_start[0, :, lanes], r.dy_start[1, :, lanes] = split(dy * r.from_start[:, lanes])

    store(r.o_gate_in, r.g_gate_in, result.gate_in)
    for g in range(2):
        wide, q = slice(g * 512, (g + 1) * 512), r.q[:, g * 128 : (g + 1) * 128]
        reached = dot(r.dy_start[0, :, wide], q, 0, 0) + dot(r.dy_start[1, :, wide], q, 0, 0)
        r.b_own[g * 4 : (g + 1) * 4] = reached.reshape(4, 128, 128)
    to_group(r.b_own, r.b_in, c.b_j)

    for t in range(4):
        turned = dot(r.resid[t], eye.astype(BF16), 0, 0)
        r.res_t[2 * t : 2 * t + 2] = turned.reshape(2, 8, 32, 128).astype(BF16)

    @pl.loop(1, 8)
    def _(d):
        peer = (j + d) % 8
        send(r.res_t.at[:, peer], r.res_in.at[j], c.gow_j, 0, z * 8 + peer, tx)

    r.res_in[j] = r.res_t[:, j]

    mixed_ring.near()
    mixed_ring.far()
    share(mixed_ring, c.mixed_c, mixed_ring.left, mixed_ring.right, mixed_ring.opp)

    got(r.b_in.at[pl.ds(0, 7)], c.b_j)
    carry_group(r.b_in, r.b_run, True)
    r.b_z[z] = r.b_run[...]
    to_planes(r.b_run, r.b_z, c.b_z)

    got(r.res_in.at[pl.ds(0, 7)], c.gow_j)
    got(r.mixed.at[pl.ds(0, 4)], c.mixed_c)

    @pl.loop(0, 4)
    def _(n):
        lanes = pl.ds(pl.multiple_of(n * 256, 256), 256)
        part = jnp.zeros((256, 256), F32)
        for i in range(8):
            part = part + dot(r.res_in[i].reshape(256, 128), r.mixed[i, :, lanes])
        part = part.reshape(8, 32, 256)
        r.gow_part[:, :, lanes] = part
        r.gow_out[:, :, lanes] = part.astype(BF16)

    @pl.loop(1, 8)
    def _(d):
        plane = (z + d) % 8
        send(r.gow_out.at[plane], r.gow_in.at[z], c.gow_z, 0, plane * 8 + j, tx)

    r.row_col[...] = jnp.zeros((128, 128), F32)
    r.dqk[...] = jnp.zeros((2, 128, 128), F32)

    @pl.loop(0, 8)
    def _(p):
        off = pl.multiple_of(p * 128, 128)
        g = p // 4
        qk = r.qk[g]
        dy = r.dy[:, pl.ds(off, 128)]
        part = dot(dy.astype(BF16), masked_values(p), 1, 1) * r.decay[p]
        r.dqk[g] += part[:, 0:128] + part[:, 128:256]
        total = r.row_col[...]
        dv = jnp.zeros((128, 128), F32)
        for n in range(2):
            lanes = slice(n * 128, (n + 1) * 128)
            weighed = (part[:, lanes] * qk).astype(BF16)
            head = hot(col == 2 * p + n)
            total = total + dot(weighed, head) - dot(weighed, head, 0, 0)
            own = jnp.where(first, dy, 0.0) if n == 0 else jnp.where(first, 0.0, dy)
            dv = dv + dot(r.score[0, p, :, lanes], own.astype(BF16), 0, 0)
        r.row_col[...] = total
        r.dv[:, pl.ds(off, 128)] = dv

    by_head = hot(iota((1024, 128), 0) // 64 == iota((1024, 128), 1))
    r.row_col[...] += fine_dot(r.dy[...] * r.carried[...], by_head)
    for g in range(2):
        state = r.state[g * 4 : (g + 1) * 4].reshape(512, 128).astype(BF16)
        r.dq[:, g * 128 : (g + 1) * 128] = dot(r.dy_start[0, :, g * 512 : (g + 1) * 512], state)

    got(r.b_z.at[pl.ds(0, 7)], c.b_z)
    carry_planes(r.b_z, r.b_back, True)
    to_group(r.b_back, r.dstate, c.b_back)

    for g in range(2):
        lanes = slice(g * 128, (g + 1) * 128)
        r.o_q[:, lanes] = r.dq[:, lanes] + dot(r.dqk[g].astype(BF16), r.k[:, lanes])
    store(r.o_q, r.g_q, result.q)

    got(r.dstate.at[pl.ds(0, 7)], c.b_back)
    for g in range(2):
        lanes, wide = slice(g * 128, (g + 1) * 128), slice(g * 512, (g + 1) * 512)
        dstate, low = split(r.dstate[g * 4 : (g + 1) * 4].reshape(512, 128))
        k = r.k[:, lanes]
        through = (dot(k, dstate, 1, 1) + dot(k, low, 1, 1)) * r.to_end[:, wide]
        r.carried[:, wide] = through
        r.o_v[:, wide] = r.dv[:, wide] + through
        r.o_k[:, lanes] = dot(r.dqk[g].astype(BF16), r.q[:, lanes], 0, 0) + dot(r.v_end[0, :, wide], dstate)
    store(r.o_v, r.g_v, result.v)
    store(r.o_k, r.g_k, result.k)
    added = fine_dot(r.v[...].astype(F32) * r.carried[...], by_head)
    high, low = split((r.dstate[...] * r.state[...]).reshape(1024, 128))
    both = dot(by_head, high, 0, 0) + dot(by_head, low, 0, 0)
    kept = dot(jnp.ones((128, 128), F32), both, 1, 1, precision=HIGHEST)
    kept = kept * jnp.exp(r.c_col[127:128, :])
    upper = hot(row <= col, F32)
    below = hot(row > col, F32)
    grad = dot(upper, r.row_col[...], precision=HIGHEST) + dot(below, added, precision=HIGHEST) + kept
    r.o_decay[...] = dot(eye[0:16], grad, 1, 1, precision=HIGHEST)
    store(r.o_decay, r.g_decay, result.decay)

    got(r.gow_in.at[pl.ds(0, 7)], c.gow_z)
    total = r.gow_part[z]
    for d in range(1, 8):
        total = total + r.gow_in[(z + d) % 8].astype(F32)
    r.o_out[...] = total
    store(r.o_out, r.g_out, result.out)

    for ring in (rows_ring, arrived_ring, residual_ring, weight_ring, mixed_ring):
        ring.sent()
    sent(r.pack_out.at[pl.ds(0, 63)], c.dispatch)
    sent(r.ret_out.at[pl.ds(0, 63)], c.back)
    for n in range(6):
        sent(r.rs_half_l, c.scatter, n)
    sent(r.weight.at[pl.ds(0, 7), 0], c.weight_z)
    sent(r.weight.at[:, pl.ds(0, 4)], c.weight_c)
    sent(r.mixed.at[pl.ds(0, 4)], c.mixed_c)
    sent(r.res_in.at[pl.ds(0, 7)], c.gow_j)
    sent(r.gow_out.at[pl.ds(0, 7)], c.gow_z)
    for channel in (c.f_j, c.f_z, c.f_back, c.b_j, c.b_back):
        sent(r.f_in.at[pl.ds(0, 7)], channel)
    sent(r.b_z.at[pl.ds(0, 7)], c.b_z)
    for channel in (c.f_jlog, c.f_zlog):
        sent(r.log_in.at[pl.ds(0, 7)], channel)
    for name in OUTPUTS:
        target = getattr(r, name)
        loaded(target, getattr(result, name[2:]))


def shards(
    out_cotangent,
    routes,
    route_weights,
    expert_rows,
    w_gate,
    w_up,
    w_down,
    out_weight,
    values,
    keys,
    queries,
    log_decay,
    gate_input,
):
    arrays = [jax.ShapeDtypeStruct(shape, dtype) for shape, dtype in OUTPUTS.values()]
    held = [pltpu.VMEM(shape, dtype) for shape, dtype in OUTPUTS.values()]
    scratch = [pltpu.VMEM(shape, dtype) for shape, dtype in BUFFERS.values()] + held
    for n in CHANNELS.values():
        scratch += [pltpu.SemaphoreType.DMA((n,))] * 2
    scratch += [pltpu.SemaphoreType.DMA((len(INPUTS),)), pltpu.SemaphoreType.DMA((len(OUTPUTS),))]
    outs = pl.pallas_call(
        kernel,
        out_shape=arrays,
        in_specs=[pl.BlockSpec(memory_space=pl.ANY)] * len(INPUTS),
        out_specs=[pl.BlockSpec(memory_space=pl.ANY)] * len(OUTPUTS),
        scratch_shapes=scratch,
        compiler_params=pltpu.CompilerParams(
            has_side_effects=True, collective_id=0, vmem_limit_bytes=66_000_000
        ),
        name="layer_backward",
    )(
        out_cotangent,
        routes.T,
        route_weights.T,
        expert_rows[0],
        w_gate[0],
        w_up[0],
        w_down[0],
        out_weight,
        values,
        keys,
        queries,
        log_decay.T,
        gate_input,
    )
    outs = pl.pallas_call(
        publish,
        out_shape=arrays,
        in_specs=[pl.BlockSpec(memory_space=pl.ANY)] * len(OUTPUTS),
        out_specs=[pl.BlockSpec(memory_space=pl.ANY)] * len(OUTPUTS),
        scratch_shapes=held + [pltpu.SemaphoreType.DMA((2, len(OUTPUTS)))],
        compiler_params=pltpu.CompilerParams(vmem_limit_bytes=66_000_000),
        name="publish",
    )(*outs)
    outs = list(outs)
    outs[8] = outs[8].T
    return (outs[0][None], outs[1][None], outs[2][None]) + tuple(outs[3:])


def solution(mesh):
    sp, both = P("sp", None), P("sp", "tp")
    columns, hidden = P("sp", None, "tp"), P("sp", "tp", None)
    in_specs = (sp, sp, sp, columns, columns, columns, hidden) + (both,) * 6
    out_specs = (columns, columns, hidden) + (both,) * 7
    return jax.shard_map(
        shards, mesh=mesh, in_specs=in_specs, out_specs=out_specs, check_vma=False
    )
```

```python
import jax
import jax.numpy as jnp
from jax import lax
from jax.experimental import pallas as pl
from jax.experimental.pallas import tpu as pltpu
from jax.sharding import PartitionSpec as P

MESH = pl.DeviceIdType.MESH
F32, BF16 = jnp.float32, jnp.bfloat16
HIGHEST = lax.Precision.HIGHEST

BUFFERS = dict(
    cot=((128, 512), BF16),
    routes=((2, 128), jnp.int32),
    route_weights=((2, 128), F32),
    w_gate=((2048, 256), BF16),
    w_up=((2048, 256), BF16),
    w_down=((256, 2048), BF16),
    v=((128, 1024), BF16),
    k=((128, 256), BF16),
    q=((128, 256), BF16),
    log_decay=((16, 128), F32),
    gate=((128, 1024), BF16),
    pack_out=((64, 8, 384), BF16),
    pack_in=((64, 8, 384), BF16),
    pack_sorted=((64, 8, 384), BF16),
    ret_out=((64, 8, 384), BF16),
    ret_in=((64, 8, 384), BF16),
    hit_a=((2, 128, 512), BF16),
    hit_b=((2, 3, 128, 512), BF16),
    sel_a=((384, 512), BF16),
    sel_b=((3, 384, 512), BF16),
    arr=((4, 384, 512), BF16),
    full=((4, 384, 512), BF16),
    gate_pre=((384, 256), F32),
    up_pre=((384, 256), F32),
    hidden_grad=((384, 256), F32),
    hidden=((384, 256), BF16),
    gate_grad=((384, 256), BF16),
    up_grad=((384, 256), BF16),
    rs_opp=((384, 512), BF16),
    rs_right=((384, 512), BF16),
    rs_left=((384, 512), BF16),
    rs_half_l=((384, 512), BF16),
    rs_half_r=((384, 512), BF16),
    rs_in_l=((384, 512), BF16),
    rs_in_r=((384, 512), BF16),
    rs_own=((384, 512), F32),
    rs_own_l=((384, 512), F32),
    rs_own_r=((384, 512), F32),
    resid=((4, 128, 512), BF16),
    res_t=((2, 8, 32, 128), BF16),
    res_in=((4, 8, 2, 32, 128), BF16),
    weight=((8, 8, 32, 1024), BF16),
    mixed=((8, 128, 1024), BF16),
    gow_part=((8, 32, 1024), F32),
    gow_out=((8, 32, 1024), BF16),
    gow_in=((8, 32, 1024), BF16),
    c_exp=((128, 1024), F32),
    to_end=((128, 1024), F32),
    from_start=((128, 1024), F32),
    c_row=((16, 128), F32),
    c_col=((128, 128), F32),
    v_end=((2, 128, 1024), BF16),
    qk=((2, 128, 128), F32),
    decay=((8, 128, 256), F32),
    score=((2, 8, 128, 256), BF16),
    y=((128, 1024), F32),
    carried=((128, 1024), F32),
    dy=((128, 1024), F32),
    dy_start=((128, 1024), BF16),
    dv=((128, 1024), F32),
    dqk=((2, 128, 128), F32),
    row_col=((128, 128), F32),
    dq=((128, 256), F32),
    log_out=((8, 8, 128), F32),
    log_in=((8, 8, 128), F32),
    log_run=((8, 128), F32),
    log_z=((8, 8, 128), F32),
    log_before=((8, 8, 128), F32),
    before=((8, 128, 128), F32),
    f_own=((8, 128, 128), F32),
    f_in=((8, 128, 128), F32),
    f_run=((128, 128), F32),
    f_z=((8, 128, 128), F32),
    f_back=((8, 128, 128), BF16),
    state=((8, 128, 128), BF16),
    b_own=((8, 128, 128), F32),
    b_in=((8, 128, 128), F32),
    b_run=((128, 128), BF16),
    b_z=((8, 128, 128), BF16),
    b_back=((8, 128, 128), F32),
    dstate=((8, 128, 128), F32),
)
CHANNELS = dict(
    rows=6,
    arrived=6,
    residual=6,
    dispatch=1,
    back=1,
    scatter=6,
    scatter_near=6,
    weight_z=1,
    weight_y=6,
    weight_c=1,
    mixed_y=6,
    mixed_c=1,
    gow_j=1,
    columns=6,
    gow_z=1,
    f_j=1,
    f_jlog=1,
    f_z=1,
    f_zlog=1,
    f_back=1,
    b_j=1,
    b_z=1,
    b_back=1,
)
INPUTS = dict(
    h_cot=((128, 2048), BF16),
    h_routes=((2, 128), jnp.int32),
    h_route_weights=((2, 128), F32),
    h_rows=((384, 512), BF16),
    h_w_gate=((2048, 256), BF16),
    h_w_up=((2048, 256), BF16),
    h_w_down=((256, 2048), BF16),
    h_out_weight=((32, 1024), BF16),
    h_v=((128, 1024), BF16),
    h_k=((128, 256), BF16),
    h_q=((128, 256), BF16),
    h_log_decay=((16, 128), F32),
    h_gate=((128, 1024), BF16),
)
OUTPUTS = dict(
    g_gate=((2048, 256), BF16),
    g_up=((2048, 256), BF16),
    g_down=((256, 2048), BF16),
    g_out=((32, 1024), F32),
    g_res=((128, 512), F32),
    g_v=((128, 1024), F32),
    g_k=((128, 256), F32),
    g_q=((128, 256), F32),
    g_decay=((16, 128), F32),
    g_gate_in=((128, 1024), F32),
)


PLANES = (4, 3, 5, 2, 6, 1, 7, 0)
FAR, NEAR = (0, 80, 144), (144, 256, 384)


class Refs:
    pass


def dot(a, b, ca=1, cb=0, precision=None):
    return lax.dot_general(
        a, b, (((ca,), (cb,)), ((), ())), precision=precision, preferred_element_type=F32
    )


def iota(shape, dim):
    return lax.broadcasted_iota(jnp.int32, shape, dim)


def hot(cond, dtype=BF16):
    return jnp.where(cond, 1.0, 0.0).astype(dtype)


def split(x):
    high = x.astype(BF16)
    return high, (x - high.astype(F32)).astype(BF16)


def fine_dot(a, b, ca=1, cb=0):
    high, low = split(a)
    return dot(high, b, ca, cb) + dot(low, b, ca, cb)


def sigmoid(x):
    return 1.0 / (1.0 + jnp.exp(-x))


def publish(*refs):
    n = len(OUTPUTS)
    sources, targets, held, sems = refs[:n], refs[n : 2 * n], refs[2 * n : 3 * n], refs[3 * n]
    loads = [pltpu.make_async_copy(sources[i], held[i], sems.at[0, i]) for i in range(n)]
    stores = [pltpu.make_async_copy(held[i], targets[i], sems.at[1, i]) for i in range(n)]
    for load in loads:
        load.start()
    for load, store in zip(loads, stores):
        load.wait()
        store.start()
    for store in stores:
        store.wait()


def kernel(*refs):
    r, c, local, result = Refs(), Refs(), Refs(), Refs()
    names = list(INPUTS) + list(OUTPUTS) + list(BUFFERS)
    for name, ref in zip(names, refs):
        setattr(r, name, ref)
    at = len(names)
    for name in OUTPUTS:
        setattr(r, name.replace("g_", "o_", 1), refs[at])
        at += 1
    for name in CHANNELS:
        setattr(c, name, (refs[at], refs[at + 1]))
        at += 2
    in_sems, out_sems = refs[at], refs[at + 1]
    for i, name in enumerate(INPUTS):
        setattr(local, name[2:], in_sems.at[i])
    for i, name in enumerate(OUTPUTS):
        setattr(result, name[2:], out_sems.at[i])

    me, tx = lax.axis_index("sp"), lax.axis_index("tp")
    z, j = me // 8, me % 8
    partner = j + 1 - 2 * (j % 2)
    right, left, opp = (tx + 1) % 4, (tx + 3) % 4, (tx + 2) % 4
    column = pl.multiple_of(tx * 512, 512)
    planes = [(z + d) % 8 for d in PLANES]

    barrier = pltpu.get_barrier_semaphore()

    @pl.loop(1, 64)
    def _(d):
        peer = (me + d) % 64
        pl.semaphore_signal(barrier, inc=1, device_id=(peer, tx), device_id_type=MESH)

    for side in (right, left):
        pl.semaphore_signal(barrier, inc=1, device_id=(me, side), device_id_type=MESH)

    loads = dict(
        routes=(r.h_routes, r.routes),
        route_weights=(r.h_route_weights, r.route_weights),
        cot=(r.h_cot.at[:, pl.ds(column, 512)], r.cot),
        log_decay=(r.h_log_decay, r.log_decay),
        k=(r.h_k, r.k),
        v=(r.h_v, r.v),
        out_weight=(r.h_out_weight, r.weight.at[z, j]),
        q=(r.h_q, r.q),
        w_gate=(r.h_w_gate, r.w_gate),
        w_up=(r.h_w_up, r.w_up),
        w_down=(r.h_w_down, r.w_down),
        gate=(r.h_gate, r.gate),
    )
    for name, (source, target) in loads.items():
        pltpu.make_async_copy(source, target, getattr(local, name)).start()

    for n in range(8):
        source = r.h_rows.at[pl.ds(pl.multiple_of(planes[n] * 48, 16), 48)]
        pltpu.make_async_copy(source, r.full.at[tx, pl.ds(n * 48, 48)], local.rows).start()

    def loaded(target, sem):
        pltpu.make_async_copy(target, target, sem).wait()

    def store(source, target, sem):
        pltpu.make_async_copy(source, target, sem).start()

    def send(src, dst, channel, n, sp, tp):
        out_sem, in_sem = channel
        pltpu.make_async_remote_copy(
            src_ref=src,
            dst_ref=dst,
            send_sem=out_sem.at[n],
            recv_sem=in_sem.at[n],
            device_id=(sp, tp),
            device_id_type=MESH,
        ).start()

    def got(ref, channel, n=0):
        pltpu.make_async_copy(ref, ref, channel[1].at[n]).wait()

    def sent(ref, channel, n=0):
        pltpu.make_async_copy(ref, ref, channel[0].at[n]).wait()

    class Ring:
        def __init__(self, piece, channel, members, targets):
            self.piece, self.channel = piece, channel
            self.mine, self.right, self.left, self.opp = members
            self.to_right, self.to_left = targets

        def go(self, n, h, sem, target):
            part = self.piece(n, h)
            send(part, part, self.channel, sem, *target)

        def start(self):
            self.first()
            self.second()

        def first(self):
            self.go(self.mine, 0, 0, self.to_right)
            self.go(self.mine, 1, 2, self.to_left)

        def second(self):
            self.go(self.mine, 1, 1, self.to_right)
            self.go(self.mine, 0, 3, self.to_left)

        def step(self):
            got(self.piece(self.left, 0), self.channel, 0)
            self.go(self.left, 0, 4, self.to_right)
            got(self.piece(self.right, 1), self.channel, 2)
            self.go(self.right, 1, 5, self.to_left)

        def near(self):
            got(self.piece(self.left, 1), self.channel, 1)
            got(self.piece(self.right, 0), self.channel, 3)

        def far(self):
            got(self.piece(self.opp, 0), self.channel, 4)
            got(self.piece(self.opp, 1), self.channel, 5)

        def sent(self):
            for sem, n, h in ((0, self.mine, 0), (1, self.mine, 1), (2, self.mine, 1), (3, self.mine, 0)):
                sent(self.piece(n, h), self.channel, sem)
            sent(self.piece(self.left, 0), self.channel, 4)
            sent(self.piece(self.right, 1), self.channel, 5)

    def tp_ring(buf, channel):
        half = buf.shape[1] // 2
        piece = lambda n, h: buf.at[n, pl.ds(h * half, half)]
        return Ring(piece, channel, (tx, right, left, opp), ((me, right), (me, left)))

    def y_ring(piece, channel):
        members = (j, (j + 2) % 8, (j + 6) % 8, (j + 4) % 8)
        return Ring(piece, channel, members, ((z * 8 + members[1], tx), (z * 8 + members[2], tx)))

    rows_ring = tp_ring(r.full, c.rows)
    arrived_ring = tp_ring(r.arr, c.arrived)
    residual_ring = tp_ring(r.resid, c.residual)
    columns_ring = tp_ring(r.res_in, c.columns)

    weight_ring = y_ring(lambda n, h: r.weight.at[pl.ds(4 * h, 4), n], c.weight_y)
    mixed_ring = y_ring(lambda n, h: r.mixed.at[n, pl.ds(64 * h, 64)], c.mixed_y)

    def share(ring, channel, *members):
        for n in members:
            for h in range(2):
                part = ring.piece(n, h)
                send(part, part, channel, 0, z * 8 + partner, tx)

    def to_plane_members(out, into, channel, n, first):
        own = PLANES[n] == 0

        @pl.loop(1 if own else 0, 8)
        def _(d):
            peer = (j + d) % 8
            send(out.at[first + peer], into.at[me], channel, 0, planes[n] * 8 + peer, tx)

        if own:
            into[me] = out[first + j]

    def to_group(out, into, channel):
        @pl.loop(1, 8)
        def _(d):
            peer = (j + d) % 8
            send(out.at[peer], into.at[j], channel, 0, z * 8 + peer, tx)

        into[j] = out[j]

    def to_planes(src, into, channel):
        @pl.loop(1, 8)
        def _(d):
            send(src, into.at[z], channel, 0, ((z + d) % 8) * 8 + j, tx)

    eye = hot(iota((128, 128), 0) == iota((128, 128), 1), F32)
    loaded(r.routes, local.routes)
    loaded(r.route_weights, local.route_weights)
    routes = dot(eye, r.routes[...].astype(F32), 1, 1, precision=HIGHEST)
    route_weights = dot(eye, r.route_weights[...], 1, 1, precision=HIGHEST)
    expert = iota((128, 64), 1).astype(F32)
    route = [routes[:, 0:1], routes[:, 1:2]]
    named = [hot(route[n] == expert, F32) for n in range(2)]
    strict = iota((128, 128), 0) > iota((128, 128), 1)
    earlier = dot(hot(strict), (named[0] + named[1]).astype(BF16))
    slot = iota((128, 512), 1).astype(F32)
    loaded(r.cot, local.cot)
    cot = r.cot[...].astype(F32)
    scaled = []
    for n in range(2):
        rank = jnp.sum(named[n] * earlier, axis=1, keepdims=True)
        upper = jnp.where(rank >= 3.0, 1.0, 0.0)
        base = route[n] * 8.0
        r.hit_a[n] = hot(slot == base + rank)
        for m in range(3):
            place = jnp.where(rank - 3.0 * upper == float(m), base + 6.0 + upper, -1.0)
            r.hit_b[n, m] = hot(slot == place)
        scaled.append((route_weights[:, n : n + 1] * cot).astype(BF16))
    for m in range(3):
        lanes = slice(m * 128, (m + 1) * 128)
        total = dot(r.hit_a[0], scaled[0][:, lanes], 0, 0)
        total = total + dot(r.hit_a[1], scaled[1][:, lanes], 0, 0)
        total = total + dot(r.hit_b[0, m], scaled[0][:, 384:512], 0, 0)
        total = total + dot(r.hit_b[1, m], scaled[1][:, 384:512], 0, 0)
        r.pack_out[:, :, lanes] = total.reshape(64, 8, 128).astype(BF16)
    row, col = iota((128, 128), 0), iota((128, 128), 1)
    tri = hot(row >= col, F32)
    head_of = iota((16, 1024), 1) // 64 == iota((16, 1024), 0)
    loaded(r.log_decay, local.log_decay)
    loaded(r.v, local.v)
    loaded(r.k, local.k)
    log_decay = r.log_decay[...]
    cumulative = dot(tri, log_decay, 1, 1, precision=HIGHEST)
    r.c_col[...] = dot(cumulative, hot(iota((16, 128), 0) == iota((16, 128), 1), F32), precision=HIGHEST)
    r.c_row[...] = dot(log_decay, tri, 1, 1, precision=HIGHEST)
    r.c_exp[...] = dot(cumulative, hot(head_of, F32), precision=HIGHEST)
    c_exp = r.c_exp[...]
    r.from_start[...] = jnp.exp(c_exp)
    r.to_end[...] = jnp.exp(r.c_exp[127:128, :] - c_exp)
    r.v_end[0], r.v_end[1] = split(r.v[...].astype(F32) * r.to_end[...])
    for g in range(2):
        wide, k = slice(g * 512, (g + 1) * 512), r.k[:, g * 128 : (g + 1) * 128]
        own = dot(r.v_end[0, :, wide], k, 0, 0) + dot(r.v_end[1, :, wide], k, 0, 0)
        r.f_own[g * 4 : (g + 1) * 4] = own.reshape(4, 128, 128)
    total = dot(log_decay, jnp.ones((128, 128), F32), precision=HIGHEST)
    spread = hot(iota((64, 16), 0) // 4 == iota((64, 16), 1), F32)
    r.log_out[...] = dot(spread, total, precision=HIGHEST).reshape(8, 8, 128)
    place, packed = iota((384, 512), 0), iota((384, 512), 1)
    source, rank = place // 6, place % 6
    r.sel_a[...] = hot(packed == source * 8 + rank)
    for m in range(3):
        r.sel_b[m] = hot((packed == source * 8 + 6 + rank // 3) & (rank % 3 == m))

    lower = row >= col
    first = col < 64
    loaded(r.q, local.q)
    for g in range(2):
        r.qk[g] = dot(r.q[:, g * 128 : (g + 1) * 128], r.k[:, g * 128 : (g + 1) * 128], 1, 1)

    def masked_values(p):
        vp = r.v[:, pl.ds(pl.multiple_of(p * 128, 128), 128)].astype(F32)
        return jnp.concatenate(
            [jnp.where(first, vp, 0.0).astype(BF16), jnp.where(first, 0.0, vp).astype(BF16)], axis=0
        )

    @pl.loop(0, 8)
    def _(p):
        off = pl.multiple_of(p * 128, 128)
        qk = r.qk[p // 4]
        c_pair = r.c_exp[:, pl.ds(off, 128)]
        for n in range(2):
            down = jnp.minimum(c_pair[:, 64 * n : 64 * n + 1] - r.c_row[pl.ds(2 * p + n, 1), :], 0.0)
            decay = jnp.where(lower, jnp.exp(down), 0.0)
            r.decay[p, :, n * 128 : (n + 1) * 128] = decay
            lanes = slice(n * 128, (n + 1) * 128)
            r.score[0, p, :, lanes], r.score[1, p, :, lanes] = split(qk * decay)
        values = masked_values(p)
        r.y[:, pl.ds(off, 128)] = dot(r.score[0, p], values) + dot(r.score[1, p], values)

    pl.semaphore_wait(barrier, 65)
    for n in range(8):
        to_plane_members(r.pack_out, r.pack_in, c.dispatch, n, planes[n] * 8)
    loaded(r.full.at[tx], local.rows)
    rows_ring.start()
    to_group(r.f_own, r.f_in, c.f_j)
    to_group(r.log_out, r.log_in, c.f_jlog)
    rows_ring.step()
    loaded(r.weight.at[z, j], local.out_weight)
    to_planes(r.weight.at[z, j], r.weight.at[:, j], c.weight_z)

    def factor(log):
        e = jnp.exp(log)
        return jnp.concatenate(
            [jnp.broadcast_to(e[0:1], (64, 128)), jnp.broadcast_to(e[4:5], (64, 128))], axis=0
        )

    def carry_group(states, run_ref, reverse):
        run, log = jnp.zeros((128, 128), F32), jnp.zeros((8, 128), F32)
        for i in reversed(range(8)) if reverse else range(8):
            r.before[i] = run
            r.log_before[i] = log
            run = factor(r.log_in[i]) * run + states[i].astype(F32)
            log = log + r.log_in[i]
        run_ref[...] = run.astype(run_ref.dtype)
        return log

    def carry_planes(planes, back, reverse):
        run = jnp.zeros((128, 128), F32)
        for i in reversed(range(8)) if reverse else range(8):
            passed = i > z if reverse else i < z
            run = jnp.where(passed, factor(r.log_z[i]) * run + planes[i].astype(F32), run)
        for i in range(8):
            back[i] = (r.before[i] + factor(r.log_before[i]) * run).astype(back.dtype)

    got(r.pack_in.at[pl.ds(0, 63)], c.dispatch)
    for n in range(8):
        r.pack_sorted[n * 8 : (n + 1) * 8] = r.pack_in[pl.ds(planes[n] * 8, 8)]
    packed_in = r.pack_sorted[...].reshape(512, 384)
    r.arr[tx, :, 0:384] = dot(r.sel_a[...], packed_in).astype(BF16)
    tail = dot(r.sel_b[0], packed_in[:, 0:128])
    tail = tail + dot(r.sel_b[1], packed_in[:, 128:256])
    tail = tail + dot(r.sel_b[2], packed_in[:, 256:384])
    r.arr[tx, :, 384:512] = tail.astype(BF16)
    arrived_ring.start()

    got(r.f_in.at[pl.ds(0, 7)], c.f_j)
    got(r.log_in.at[pl.ds(0, 7)], c.f_jlog)
    r.log_run[...] = carry_group(r.f_in, r.f_run, False)
    r.log_z[z] = r.log_run[...]
    r.f_z[z] = r.f_run[...]
    to_planes(r.f_run, r.f_z, c.f_z)
    to_planes(r.log_run, r.log_z, c.f_zlog)


    rows_ring.near()
    rows_ring.far()
    loaded(r.w_gate, local.w_gate)
    loaded(r.w_up, local.w_up)
    loaded(r.w_down, local.w_down)
    gate_pre, up_pre = jnp.zeros((384, 256), F32), jnp.zeros((384, 256), F32)
    for t in range(4):
        gate_pre = gate_pre + dot(r.full[t], r.w_gate[t * 512 : (t + 1) * 512, :])
    r.gate_pre[...] = gate_pre
    for t in range(4):
        up_pre = up_pre + dot(r.full[t], r.w_up[t * 512 : (t + 1) * 512, :])
    r.up_pre[...] = up_pre
    gate_pre = r.gate_pre[...]
    r.hidden[...] = (gate_pre * sigmoid(gate_pre) * up_pre).astype(BF16)

    def hidden_part(t):
        return dot(r.arr[t], r.w_down[:, pl.ds(pl.multiple_of(t * 512, 512), 512)], 1, 1)

    r.hidden_grad[...] = hidden_part(tx)
    arrived_ring.step()
    arrived_ring.near()
    r.hidden_grad[...] += hidden_part(left)
    r.hidden_grad[...] += hidden_part(right)

    got(r.weight.at[pl.ds(0, 7), 0], c.weight_z)
    weight_ring.first()
    share(weight_ring, c.weight_c, j)
    weight_ring.second()


    arrived_ring.far()
    hidden_grad = r.hidden_grad[...] + hidden_part(opp)
    gate_pre = r.gate_pre[...]
    gate_sig = sigmoid(gate_pre)
    slope = gate_sig * (1.0 + gate_pre * (1.0 - gate_sig))
    r.gate_grad[...] = (hidden_grad * r.up_pre[...] * slope).astype(BF16)
    r.up_grad[...] = (hidden_grad * (gate_pre * gate_sig)).astype(BF16)

    def row_part(t, start, end):
        rows = pl.ds(pl.multiple_of(t * 512, 512), 512)
        part = dot(r.gate_grad[start:end], r.w_gate[rows, :], 1, 1)
        return part + dot(r.up_grad[start:end], r.w_up[rows, :], 1, 1)

    def half_send(source, target, channel, n, start, end, side):
        part = pl.ds(start, end - start)
        send(source.at[part], target.at[part], channel, n, me, side)

    def scatter_parts(group):
        start, _, end = group
        r.rs_opp[start:end] = row_part(opp, start, end).astype(BF16)
        r.rs_own_r[start:end] = row_part(right, start, end)
        r.rs_own_l[start:end] = row_part(left, start, end)

    def scatter_start(group, channel):
        start, middle, end = group
        half_send(r.rs_opp, r.rs_half_l, channel, 0, start, middle, right)
        half_send(r.rs_opp, r.rs_half_r, channel, 1, middle, end, left)
        r.rs_right[middle:end] = r.rs_own_r[middle:end].astype(BF16)
        half_send(r.rs_right, r.rs_in_l, channel, 2, middle, end, right)
        r.rs_left[start:middle] = r.rs_own_l[start:middle].astype(BF16)
        half_send(r.rs_left, r.rs_in_r, channel, 3, start, middle, left)

    def scatter_step(group, channel):
        start, middle, end = group
        got(r.rs_half_l.at[pl.ds(start, middle - start)], channel, 0)
        total = r.rs_own_r[start:middle] + r.rs_half_l[start:middle].astype(F32)
        r.rs_right[start:middle] = total.astype(BF16)
        half_send(r.rs_right, r.rs_in_l, channel, 4, start, middle, right)
        got(r.rs_half_r.at[pl.ds(middle, end - middle)], channel, 1)
        total = r.rs_own_l[middle:end] + r.rs_half_r[middle:end].astype(F32)
        r.rs_left[middle:end] = total.astype(BF16)
        half_send(r.rs_left, r.rs_in_r, channel, 5, middle, end, left)

    def scatter_end(group, channel):
        start, middle, end = group
        top, bottom = pl.ds(start, middle - start), pl.ds(middle, end - middle)
        got(r.rs_in_l.at[bottom], channel, 2)
        got(r.rs_in_r.at[top], channel, 3)
        got(r.rs_in_l.at[top], channel, 4)
        got(r.rs_in_r.at[bottom], channel, 5)
        total = r.rs_own[start:end] + r.rs_in_l[start:end].astype(F32)
        return (total + r.rs_in_r[start:end].astype(F32)).astype(BF16)

    def scatter_sent(group, channel):
        start, middle, end = group
        top, bottom = pl.ds(start, middle - start), pl.ds(middle, end - middle)
        for n, part in enumerate((top, bottom, bottom, top, top, bottom)):
            sent(r.rs_half_l.at[part], channel, n)

    def pack_rows(summed, group, lanes, first, last):
        start, _, end = group
        skip = first * 8 - lanes.start
        for m in range(3):
            part = slice(m * 128, (m + 1) * 128)
            total = dot(r.sel_a[start:end, lanes], summed[:, part], 0, 0)
            total = total + dot(r.sel_b[m, start:end, lanes], summed[:, 384:512], 0, 0)
            total = total[skip : skip + (last - first) * 8].reshape(last - first, 8, 128)
            r.ret_out[first:last, :, part] = total.astype(BF16)

    scatter_parts(FAR)
    scatter_start(FAR, c.scatter)
    scatter_parts(NEAR)
    scatter_step(FAR, c.scatter)
    scatter_start(NEAR, c.scatter_near)
    weight_ring.step()
    r.rs_own[...] = row_part(tx, 0, 384)

    @pl.loop(0, 4)
    def _(t):
        rows = pl.ds(pl.multiple_of(t * 512, 512), 512)
        r.o_gate[rows, :] = dot(r.full[t], r.gate_grad[...], 0, 0).astype(BF16)
        r.o_up[rows, :] = dot(r.full[t], r.up_grad[...], 0, 0).astype(BF16)
        r.o_down[:, rows] = dot(r.hidden[...], r.arr[t], 0, 0).astype(BF16)

    store(r.o_gate, r.g_gate, result.gate)
    store(r.o_up, r.g_up, result.up)
    store(r.o_down, r.g_down, result.down)

    summed = scatter_end(FAR, c.scatter)
    pack_rows(summed, FAR, slice(0, 256), 0, 24)
    for n in range(3):
        to_plane_members(r.ret_out, r.ret_in, c.back, n, n * 8)
    scatter_step(NEAR, c.scatter_near)

    summed = scatter_end(NEAR, c.scatter_near)
    pack_rows(summed, NEAR, slice(128, 512), 24, 64)
    for n in range(3, 8):
        to_plane_members(r.ret_out, r.ret_in, c.back, n, n * 8)
    got(r.f_z.at[pl.ds(0, 7)], c.f_z)
    got(r.log_z.at[pl.ds(0, 7)], c.f_zlog)
    carry_planes(r.f_z, r.f_back, False)
    to_group(r.f_back, r.state, c.f_back)
    weight_ring.near()
    weight_ring.far()
    share(weight_ring, c.weight_c, weight_ring.left, weight_ring.right, weight_ring.opp)

    got(r.ret_in.at[pl.ds(0, 63)], c.back)
    packed_back = r.ret_in[...].reshape(512, 384)
    picked = dot(r.hit_a[0] + r.hit_a[1], packed_back)
    tail = dot(r.hit_b[0, 0] + r.hit_b[1, 0], packed_back[:, 0:128])
    tail = tail + dot(r.hit_b[0, 1] + r.hit_b[1, 1], packed_back[:, 128:256])
    tail = tail + dot(r.hit_b[0, 2] + r.hit_b[1, 2], packed_back[:, 256:384])
    picked = jnp.concatenate([picked, tail], axis=1)
    residual = r.cot[...].astype(F32) + picked
    r.resid[tx] = residual.astype(BF16)
    residual_ring.start()

    r.res_t[...] = dot(r.resid[tx], eye.astype(BF16), 0, 0).reshape(2, 8, 32, 128).astype(BF16)

    @pl.loop(1, 8)
    def _(d):
        peer = (j + d) % 8
        send(r.res_t.at[:, peer], r.res_in.at[tx, j], c.gow_j, 0, z * 8 + peer, tx)

    r.res_in[tx, j] = r.res_t[:, j]
    r.o_res[...] = residual
    store(r.o_res, r.g_res, result.res)

    got(r.state.at[pl.ds(0, 7)], c.f_back)
    for g in range(2):
        lanes = slice(g * 512, (g + 1) * 512)
        state = r.state[g * 4 : (g + 1) * 4].reshape(512, 128)
        r.carried[:, lanes] = dot(r.q[:, g * 128 : (g + 1) * 128], state, 1, 1) * r.from_start[:, lanes]
    y = r.y[...] + r.carried[...]
    r.y[...] = y
    loaded(r.gate, local.gate)
    gate = r.gate[...].astype(F32)
    r.mixed[j] = (y * (gate * sigmoid(gate))).astype(BF16)
    mixed_ring.start()
    share(mixed_ring, c.mixed_c, j)

    residual_ring.step()
    got(r.res_in.at[tx, pl.ds(0, 7)], c.gow_j)
    columns_ring.start()

    residual_ring.near()
    mixed_ring.step()
    residual_ring.far()
    got(r.weight.at[:, pl.ds(0, 4)], c.weight_c)

    for n in range(4):
        lanes = slice(n * 256, (n + 1) * 256)
        grad = jnp.zeros((128, 256), F32)
        for t in range(4):
            w = r.weight[2 * t : 2 * t + 2, :, :, lanes].reshape(512, 256)
            grad = grad + dot(r.resid[t], w)
        gate = r.gate[:, lanes].astype(F32)
        sig = sigmoid(gate)
        r.o_gate_in[:, lanes] = grad * r.y[:, lanes] * (sig * (1.0 + gate * (1.0 - sig)))
        dy = grad * (gate * sig)
        r.dy[:, lanes] = dy
        high, low = split(dy * r.from_start[:, lanes])
        r.dy_start[:, lanes] = high
        q = r.q[:, (n // 2) * 128 : (n // 2 + 1) * 128]
        reached = dot(high, q, 0, 0) + dot(low, q, 0, 0)
        r.b_own[2 * n : 2 * n + 2] = reached.reshape(2, 128, 128)
        for peer in (2 * n, 2 * n + 1):

            @pl.when(j != peer)
            def _():
                send(r.b_own.at[peer], r.b_in.at[j], c.b_j, 0, z * 8 + peer, tx)

        if n == 1:
            columns_ring.step()

    r.b_in[j] = r.b_own[j]
    store(r.o_gate_in, r.g_gate_in, result.gate_in)

    mixed_ring.near()
    mixed_ring.far()
    share(mixed_ring, c.mixed_c, mixed_ring.left, mixed_ring.right, mixed_ring.opp)

    columns_ring.near()
    columns_ring.far()
    got(r.mixed.at[pl.ds(0, 4)], c.mixed_c)

    @pl.loop(0, 4)
    def _(n):
        lanes = pl.ds(pl.multiple_of(n * 256, 256), 256)
        part = jnp.zeros((256, 256), F32)
        for i in range(8):
            part = part + dot(r.res_in[:, i].reshape(256, 128), r.mixed[i, :, lanes])
        part = part.reshape(8, 32, 256)
        r.gow_part[:, :, lanes] = part
        r.gow_out[:, :, lanes] = part.astype(BF16)

    def gow_send(*distances):
        for d in distances:
            plane = (z + d) % 8
            send(r.gow_out.at[plane], r.gow_in.at[z], c.gow_z, 0, plane * 8 + j, tx)

    gow_send(1, 7)

    got(r.b_in.at[pl.ds(0, 7)], c.b_j)
    carry_group(r.b_in, r.b_run, True)
    r.b_z[z] = r.b_run[...]
    to_planes(r.b_run, r.b_z, c.b_z)
    gow_send(2, 6, 3, 5, 4)

    r.row_col[...] = jnp.zeros((128, 128), F32)
    r.dqk[...] = jnp.zeros((2, 128, 128), F32)

    @pl.loop(0, 8)
    def _(p):
        off = pl.multiple_of(p * 128, 128)
        g = p // 4
        qk = r.qk[g]
        dy = r.dy[:, pl.ds(off, 128)]
        part = dot(dy.astype(BF16), masked_values(p), 1, 1) * r.decay[p]
        r.dqk[g] += part[:, 0:128] + part[:, 128:256]
        total = r.row_col[...]
        dv = jnp.zeros((128, 128), F32)
        for n in range(2):
            lanes = slice(n * 128, (n + 1) * 128)
            weighed = (part[:, lanes] * qk).astype(BF16)
            head = hot(col == 2 * p + n)
            total = total + dot(weighed, head) - dot(weighed, head, 0, 0)
            own = jnp.where(first, dy, 0.0) if n == 0 else jnp.where(first, 0.0, dy)
            dv = dv + dot(r.score[0, p, :, lanes], own.astype(BF16), 0, 0)
        r.row_col[...] = total
        r.dv[:, pl.ds(off, 128)] = dv

    by_head = hot(iota((1024, 128), 0) // 64 == iota((1024, 128), 1))
    r.row_col[...] += fine_dot(r.dy[...] * r.carried[...], by_head)
    for g in range(2):
        state = r.state[g * 4 : (g + 1) * 4].reshape(512, 128)
        r.dq[:, g * 128 : (g + 1) * 128] = dot(r.dy_start[:, g * 512 : (g + 1) * 512], state)

    for g in range(2):
        lanes = slice(g * 128, (g + 1) * 128)
        r.o_q[:, lanes] = r.dq[:, lanes] + dot(r.dqk[g].astype(BF16), r.k[:, lanes])
    store(r.o_q, r.g_q, result.q)


    got(r.b_z.at[pl.ds(0, 7)], c.b_z)
    carry_planes(r.b_z, r.b_back, True)
    to_group(r.b_back, r.dstate, c.b_back)

    got(r.dstate.at[pl.ds(0, 7)], c.b_back)
    for g in range(2):
        lanes, wide = slice(g * 128, (g + 1) * 128), slice(g * 512, (g + 1) * 512)
        dstate, low = split(r.dstate[g * 4 : (g + 1) * 4].reshape(512, 128))
        k = r.k[:, lanes]
        through = (dot(k, dstate, 1, 1) + dot(k, low, 1, 1)) * r.to_end[:, wide]
        r.carried[:, wide] = through
        r.o_v[:, wide] = r.dv[:, wide] + through
        r.o_k[:, lanes] = dot(r.dqk[g].astype(BF16), r.q[:, lanes], 0, 0) + dot(r.v_end[0, :, wide], dstate)
    store(r.o_v, r.g_v, result.v)
    store(r.o_k, r.g_k, result.k)
    added = fine_dot(r.v[...].astype(F32) * r.carried[...], by_head)
    high, low = split((r.dstate[...] * r.state[...].astype(F32)).reshape(1024, 128))
    both = dot(by_head, high, 0, 0) + dot(by_head, low, 0, 0)
    kept = dot(jnp.ones((128, 128), F32), both, 1, 1, precision=HIGHEST)
    kept = kept * jnp.exp(r.c_col[127:128, :])
    upper = hot(row <= col, F32)
    below = hot(row > col, F32)
    grad = dot(upper, r.row_col[...], precision=HIGHEST) + dot(below, added, precision=HIGHEST) + kept
    r.o_decay[...] = dot(eye[0:16], grad, 1, 1, precision=HIGHEST)
    store(r.o_decay, r.g_decay, result.decay)

    got(r.gow_in.at[pl.ds(0, 7)], c.gow_z)
    total = r.gow_part[z]
    for d in range(1, 8):
        total = total + r.gow_in[(z + d) % 8].astype(F32)
    r.o_out[...] = total
    store(r.o_out, r.g_out, result.out)

    for ring in (rows_ring, arrived_ring, residual_ring, columns_ring, weight_ring, mixed_ring):
        ring.sent()
    sent(r.pack_out.at[pl.ds(0, 63)], c.dispatch)
    sent(r.ret_out.at[pl.ds(0, 63)], c.back)
    scatter_sent(FAR, c.scatter)
    scatter_sent(NEAR, c.scatter_near)
    sent(r.weight.at[pl.ds(0, 7), 0], c.weight_z)
    sent(r.weight.at[:, pl.ds(0, 4)], c.weight_c)
    sent(r.mixed.at[pl.ds(0, 4)], c.mixed_c)
    sent(r.res_in.at[tx, pl.ds(0, 7)], c.gow_j)
    sent(r.gow_out.at[pl.ds(0, 7)], c.gow_z)
    for channel in (c.f_j, c.f_z, c.b_j, c.b_back):
        sent(r.f_in.at[pl.ds(0, 7)], channel)
    sent(r.state.at[pl.ds(0, 7)], c.f_back)
    sent(r.b_z.at[pl.ds(0, 7)], c.b_z)
    for channel in (c.f_jlog, c.f_zlog):
        sent(r.log_in.at[pl.ds(0, 7)], channel)
    for name in OUTPUTS:
        target = getattr(r, name)
        loaded(target, getattr(result, name[2:]))


def shards(
    out_cotangent,
    routes,
    route_weights,
    expert_rows,
    w_gate,
    w_up,
    w_down,
    out_weight,
    values,
    keys,
    queries,
    log_decay,
    gate_input,
):
    arrays = [jax.ShapeDtypeStruct(shape, dtype) for shape, dtype in OUTPUTS.values()]
    held = [pltpu.VMEM(shape, dtype) for shape, dtype in OUTPUTS.values()]
    scratch = [pltpu.VMEM(shape, dtype) for shape, dtype in BUFFERS.values()] + held
    for n in CHANNELS.values():
        scratch += [pltpu.SemaphoreType.DMA((n,))] * 2
    scratch += [pltpu.SemaphoreType.DMA((len(INPUTS),)), pltpu.SemaphoreType.DMA((len(OUTPUTS),))]
    outs = pl.pallas_call(
        kernel,
        out_shape=arrays,
        in_specs=[pl.BlockSpec(memory_space=pl.ANY)] * len(INPUTS),
        out_specs=[pl.BlockSpec(memory_space=pl.ANY)] * len(OUTPUTS),
        scratch_shapes=scratch,
        compiler_params=pltpu.CompilerParams(
            has_side_effects=True, collective_id=0, vmem_limit_bytes=66_000_000
        ),
        name="layer_backward",
    )(
        out_cotangent,
        routes.T,
        route_weights.T,
        expert_rows[0],
        w_gate[0],
        w_up[0],
        w_down[0],
        out_weight,
        values,
        keys,
        queries,
        log_decay.T,
        gate_input,
    )
    outs = pl.pallas_call(
        publish,
        out_shape=arrays,
        in_specs=[pl.BlockSpec(memory_space=pl.ANY)] * len(OUTPUTS),
        out_specs=[pl.BlockSpec(memory_space=pl.ANY)] * len(OUTPUTS),
        scratch_shapes=held + [pltpu.SemaphoreType.DMA((2, len(OUTPUTS)))],
        compiler_params=pltpu.CompilerParams(vmem_limit_bytes=66_000_000),
        name="publish",
    )(*outs)
    outs = list(outs)
    outs[8] = outs[8].T
    return (outs[0][None], outs[1][None], outs[2][None]) + tuple(outs[3:])


def solution(mesh):
    sp, both = P("sp", None), P("sp", "tp")
    columns, hidden = P("sp", None, "tp"), P("sp", "tp", None)
    in_specs = (sp, sp, sp, columns, columns, columns, hidden) + (both,) * 6
    out_specs = (columns, columns, hidden) + (both,) * 7
    return jax.shard_map(
        shards, mesh=mesh, in_specs=in_specs, out_specs=out_specs, check_vma=False
    )
```

```python
import jax
import jax.numpy as jnp
from jax import lax
from jax.experimental import pallas as pl
from jax.experimental.pallas import tpu as pltpu
from jax.sharding import PartitionSpec as P

MESH = pl.DeviceIdType.MESH
F32, BF16 = jnp.float32, jnp.bfloat16
HIGHEST = lax.Precision.HIGHEST

BUFFERS = dict(
    cot=((128, 512), BF16),
    routes=((2, 128), jnp.int32),
    route_weights=((2, 128), F32),
    w_gate=((2048, 256), BF16),
    w_up=((2048, 256), BF16),
    w_down=((256, 2048), BF16),
    v=((128, 1024), BF16),
    k=((128, 256), BF16),
    q=((128, 256), BF16),
    log_decay=((16, 128), F32),
    gate=((128, 1024), BF16),
    pack_out=((64, 8, 384), BF16),
    pack_in=((64, 8, 384), BF16),
    pack_sorted=((64, 8, 384), BF16),
    ret_out=((64, 8, 384), BF16),
    ret_in=((64, 8, 384), BF16),
    hit_a=((2, 128, 512), BF16),
    hit_b=((2, 3, 128, 512), BF16),
    sel_a=((384, 512), BF16),
    sel_b=((3, 384, 512), BF16),
    arr=((4, 384, 512), BF16),
    full=((4, 384, 512), BF16),
    gate_pre=((384, 256), F32),
    up_pre=((384, 256), F32),
    hidden_grad=((384, 256), F32),
    hidden=((384, 256), BF16),
    gate_grad=((384, 256), BF16),
    up_grad=((384, 256), BF16),
    rs_opp=((384, 512), BF16),
    rs_right=((384, 512), BF16),
    rs_left=((384, 512), BF16),
    rs_half_l=((384, 512), BF16),
    rs_half_r=((384, 512), BF16),
    rs_in_l=((384, 512), BF16),
    rs_in_r=((384, 512), BF16),
    rs_own=((384, 512), F32),
    rs_own_l=((384, 512), F32),
    rs_own_r=((384, 512), F32),
    resid=((4, 128, 512), BF16),
    res_t=((2, 8, 32, 128), BF16),
    res_in=((4, 8, 2, 32, 128), BF16),
    weight=((8, 8, 32, 1024), BF16),
    mixed=((8, 128, 1024), BF16),
    gow_part=((8, 32, 1024), F32),
    gow_out=((8, 32, 1024), BF16),
    gow_in=((8, 32, 1024), BF16),
    c_exp=((128, 1024), F32),
    to_end=((128, 1024), F32),
    from_start=((128, 1024), F32),
    c_row=((16, 128), F32),
    c_col=((128, 128), F32),
    v_end=((2, 128, 1024), BF16),
    qk=((2, 128, 128), F32),
    decay=((8, 128, 256), F32),
    score=((2, 8, 128, 256), BF16),
    y=((128, 1024), F32),
    carried=((128, 1024), F32),
    dy=((128, 1024), F32),
    mixed_grad=((128, 1024), F32),
    dy_start=((128, 1024), BF16),
    dv=((128, 1024), F32),
    dqk=((2, 128, 128), F32),
    row_col=((128, 128), F32),
    dq=((128, 256), F32),
    log_out=((8, 8, 128), F32),
    log_in=((8, 8, 128), F32),
    log_run=((8, 128), F32),
    log_z=((8, 8, 128), F32),
    log_before=((8, 8, 128), F32),
    before=((8, 128, 128), F32),
    f_own=((8, 128, 128), F32),
    f_in=((8, 128, 128), F32),
    f_run=((128, 128), F32),
    f_z=((8, 128, 128), F32),
    f_back=((8, 128, 128), BF16),
    state=((8, 128, 128), BF16),
    b_own=((8, 128, 128), F32),
    b_in=((8, 128, 128), F32),
    b_run=((8, 16, 128), F32),
    b_z=((8, 16, 128), F32),
    b_scan=((8, 16, 128), F32),
    b_pre=((8, 16, 128), F32),
    b_back=((8, 128, 128), F32),
    dstate=((8, 128, 128), F32),
)
CHANNELS = dict(
    rows=6,
    arrived=6,
    arrived_near=6,
    residual=3,
    dispatch=1,
    dispatch_near=1,
    back=1,
    scatter=6,
    scatter_near=6,
    weight_z=1,
    weight_y=6,
    weight_c=1,
    mixed_y=6,
    mixed_c=1,
    gow_j=1,
    columns=3,
    gow_z=1,
    f_j=1,
    f_jlog=1,
    f_z=1,
    f_zlog=1,
    f_back=1,
    b_j=1,
    b_z=1,
    b_pre=1,
    b_back=1,
)
INPUTS = dict(
    h_cot=((128, 2048), BF16),
    h_routes=((2, 128), jnp.int32),
    h_route_weights=((2, 128), F32),
    h_rows=((384, 512), BF16),
    h_w_gate=((2048, 256), BF16),
    h_w_up=((2048, 256), BF16),
    h_w_down=((256, 2048), BF16),
    h_out_weight=((32, 1024), BF16),
    h_v=((128, 1024), BF16),
    h_k=((128, 256), BF16),
    h_q=((128, 256), BF16),
    h_log_decay=((16, 128), F32),
    h_gate=((128, 1024), BF16),
)
OUTPUTS = dict(
    g_gate=((2048, 256), BF16),
    g_up=((2048, 256), BF16),
    g_down=((256, 2048), BF16),
    g_out=((32, 1024), F32),
    g_res=((128, 512), F32),
    g_v=((128, 1024), F32),
    g_k=((128, 256), F32),
    g_q=((128, 256), F32),
    g_decay=((16, 128), F32),
    g_gate_in=((128, 1024), F32),
)


PLANES = (4, 3, 5, 2, 6, 1, 7, 0)
FAR, NEAR = (0, 80, 144), (144, 256, 384)


class Refs:
    pass


def dot(a, b, ca=1, cb=0, precision=None):
    return lax.dot_general(
        a, b, (((ca,), (cb,)), ((), ())), precision=precision, preferred_element_type=F32
    )


def iota(shape, dim):
    return lax.broadcasted_iota(jnp.int32, shape, dim)


def hot(cond, dtype=BF16):
    return jnp.where(cond, 1.0, 0.0).astype(dtype)


def split(x):
    high = x.astype(BF16)
    return high, (x - high.astype(F32)).astype(BF16)


def fine_dot(a, b, ca=1, cb=0):
    high, low = split(a)
    return dot(high, b, ca, cb) + dot(low, b, ca, cb)


def sigmoid(x):
    return 1.0 / (1.0 + jnp.exp(-x))


def publish(*refs):
    n = len(OUTPUTS)
    sources, targets, sems = refs[:n], refs[n : 2 * n], refs[2 * n]
    stores = [pltpu.make_async_copy(sources[i], targets[i], sems.at[i]) for i in range(n)]
    for store in stores:
        store.start()
    for store in stores:
        store.wait()


def kernel(*refs):
    r, c, local = Refs(), Refs(), Refs()
    names = list(INPUTS) + list(OUTPUTS) + list(BUFFERS)
    for name, ref in zip(names, refs):
        setattr(r, name, ref)
    at = len(names)
    for name in CHANNELS:
        setattr(c, name, (refs[at], refs[at + 1]))
        at += 2
    in_sems = refs[at]
    for i, name in enumerate(INPUTS):
        setattr(local, name[2:], in_sems.at[i])

    me, tx = lax.axis_index("sp"), lax.axis_index("tp")
    z, j = me // 8, me % 8
    partner = j + 1 - 2 * (j % 2)
    right, left, opp = (tx + 1) % 4, (tx + 3) % 4, (tx + 2) % 4
    column = pl.multiple_of(tx * 512, 512)
    planes = [(z + d) % 8 for d in PLANES]

    barrier = pltpu.get_barrier_semaphore()

    @pl.loop(1, 64)
    def _(d):
        peer = (me + d) % 64
        pl.semaphore_signal(barrier, inc=1, device_id=(peer, tx), device_id_type=MESH)

    for side in (right, left, opp):
        pl.semaphore_signal(barrier, inc=1, device_id=(me, side), device_id_type=MESH)

    loads = dict(
        routes=(r.h_routes, r.routes),
        route_weights=(r.h_route_weights, r.route_weights),
        cot=(r.h_cot.at[:, pl.ds(column, 512)], r.cot),
        log_decay=(r.h_log_decay, r.log_decay),
        k=(r.h_k, r.k),
        v=(r.h_v, r.v),
        out_weight=(r.h_out_weight, r.weight.at[z, j]),
        q=(r.h_q, r.q),
        w_gate=(r.h_w_gate, r.w_gate),
        w_up=(r.h_w_up, r.w_up),
        w_down=(r.h_w_down, r.w_down),
        gate=(r.h_gate, r.gate),
    )
    for name, (source, target) in loads.items():
        pltpu.make_async_copy(source, target, getattr(local, name)).start()

    for n in range(8):
        source = r.h_rows.at[pl.ds(pl.multiple_of(planes[n] * 48, 16), 48)]
        pltpu.make_async_copy(source, r.full.at[tx, pl.ds(n * 48, 48)], local.rows).start()

    def loaded(target, sem):
        pltpu.make_async_copy(target, target, sem).wait()

    def send(src, dst, channel, n, sp, tp):
        out_sem, in_sem = channel
        pltpu.make_async_remote_copy(
            src_ref=src,
            dst_ref=dst,
            send_sem=out_sem.at[n],
            recv_sem=in_sem.at[n],
            device_id=(sp, tp),
            device_id_type=MESH,
        ).start()

    def got(ref, channel, n=0):
        pltpu.make_async_copy(ref, ref, channel[1].at[n]).wait()

    def sent(ref, channel, n=0):
        pltpu.make_async_copy(ref, ref, channel[0].at[n]).wait()

    class Ring:
        def __init__(self, piece, channel, members, targets):
            self.piece, self.channel = piece, channel
            self.mine, self.right, self.left, self.opp = members
            self.to_right, self.to_left = targets

        def go(self, n, h, sem, target):
            part = self.piece(n, h)
            send(part, part, self.channel, sem, *target)

        def start(self):
            self.first()
            self.second()

        def first(self):
            self.go(self.mine, 0, 0, self.to_right)
            self.go(self.mine, 1, 2, self.to_left)

        def second(self):
            self.go(self.mine, 1, 1, self.to_right)
            self.go(self.mine, 0, 3, self.to_left)

        def step(self):
            got(self.piece(self.left, 0), self.channel, 0)
            self.go(self.left, 0, 4, self.to_right)
            got(self.piece(self.right, 1), self.channel, 2)
            self.go(self.right, 1, 5, self.to_left)

        def near(self):
            got(self.piece(self.left, 1), self.channel, 1)
            got(self.piece(self.right, 0), self.channel, 3)

        def far(self):
            got(self.piece(self.opp, 0), self.channel, 4)
            got(self.piece(self.opp, 1), self.channel, 5)

        def sent(self):
            for sem, n, h in ((0, self.mine, 0), (1, self.mine, 1), (2, self.mine, 1), (3, self.mine, 0)):
                sent(self.piece(n, h), self.channel, sem)
            sent(self.piece(self.left, 0), self.channel, 4)
            sent(self.piece(self.right, 1), self.channel, 5)

    def tp_ring(buf, channel, group=None):
        start, middle, end = group or (0, buf.shape[1] // 2, buf.shape[1])
        parts = (pl.ds(start, middle - start), pl.ds(middle, end - middle))
        piece = lambda n, h: buf.at[n, parts[h]]
        return Ring(piece, channel, (tx, right, left, opp), ((me, right), (me, left)))

    class Direct:
        def __init__(self, buf, channel):
            self.buf, self.channel = buf, channel

        def start(self):
            for n, side in enumerate((right, left, opp)):
                send(self.buf.at[tx], self.buf.at[tx], self.channel, n, me, side)

        def near(self):
            got(self.buf.at[left], self.channel, 0)
            got(self.buf.at[right], self.channel, 1)

        def far(self):
            got(self.buf.at[opp], self.channel, 2)

        def sent(self):
            for n in range(3):
                sent(self.buf.at[tx], self.channel, n)

    def y_ring(piece, channel):
        members = (j, (j + 2) % 8, (j + 6) % 8, (j + 4) % 8)
        return Ring(piece, channel, members, ((z * 8 + members[1], tx), (z * 8 + members[2], tx)))

    rows_ring = tp_ring(r.full, c.rows)
    far_ring = tp_ring(r.arr, c.arrived, FAR)
    near_ring = tp_ring(r.arr, c.arrived_near, NEAR)
    residual_ring = Direct(r.resid, c.residual)
    columns_ring = Direct(r.res_in, c.columns)

    weight_ring = y_ring(lambda n, h: r.weight.at[pl.ds(4 * h, 4), n], c.weight_y)
    mixed_ring = y_ring(lambda n, h: r.mixed.at[n, pl.ds(64 * h, 64)], c.mixed_y)

    def share(ring, channel, *members):
        for n in members:
            for h in range(2):
                part = ring.piece(n, h)
                send(part, part, channel, 0, z * 8 + partner, tx)

    def to_plane_members(out, into, channel, n, first):
        own = PLANES[n] == 0

        @pl.loop(1 if own else 0, 8)
        def _(d):
            peer = (j + d) % 8
            send(out.at[first + peer], into.at[me], channel, 0, planes[n] * 8 + peer, tx)

        if own:
            into[me] = out[first + j]

    def to_group(out, into, channel):
        @pl.loop(1, 8)
        def _(d):
            peer = (j + d) % 8
            send(out.at[peer], into.at[j], channel, 0, z * 8 + peer, tx)

        into[j] = out[j]

    def across_planes(out, into, channel):
        @pl.loop(1, 8)
        def _(d):
            plane = (z + d) % 8
            send(out.at[plane], into.at[z], channel, 0, plane * 8 + j, tx)

        into[z] = out[z]

    def to_planes(src, into, channel):
        @pl.loop(1, 8)
        def _(d):
            send(src, into.at[z], channel, 0, ((z + d) % 8) * 8 + j, tx)

    eye = hot(iota((128, 128), 0) == iota((128, 128), 1), F32)
    loaded(r.routes, local.routes)
    loaded(r.route_weights, local.route_weights)
    routes = dot(eye, r.routes[...].astype(F32), 1, 1, precision=HIGHEST)
    route_weights = dot(eye, r.route_weights[...], 1, 1, precision=HIGHEST)
    expert = iota((128, 64), 1).astype(F32)
    route = [routes[:, 0:1], routes[:, 1:2]]
    named = [hot(route[n] == expert, F32) for n in range(2)]
    strict = iota((128, 128), 0) > iota((128, 128), 1)
    earlier = dot(hot(strict), (named[0] + named[1]).astype(BF16))
    slot = iota((128, 512), 1).astype(F32)
    loaded(r.cot, local.cot)
    cot = r.cot[...].astype(F32)
    scaled = []
    for n in range(2):
        rank = jnp.sum(named[n] * earlier, axis=1, keepdims=True)
        upper = jnp.where(rank >= 3.0, 1.0, 0.0)
        base = route[n] * 8.0
        r.hit_a[n] = hot(slot == base + rank)
        for m in range(3):
            place = jnp.where(rank - 3.0 * upper == float(m), base + 6.0 + upper, -1.0)
            r.hit_b[n, m] = hot(slot == place)
        scaled.append((route_weights[:, n : n + 1] * cot).astype(BF16))
    for m in range(3):
        lanes = slice(m * 128, (m + 1) * 128)
        total = dot(r.hit_a[0], scaled[0][:, lanes], 0, 0)
        total = total + dot(r.hit_a[1], scaled[1][:, lanes], 0, 0)
        total = total + dot(r.hit_b[0, m], scaled[0][:, 384:512], 0, 0)
        total = total + dot(r.hit_b[1, m], scaled[1][:, 384:512], 0, 0)
        r.pack_out[:, :, lanes] = total.reshape(64, 8, 128).astype(BF16)
    row, col = iota((128, 128), 0), iota((128, 128), 1)
    tri = hot(row >= col, F32)
    head_of = iota((16, 1024), 1) // 64 == iota((16, 1024), 0)
    loaded(r.log_decay, local.log_decay)
    loaded(r.v, local.v)
    loaded(r.k, local.k)
    log_decay = r.log_decay[...]
    cumulative = dot(tri, log_decay, 1, 1, precision=HIGHEST)
    r.c_col[...] = dot(cumulative, hot(iota((16, 128), 0) == iota((16, 128), 1), F32), precision=HIGHEST)
    r.c_row[...] = dot(log_decay, tri, 1, 1, precision=HIGHEST)
    r.c_exp[...] = dot(cumulative, hot(head_of, F32), precision=HIGHEST)
    c_exp = r.c_exp[...]
    r.from_start[...] = jnp.exp(c_exp)
    r.to_end[...] = jnp.exp(r.c_exp[127:128, :] - c_exp)
    r.v_end[0], r.v_end[1] = split(r.v[...].astype(F32) * r.to_end[...])
    for g in range(2):
        wide, k = slice(g * 512, (g + 1) * 512), r.k[:, g * 128 : (g + 1) * 128]
        own = dot(r.v_end[0, :, wide], k, 0, 0) + dot(r.v_end[1, :, wide], k, 0, 0)
        r.f_own[g * 4 : (g + 1) * 4] = own.reshape(4, 128, 128)
    total = dot(log_decay, jnp.ones((128, 128), F32), precision=HIGHEST)
    spread = hot(iota((64, 16), 0) // 4 == iota((64, 16), 1), F32)
    r.log_out[...] = dot(spread, total, precision=HIGHEST).reshape(8, 8, 128)
    place, packed = iota((384, 512), 0), iota((384, 512), 1)
    source, rank = place // 6, place % 6
    r.sel_a[...] = hot(packed == source * 8 + rank)
    for m in range(3):
        r.sel_b[m] = hot((packed == source * 8 + 6 + rank // 3) & (rank % 3 == m))

    lower = row >= col
    first = col < 64
    loaded(r.q, local.q)
    for g in range(2):
        r.qk[g] = dot(r.q[:, g * 128 : (g + 1) * 128], r.k[:, g * 128 : (g + 1) * 128], 1, 1)

    def masked_values(p):
        vp = r.v[:, pl.ds(pl.multiple_of(p * 128, 128), 128)].astype(F32)
        return jnp.concatenate(
            [jnp.where(first, vp, 0.0).astype(BF16), jnp.where(first, 0.0, vp).astype(BF16)], axis=0
        )

    @pl.loop(0, 8)
    def _(p):
        off = pl.multiple_of(p * 128, 128)
        qk = r.qk[p // 4]
        c_pair = r.c_exp[:, pl.ds(off, 128)]
        for n in range(2):
            down = jnp.minimum(c_pair[:, 64 * n : 64 * n + 1] - r.c_row[pl.ds(2 * p + n, 1), :], 0.0)
            decay = jnp.where(lower, jnp.exp(down), 0.0)
            r.decay[p, :, n * 128 : (n + 1) * 128] = decay
            lanes = slice(n * 128, (n + 1) * 128)
            r.score[0, p, :, lanes], r.score[1, p, :, lanes] = split(qk * decay)
        values = masked_values(p)
        r.y[:, pl.ds(off, 128)] = dot(r.score[0, p], values) + dot(r.score[1, p], values)

    pl.semaphore_wait(barrier, 66)
    for n in range(8):
        channel = c.dispatch if n < 3 else c.dispatch_near
        to_plane_members(r.pack_out, r.pack_in, channel, n, planes[n] * 8)
    loaded(r.full.at[tx], local.rows)
    rows_ring.start()
    to_group(r.f_own, r.f_in, c.f_j)
    to_group(r.log_out, r.log_in, c.f_jlog)
    rows_ring.step()
    loaded(r.weight.at[z, j], local.out_weight)
    to_planes(r.weight.at[z, j], r.weight.at[:, j], c.weight_z)

    def factor(log):
        e = jnp.exp(log)
        return jnp.concatenate(
            [jnp.broadcast_to(e[0:1], (64, 128)), jnp.broadcast_to(e[4:5], (64, 128))], axis=0
        )

    def carry_group(states, run_ref, reverse):
        run, log = jnp.zeros((128, 128), F32), jnp.zeros((8, 128), F32)
        for i in reversed(range(8)) if reverse else range(8):
            r.before[i] = run
            r.log_before[i] = log
            run = factor(r.log_in[i]) * run + states[i].astype(F32)
            log = log + r.log_in[i]
        run_ref[...] = run.reshape(run_ref.shape)
        return log

    def scan_planes(planes_in, scan):
        run = jnp.zeros((16, 128), F32)
        for i in reversed(range(8)):
            scan[i] = run
            run = jnp.exp(r.log_z[i, pl.ds(4 * (z // 4), 1), :]) * run + planes_in[i]

    def carry_planes(planes, back):
        run = jnp.zeros((128, 128), F32)
        for i in range(8):
            run = jnp.where(i < z, factor(r.log_z[i]) * run + planes[i], run)
        back_to_group(run, back)

    def back_to_group(run, back):
        for i in range(8):
            back[i] = (r.before[i] + factor(r.log_before[i]) * run).astype(back.dtype)

    def unpack(group, lanes, first, last):
        start, _, end = group
        for n in range(first // 8, last // 8):
            r.pack_sorted[n * 8 : (n + 1) * 8] = r.pack_in[pl.ds(planes[n] * 8, 8)]
        packed = r.pack_sorted[lanes.start // 8 : lanes.stop // 8].reshape(lanes.stop - lanes.start, 384)
        r.arr[tx, start:end, 0:384] = dot(r.sel_a[start:end, lanes], packed).astype(BF16)
        tail = dot(r.sel_b[0, start:end, lanes], packed[:, 0:128])
        tail = tail + dot(r.sel_b[1, start:end, lanes], packed[:, 128:256])
        tail = tail + dot(r.sel_b[2, start:end, lanes], packed[:, 256:384])
        r.arr[tx, start:end, 384:512] = tail.astype(BF16)

    r.pack_sorted[24:32] = jnp.zeros((8, 8, 384), BF16)
    got(r.pack_in.at[pl.ds(0, 24)], c.dispatch)
    unpack(FAR, slice(0, 256), 0, 24)
    far_ring.start()
    got(r.pack_in.at[pl.ds(0, 39)], c.dispatch_near)
    unpack(NEAR, slice(128, 512), 24, 64)
    far_ring.step()
    near_ring.start()

    got(r.f_in.at[pl.ds(0, 7)], c.f_j)
    got(r.log_in.at[pl.ds(0, 7)], c.f_jlog)
    r.log_run[...] = carry_group(r.f_in, r.f_run, False)
    r.log_z[z] = r.log_run[...]
    r.f_z[z] = r.f_run[...]
    to_planes(r.f_run, r.f_z, c.f_z)
    to_planes(r.log_run, r.log_z, c.f_zlog)


    rows_ring.near()
    rows_ring.far()
    loaded(r.w_gate, local.w_gate)
    loaded(r.w_up, local.w_up)
    loaded(r.w_down, local.w_down)
    gate_pre, up_pre = jnp.zeros((384, 256), F32), jnp.zeros((384, 256), F32)
    for t in range(4):
        gate_pre = gate_pre + dot(r.full[t], r.w_gate[t * 512 : (t + 1) * 512, :])
    r.gate_pre[...] = gate_pre
    for t in range(4):
        up_pre = up_pre + dot(r.full[t], r.w_up[t * 512 : (t + 1) * 512, :])
    r.up_pre[...] = up_pre
    gate_pre = r.gate_pre[...]
    r.hidden[...] = (gate_pre * sigmoid(gate_pre) * up_pre).astype(BF16)

    def hidden_part(t, group):
        lanes = pl.ds(pl.multiple_of(t * 512, 512), 512)
        return dot(r.arr[t, group[0] : group[2]], r.w_down[:, lanes], 1, 1)

    def hidden_grads(group):
        start, _, end = group
        hidden_grad = r.hidden_grad[start:end] + hidden_part(opp, group)
        gate_pre = r.gate_pre[start:end]
        gate_sig = sigmoid(gate_pre)
        slope = gate_sig * (1.0 + gate_pre * (1.0 - gate_sig))
        r.gate_grad[start:end] = (hidden_grad * r.up_pre[start:end] * slope).astype(BF16)
        r.up_grad[start:end] = (hidden_grad * (gate_pre * gate_sig)).astype(BF16)

    def row_part(t, start, end):
        rows = pl.ds(pl.multiple_of(t * 512, 512), 512)
        part = dot(r.gate_grad[start:end], r.w_gate[rows, :], 1, 1)
        return part + dot(r.up_grad[start:end], r.w_up[rows, :], 1, 1)

    def half_send(source, target, channel, n, start, end, side):
        part = pl.ds(start, end - start)
        send(source.at[part], target.at[part], channel, n, me, side)

    def scatter_parts(group):
        start, _, end = group
        r.rs_opp[start:end] = row_part(opp, start, end).astype(BF16)
        r.rs_own_r[start:end] = row_part(right, start, end)
        r.rs_own_l[start:end] = row_part(left, start, end)

    def scatter_start(group, channel):
        start, middle, end = group
        half_send(r.rs_opp, r.rs_half_l, channel, 0, start, middle, right)
        half_send(r.rs_opp, r.rs_half_r, channel, 1, middle, end, left)
        r.rs_right[middle:end] = r.rs_own_r[middle:end].astype(BF16)
        half_send(r.rs_right, r.rs_in_l, channel, 2, middle, end, right)
        r.rs_left[start:middle] = r.rs_own_l[start:middle].astype(BF16)
        half_send(r.rs_left, r.rs_in_r, channel, 3, start, middle, left)

    def scatter_step(group, channel):
        start, middle, end = group
        got(r.rs_half_l.at[pl.ds(start, middle - start)], channel, 0)
        total = r.rs_own_r[start:middle] + r.rs_half_l[start:middle].astype(F32)
        r.rs_right[start:middle] = total.astype(BF16)
        half_send(r.rs_right, r.rs_in_l, channel, 4, start, middle, right)
        got(r.rs_half_r.at[pl.ds(middle, end - middle)], channel, 1)
        total = r.rs_own_l[middle:end] + r.rs_half_r[middle:end].astype(F32)
        r.rs_left[middle:end] = total.astype(BF16)
        half_send(r.rs_left, r.rs_in_r, channel, 5, middle, end, left)

    def scatter_end(group, channel):
        start, middle, end = group
        top, bottom = pl.ds(start, middle - start), pl.ds(middle, end - middle)
        got(r.rs_in_l.at[bottom], channel, 2)
        got(r.rs_in_r.at[top], channel, 3)
        got(r.rs_in_l.at[top], channel, 4)
        got(r.rs_in_r.at[bottom], channel, 5)
        total = r.rs_own[start:end] + r.rs_in_l[start:end].astype(F32)
        return (total + r.rs_in_r[start:end].astype(F32)).astype(BF16)

    def scatter_sent(group, channel):
        start, middle, end = group
        top, bottom = pl.ds(start, middle - start), pl.ds(middle, end - middle)
        for n, part in enumerate((top, bottom, bottom, top, top, bottom)):
            sent(r.rs_half_l.at[part], channel, n)

    def pack_rows(summed, group, lanes, first, last):
        start, _, end = group
        skip = first * 8 - lanes.start
        for m in range(3):
            part = slice(m * 128, (m + 1) * 128)
            total = dot(r.sel_a[start:end, lanes], summed[:, part], 0, 0)
            total = total + dot(r.sel_b[m, start:end, lanes], summed[:, 384:512], 0, 0)
            total = total[skip : skip + (last - first) * 8].reshape(last - first, 8, 128)
            r.ret_out[first:last, :, part] = total.astype(BF16)

    r.hidden_grad[0:144] = hidden_part(tx, FAR)
    far_ring.near()
    r.hidden_grad[0:144] += hidden_part(left, FAR)
    r.hidden_grad[0:144] += hidden_part(right, FAR)
    far_ring.far()
    hidden_grads(FAR)
    scatter_parts(FAR)
    scatter_start(FAR, c.scatter)
    near_ring.step()
    r.hidden_grad[144:384] = hidden_part(tx, NEAR)
    scatter_step(FAR, c.scatter)

    got(r.weight.at[pl.ds(0, 7), 0], c.weight_z)
    weight_ring.first()
    share(weight_ring, c.weight_c, j)
    weight_ring.second()

    near_ring.near()
    r.hidden_grad[144:384] += hidden_part(left, NEAR)
    r.hidden_grad[144:384] += hidden_part(right, NEAR)
    near_ring.far()
    hidden_grads(NEAR)
    scatter_parts(NEAR)
    scatter_start(NEAR, c.scatter_near)
    r.rs_own[...] = row_part(tx, 0, 384)
    summed = scatter_end(FAR, c.scatter)
    pack_rows(summed, FAR, slice(0, 256), 0, 24)
    for n in range(3):
        to_plane_members(r.ret_out, r.ret_in, c.back, n, n * 8)

    got(r.f_z.at[pl.ds(0, 7)], c.f_z)
    got(r.log_z.at[pl.ds(0, 7)], c.f_zlog)
    carry_planes(r.f_z, r.f_back)
    to_group(r.f_back, r.state, c.f_back)
    scatter_step(NEAR, c.scatter_near)

    @pl.loop(0, 4)
    def _(t):
        rows = pl.ds(pl.multiple_of(t * 512, 512), 512)
        r.g_gate[rows, :] = dot(r.full[t], r.gate_grad[...], 0, 0).astype(BF16)
        r.g_up[rows, :] = dot(r.full[t], r.up_grad[...], 0, 0).astype(BF16)
        r.g_down[:, rows] = dot(r.hidden[...], r.arr[t], 0, 0).astype(BF16)


    summed = scatter_end(NEAR, c.scatter_near)
    pack_rows(summed, NEAR, slice(128, 512), 24, 64)
    for n in range(3, 8):
        to_plane_members(r.ret_out, r.ret_in, c.back, n, n * 8)
    weight_ring.step()
    weight_ring.near()
    share(weight_ring, c.weight_c, weight_ring.left, weight_ring.right)

    got(r.state.at[pl.ds(0, 7)], c.f_back)
    for g in range(2):
        lanes = slice(g * 512, (g + 1) * 512)
        state = r.state[g * 4 : (g + 1) * 4].reshape(512, 128)
        r.carried[:, lanes] = dot(r.q[:, g * 128 : (g + 1) * 128], state, 1, 1) * r.from_start[:, lanes]
    y = r.y[...] + r.carried[...]
    r.y[...] = y
    loaded(r.gate, local.gate)
    gate = r.gate[...].astype(F32)
    r.mixed[j] = (y * (gate * sigmoid(gate))).astype(BF16)
    got(r.ret_in.at[pl.ds(0, 63)], c.back)
    packed_back = r.ret_in[...].reshape(512, 384)
    picked = dot(r.hit_a[0] + r.hit_a[1], packed_back)
    tail = dot(r.hit_b[0, 0] + r.hit_b[1, 0], packed_back[:, 0:128])
    tail = tail + dot(r.hit_b[0, 1] + r.hit_b[1, 1], packed_back[:, 128:256])
    tail = tail + dot(r.hit_b[0, 2] + r.hit_b[1, 2], packed_back[:, 256:384])
    picked = jnp.concatenate([picked, tail], axis=1)
    residual = r.cot[...].astype(F32) + picked
    r.resid[tx] = residual.astype(BF16)
    residual_ring.start()

    r.res_t[...] = dot(r.resid[tx], eye.astype(BF16), 0, 0).reshape(2, 8, 32, 128).astype(BF16)

    @pl.loop(1, 8)
    def _(d):
        peer = (j + d) % 8
        send(r.res_t.at[:, peer], r.res_in.at[tx, j], c.gow_j, 0, z * 8 + peer, tx)

    r.res_in[tx, j] = r.res_t[:, j]
    r.g_res[...] = residual

    mixed_ring.start()
    share(mixed_ring, c.mixed_c, j)

    weight_ring.far()
    share(weight_ring, c.weight_c, weight_ring.opp)

    got(r.weight.at[:, pl.ds(0, 4)], c.weight_c)

    def mixed_grad_part(t, lanes):
        w = r.weight[pl.ds(2 * t, 2), :, :, lanes].reshape(512, 256)
        return dot(r.resid[t], w)

    residual_ring.near()
    for n in range(4):
        lanes = slice(n * 256, (n + 1) * 256)
        grad = mixed_grad_part(tx, lanes) + mixed_grad_part(left, lanes)
        r.mixed_grad[:, lanes] = grad + mixed_grad_part(right, lanes)
    got(r.res_in.at[tx, pl.ds(0, 7)], c.gow_j)
    columns_ring.start()
    residual_ring.far()

    for n in range(4):
        lanes = slice(n * 256, (n + 1) * 256)
        grad = r.mixed_grad[:, lanes] + mixed_grad_part(opp, lanes)
        gate = r.gate[:, lanes].astype(F32)
        sig = sigmoid(gate)
        r.g_gate_in[:, lanes] = grad * r.y[:, lanes] * (sig * (1.0 + gate * (1.0 - sig)))
        dy = grad * (gate * sig)
        r.dy[:, lanes] = dy
        high, low = split(dy * r.from_start[:, lanes])
        r.dy_start[:, lanes] = high
        q = r.q[:, (n // 2) * 128 : (n // 2 + 1) * 128]
        reached = dot(high, q, 0, 0) + dot(low, q, 0, 0)
        r.b_own[2 * n : 2 * n + 2] = reached.reshape(2, 128, 128)
        for peer in (2 * n, 2 * n + 1):

            @pl.when(j != peer)
            def _():
                send(r.b_own.at[peer], r.b_in.at[j], c.b_j, 0, z * 8 + peer, tx)


    r.b_in[j] = r.b_own[j]

    mixed_ring.step()

    got(r.b_in.at[pl.ds(0, 7)], c.b_j)
    carry_group(r.b_in, r.b_run, True)
    across_planes(r.b_run, r.b_z, c.b_z)
    mixed_ring.near()
    mixed_ring.far()
    share(mixed_ring, c.mixed_c, mixed_ring.left, mixed_ring.right, mixed_ring.opp)

    got(r.b_z.at[pl.ds(0, 7)], c.b_z)
    scan_planes(r.b_z, r.b_scan)
    across_planes(r.b_scan, r.b_pre, c.b_pre)

    columns_ring.near()
    columns_ring.far()
    got(r.mixed.at[pl.ds(0, 4)], c.mixed_c)

    @pl.loop(0, 4)
    def _(n):
        lanes = pl.ds(pl.multiple_of(n * 256, 256), 256)
        part = jnp.zeros((256, 256), F32)
        for i in range(8):
            part = part + dot(r.res_in[:, i].reshape(256, 128), r.mixed[i, :, lanes])
        part = part.reshape(8, 32, 256)
        r.gow_part[:, :, lanes] = part
        r.gow_out[:, :, lanes] = part.astype(BF16)

    def gow_send(*distances):
        for d in distances:
            plane = (z + d) % 8
            send(r.gow_out.at[plane], r.gow_in.at[z], c.gow_z, 0, plane * 8 + j, tx)

    gow_send(1, 7)

    got(r.b_pre.at[pl.ds(0, 7)], c.b_pre)
    back_to_group(r.b_pre[...].reshape(128, 128), r.b_back)
    to_group(r.b_back, r.dstate, c.b_back)
    gow_send(3, 5, 4, 2, 6)

    r.row_col[...] = jnp.zeros((128, 128), F32)
    r.dqk[...] = jnp.zeros((2, 128, 128), F32)

    @pl.loop(0, 8)
    def _(p):
        off = pl.multiple_of(p * 128, 128)
        g = p // 4
        qk = r.qk[g]
        dy = r.dy[:, pl.ds(off, 128)]
        part = dot(dy.astype(BF16), masked_values(p), 1, 1) * r.decay[p]
        r.dqk[g] += part[:, 0:128] + part[:, 128:256]
        total = r.row_col[...]
        dv = jnp.zeros((128, 128), F32)
        for n in range(2):
            lanes = slice(n * 128, (n + 1) * 128)
            weighed = (part[:, lanes] * qk).astype(BF16)
            head = hot(col == 2 * p + n)
            total = total + dot(weighed, head) - dot(weighed, head, 0, 0)
            own = jnp.where(first, dy, 0.0) if n == 0 else jnp.where(first, 0.0, dy)
            dv = dv + dot(r.score[0, p, :, lanes], own.astype(BF16), 0, 0)
        r.row_col[...] = total
        r.dv[:, pl.ds(off, 128)] = dv

    by_head = hot(iota((1024, 128), 0) // 64 == iota((1024, 128), 1))
    r.row_col[...] += fine_dot(r.dy[...] * r.carried[...], by_head)
    for g in range(2):
        state = r.state[g * 4 : (g + 1) * 4].reshape(512, 128)
        r.dq[:, g * 128 : (g + 1) * 128] = dot(r.dy_start[:, g * 512 : (g + 1) * 512], state)

    for g in range(2):
        lanes = slice(g * 128, (g + 1) * 128)
        r.g_q[:, lanes] = r.dq[:, lanes] + dot(r.dqk[g].astype(BF16), r.k[:, lanes])


    got(r.dstate.at[pl.ds(0, 7)], c.b_back)
    for g in range(2):
        lanes, wide = slice(g * 128, (g + 1) * 128), slice(g * 512, (g + 1) * 512)
        dstate, low = split(r.dstate[g * 4 : (g + 1) * 4].reshape(512, 128))
        k = r.k[:, lanes]
        through = (dot(k, dstate, 1, 1) + dot(k, low, 1, 1)) * r.to_end[:, wide]
        r.carried[:, wide] = through
        r.g_v[:, wide] = r.dv[:, wide] + through
        r.g_k[:, lanes] = dot(r.dqk[g].astype(BF16), r.q[:, lanes], 0, 0) + dot(r.v_end[0, :, wide], dstate)
    added = fine_dot(r.v[...].astype(F32) * r.carried[...], by_head)
    high, low = split((r.dstate[...] * r.state[...].astype(F32)).reshape(1024, 128))
    both = dot(by_head, high, 0, 0) + dot(by_head, low, 0, 0)
    kept = dot(jnp.ones((128, 128), F32), both, 1, 1, precision=HIGHEST)
    kept = kept * jnp.exp(r.c_col[127:128, :])
    upper = hot(row <= col, F32)
    below = hot(row > col, F32)
    grad = dot(upper, r.row_col[...], precision=HIGHEST) + dot(below, added, precision=HIGHEST) + kept
    r.g_decay[...] = dot(eye[0:16], grad, 1, 1, precision=HIGHEST)

    got(r.gow_in.at[pl.ds(0, 7)], c.gow_z)
    total = r.gow_part[z]
    for d in range(1, 8):
        total = total + r.gow_in[(z + d) % 8].astype(F32)
    r.g_out[...] = total

    for ring in (rows_ring, far_ring, near_ring, residual_ring, columns_ring, weight_ring, mixed_ring):
        ring.sent()
    sent(r.pack_out.at[pl.ds(0, 24)], c.dispatch)
    sent(r.pack_out.at[pl.ds(0, 39)], c.dispatch_near)
    sent(r.ret_out.at[pl.ds(0, 63)], c.back)
    scatter_sent(FAR, c.scatter)
    scatter_sent(NEAR, c.scatter_near)
    sent(r.weight.at[pl.ds(0, 7), 0], c.weight_z)
    sent(r.weight.at[:, pl.ds(0, 4)], c.weight_c)
    sent(r.mixed.at[pl.ds(0, 4)], c.mixed_c)
    sent(r.res_in.at[tx, pl.ds(0, 7)], c.gow_j)
    sent(r.gow_out.at[pl.ds(0, 7)], c.gow_z)
    for channel in (c.f_j, c.f_z, c.b_j, c.b_back):
        sent(r.f_in.at[pl.ds(0, 7)], channel)
    sent(r.state.at[pl.ds(0, 7)], c.f_back)
    sent(r.b_z.at[pl.ds(0, 7)], c.b_z)
    sent(r.b_z.at[pl.ds(0, 7)], c.b_pre)
    for channel in (c.f_jlog, c.f_zlog):
        sent(r.log_in.at[pl.ds(0, 7)], channel)


def shards(
    out_cotangent,
    routes,
    route_weights,
    expert_rows,
    w_gate,
    w_up,
    w_down,
    out_weight,
    values,
    keys,
    queries,
    log_decay,
    gate_input,
):
    arrays = [jax.ShapeDtypeStruct(shape, dtype) for shape, dtype in OUTPUTS.values()]
    scratch = [pltpu.VMEM(shape, dtype) for shape, dtype in BUFFERS.values()]
    for n in CHANNELS.values():
        scratch += [pltpu.SemaphoreType.DMA((n,))] * 2
    scratch += [pltpu.SemaphoreType.DMA((len(INPUTS),))]
    arguments = (
        out_cotangent,
        routes.T,
        route_weights.T,
        expert_rows[0],
        w_gate[0],
        w_up[0],
        w_down[0],
        out_weight,
        values,
        keys,
        queries,
        log_decay.T,
        gate_input,
    )
    outs = pl.pallas_call(
        kernel,
        out_shape=arrays,
        in_specs=[pl.BlockSpec(memory_space=pltpu.HBM)] * len(INPUTS),
        out_specs=[pl.BlockSpec(memory_space=pltpu.VMEM)] * len(OUTPUTS),
        scratch_shapes=scratch,
        compiler_params=pltpu.CompilerParams(
            has_side_effects=True, collective_id=0, vmem_limit_bytes=50000000
        ),
        name="layer_backward",
    )(*[pltpu.with_memory_space_constraint(value, pltpu.HBM) for value in arguments])
    outs = pl.pallas_call(
        publish,
        out_shape=arrays,
        in_specs=[pl.BlockSpec(memory_space=pltpu.VMEM)] * len(OUTPUTS),
        out_specs=[pl.BlockSpec(memory_space=pltpu.HBM)] * len(OUTPUTS),
        scratch_shapes=[pltpu.SemaphoreType.DMA((len(OUTPUTS),))],
        compiler_params=pltpu.CompilerParams(vmem_limit_bytes=8_000_000),
        name="publish",
    )(*outs)
    outs = list(outs)
    outs[8] = outs[8].T
    return (outs[0][None], outs[1][None], outs[2][None]) + tuple(outs[3:])


def solution(mesh):
    sp, both = P("sp", None), P("sp", "tp")
    columns, hidden = P("sp", None, "tp"), P("sp", "tp", None)
    in_specs = (sp, sp, sp, columns, columns, columns, hidden) + (both,) * 6
    out_specs = (columns, columns, hidden) + (both,) * 7
    return jax.shard_map(
        shards, mesh=mesh, in_specs=in_specs, out_specs=out_specs, check_vma=False
    )
```

```python
import jax
import jax.numpy as jnp
from jax import lax
from jax.experimental import pallas as pl
from jax.experimental.pallas import tpu as pltpu
from jax.sharding import PartitionSpec as P

MESH = pl.DeviceIdType.MESH
F32, BF16 = jnp.float32, jnp.bfloat16
HIGHEST = lax.Precision.HIGHEST

BUFFERS = dict(
    cot=((128, 512), BF16),
    routes=((2, 128), jnp.int32),
    route_weights=((2, 128), F32),
    w_gate=((2048, 256), BF16),
    w_up=((2048, 256), BF16),
    w_down=((256, 2048), BF16),
    v=((128, 1024), BF16),
    k=((128, 256), BF16),
    q=((128, 256), BF16),
    log_decay=((16, 128), F32),
    gate=((128, 1024), BF16),
    pack_out=((64, 8, 384), BF16),
    pack_in=((64, 8, 384), BF16),
    pack_sorted=((64, 8, 384), BF16),
    ret_out=((64, 8, 384), BF16),
    ret_in=((64, 8, 384), BF16),
    hit_a=((2, 128, 512), BF16),
    hit_b=((2, 3, 128, 512), BF16),
    sel_a=((384, 512), BF16),
    sel_b=((3, 384, 512), BF16),
    arr=((4, 384, 512), BF16),
    full=((4, 384, 512), BF16),
    gate_pre=((384, 256), F32),
    up_pre=((384, 256), F32),
    hidden_grad=((384, 256), F32),
    hidden=((384, 256), BF16),
    gate_grad=((384, 256), BF16),
    up_grad=((384, 256), BF16),
    rs_opp=((384, 512), BF16),
    rs_right=((384, 512), BF16),
    rs_left=((384, 512), BF16),
    rs_half_l=((384, 512), BF16),
    rs_half_r=((384, 512), BF16),
    rs_in_l=((384, 512), BF16),
    rs_in_r=((384, 512), BF16),
    rs_own=((384, 512), F32),
    rs_own_l=((384, 512), F32),
    rs_own_r=((384, 512), F32),
    resid=((4, 128, 512), BF16),
    res_t=((2, 8, 32, 128), BF16),
    res_in=((4, 8, 2, 32, 128), BF16),
    weight=((8, 8, 32, 1024), BF16),
    mixed=((8, 128, 1024), BF16),
    gow_part=((8, 32, 1024), F32),
    gow_out=((8, 32, 1024), BF16),
    gow_in=((8, 32, 1024), BF16),
    c_exp=((128, 1024), F32),
    to_end=((128, 1024), F32),
    from_start=((128, 1024), F32),
    c_row=((16, 128), F32),
    c_col=((128, 128), F32),
    v_end=((2, 128, 1024), BF16),
    qk=((2, 128, 128), F32),
    decay=((8, 128, 256), F32),
    score=((2, 8, 128, 256), BF16),
    y=((128, 1024), F32),
    carried=((128, 1024), F32),
    dy=((128, 1024), F32),
    mixed_grad=((128, 1024), F32),
    dy_start=((128, 1024), BF16),
    dv=((128, 1024), F32),
    dqk=((2, 128, 128), F32),
    row_col=((128, 128), F32),
    dq=((128, 256), F32),
    log_out=((8, 8, 128), F32),
    log_in=((8, 8, 128), F32),
    log_run=((8, 128), F32),
    log_z=((8, 8, 128), F32),
    log_before=((8, 8, 128), F32),
    before=((8, 128, 128), F32),
    f_own=((8, 128, 128), F32),
    f_in=((8, 128, 128), F32),
    f_run=((128, 128), F32),
    f_z=((8, 128, 128), F32),
    f_back=((8, 128, 128), BF16),
    state=((8, 128, 128), BF16),
    b_own=((8, 128, 128), F32),
    b_in=((8, 128, 128), F32),
    b_run=((8, 16, 128), F32),
    b_z=((8, 16, 128), F32),
    b_scan=((8, 16, 128), F32),
    b_pre=((8, 16, 128), F32),
    b_plane=((128, 128), BF16),
    b_planes=((8, 128, 128), BF16),
    b_group=((8, 128, 128), F32),
    b_log=((8, 8, 128), F32),
    dstate=((8, 128, 128), F32),
    carry=((8, 128, 128), F32),
)
CHANNELS = dict(
    rows=6,
    arrived=6,
    arrived_near=6,
    residual=3,
    dispatch=1,
    dispatch_near=1,
    back=1,
    scatter=6,
    scatter_near=6,
    weight_z=1,
    weight_y=6,
    weight_c=1,
    mixed_y=6,
    mixed_c=1,
    gow_j=1,
    columns=3,
    gow_z=1,
    f_j=1,
    f_jlog=1,
    f_z=1,
    f_zlog=1,
    f_back=1,
    b_j=1,
    b_z=1,
    b_pre=1,
    b_back=1,
    b_group=1,
    b_log=1,
)
INPUTS = dict(
    h_cot=((128, 2048), BF16),
    h_routes=((2, 128), jnp.int32),
    h_route_weights=((2, 128), F32),
    h_rows=((384, 512), BF16),
    h_w_gate=((2048, 256), BF16),
    h_w_up=((2048, 256), BF16),
    h_w_down=((256, 2048), BF16),
    h_out_weight=((32, 1024), BF16),
    h_v=((128, 1024), BF16),
    h_k=((128, 256), BF16),
    h_q=((128, 256), BF16),
    h_log_decay=((16, 128), F32),
    h_gate=((128, 1024), BF16),
)
OUTPUTS = dict(
    g_gate=((2048, 256), BF16),
    g_up=((2048, 256), BF16),
    g_down=((256, 2048), BF16),
    g_out=((32, 1024), F32),
    g_res=((128, 512), F32),
    g_v=((128, 1024), F32),
    g_k=((128, 256), F32),
    g_q=((128, 256), F32),
    g_decay=((16, 128), F32),
    g_gate_in=((128, 1024), F32),
)


PLANES = (4, 3, 5, 2, 6, 1, 7, 0)
FAR, NEAR = (0, 80, 144), (144, 256, 384)


class Refs:
    pass


def dot(a, b, ca=1, cb=0, precision=None):
    return lax.dot_general(
        a, b, (((ca,), (cb,)), ((), ())), precision=precision, preferred_element_type=F32
    )


def iota(shape, dim):
    return lax.broadcasted_iota(jnp.int32, shape, dim)


def hot(cond, dtype=BF16):
    return jnp.where(cond, 1.0, 0.0).astype(dtype)


def split(x):
    high = x.astype(BF16)
    return high, (x - high.astype(F32)).astype(BF16)


def fine_dot(a, b, ca=1, cb=0):
    high, low = split(a)
    return dot(high, b, ca, cb) + dot(low, b, ca, cb)


def sigmoid(x):
    return 1.0 / (1.0 + jnp.exp(-x))


def publish(*refs):
    n = len(OUTPUTS)
    sources, targets, sems = refs[:n], refs[n : 2 * n], refs[2 * n]
    stores = [pltpu.make_async_copy(sources[i], targets[i], sems.at[i]) for i in range(n)]
    for store in stores:
        store.start()
    for store in stores:
        store.wait()


def kernel(*refs):
    r, c, local = Refs(), Refs(), Refs()
    names = list(INPUTS) + list(OUTPUTS) + list(BUFFERS)
    for name, ref in zip(names, refs):
        setattr(r, name, ref)
    at = len(names)
    for name in CHANNELS:
        setattr(c, name, (refs[at], refs[at + 1]))
        at += 2
    in_sems = refs[at]
    for i, name in enumerate(INPUTS):
        setattr(local, name[2:], in_sems.at[i])

    me, tx = lax.axis_index("sp"), lax.axis_index("tp")
    z, j = me // 8, me % 8
    partner = j + 1 - 2 * (j % 2)
    right, left, opp = (tx + 1) % 4, (tx + 3) % 4, (tx + 2) % 4
    column = pl.multiple_of(tx * 512, 512)
    planes = [(z + d) % 8 for d in PLANES]

    barrier = pltpu.get_barrier_semaphore()

    @pl.loop(1, 64)
    def _(d):
        peer = (me + d) % 64
        pl.semaphore_signal(barrier, inc=1, device_id=(peer, tx), device_id_type=MESH)

    for side in (right, left, opp):
        pl.semaphore_signal(barrier, inc=1, device_id=(me, side), device_id_type=MESH)

    loads = dict(
        routes=(r.h_routes, r.routes),
        route_weights=(r.h_route_weights, r.route_weights),
        cot=(r.h_cot.at[:, pl.ds(column, 512)], r.cot),
        log_decay=(r.h_log_decay, r.log_decay),
        k=(r.h_k, r.k),
        v=(r.h_v, r.v),
        out_weight=(r.h_out_weight, r.weight.at[z, j]),
        q=(r.h_q, r.q),
        w_gate=(r.h_w_gate, r.w_gate),
        w_up=(r.h_w_up, r.w_up),
        w_down=(r.h_w_down, r.w_down),
        gate=(r.h_gate, r.gate),
    )
    for name, (source, target) in loads.items():
        pltpu.make_async_copy(source, target, getattr(local, name)).start()

    for n in range(8):
        source = r.h_rows.at[pl.ds(pl.multiple_of(planes[n] * 48, 16), 48)]
        pltpu.make_async_copy(source, r.full.at[tx, pl.ds(n * 48, 48)], local.rows).start()

    def loaded(target, sem):
        pltpu.make_async_copy(target, target, sem).wait()

    def send(src, dst, channel, n, sp, tp):
        out_sem, in_sem = channel
        pltpu.make_async_remote_copy(
            src_ref=src,
            dst_ref=dst,
            send_sem=out_sem.at[n],
            recv_sem=in_sem.at[n],
            device_id=(sp, tp),
            device_id_type=MESH,
        ).start()

    def got(ref, channel, n=0):
        pltpu.make_async_copy(ref, ref, channel[1].at[n]).wait()

    def sent(ref, channel, n=0):
        pltpu.make_async_copy(ref, ref, channel[0].at[n]).wait()

    class Ring:
        def __init__(self, piece, channel, members, targets):
            self.piece, self.channel = piece, channel
            self.mine, self.right, self.left, self.opp = members
            self.to_right, self.to_left = targets

        def go(self, n, h, sem, target):
            part = self.piece(n, h)
            send(part, part, self.channel, sem, *target)

        def start(self):
            self.first()
            self.second()

        def first(self):
            self.go(self.mine, 0, 0, self.to_right)
            self.go(self.mine, 1, 2, self.to_left)

        def second(self):
            self.go(self.mine, 1, 1, self.to_right)
            self.go(self.mine, 0, 3, self.to_left)

        def step(self):
            got(self.piece(self.left, 0), self.channel, 0)
            self.go(self.left, 0, 4, self.to_right)
            got(self.piece(self.right, 1), self.channel, 2)
            self.go(self.right, 1, 5, self.to_left)

        def near(self):
            got(self.piece(self.left, 1), self.channel, 1)
            got(self.piece(self.right, 0), self.channel, 3)

        def far(self):
            got(self.piece(self.opp, 0), self.channel, 4)
            got(self.piece(self.opp, 1), self.channel, 5)

        def sent(self):
            for sem, n, h in ((0, self.mine, 0), (1, self.mine, 1), (2, self.mine, 1), (3, self.mine, 0)):
                sent(self.piece(n, h), self.channel, sem)
            sent(self.piece(self.left, 0), self.channel, 4)
            sent(self.piece(self.right, 1), self.channel, 5)

    def tp_ring(buf, channel, group=None):
        start, middle, end = group or (0, buf.shape[1] // 2, buf.shape[1])
        parts = (pl.ds(start, middle - start), pl.ds(middle, end - middle))
        piece = lambda n, h: buf.at[n, parts[h]]
        return Ring(piece, channel, (tx, right, left, opp), ((me, right), (me, left)))

    class Direct:
        def __init__(self, buf, channel):
            self.buf, self.channel = buf, channel

        def start(self):
            for n, side in enumerate((right, left, opp)):
                send(self.buf.at[tx], self.buf.at[tx], self.channel, n, me, side)

        def near(self):
            got(self.buf.at[left], self.channel, 0)
            got(self.buf.at[right], self.channel, 1)

        def far(self):
            got(self.buf.at[opp], self.channel, 2)

        def sent(self):
            for n in range(3):
                sent(self.buf.at[tx], self.channel, n)

    def y_ring(piece, channel):
        members = (j, (j + 2) % 8, (j + 6) % 8, (j + 4) % 8)
        return Ring(piece, channel, members, ((z * 8 + members[1], tx), (z * 8 + members[2], tx)))

    rows_ring = tp_ring(r.full, c.rows)
    far_ring = tp_ring(r.arr, c.arrived, FAR)
    near_ring = tp_ring(r.arr, c.arrived_near, NEAR)
    residual_ring = Direct(r.resid, c.residual)
    columns_ring = Direct(r.res_in, c.columns)

    weight_ring = y_ring(lambda n, h: r.weight.at[pl.ds(4 * h, 4), n], c.weight_y)
    mixed_ring = y_ring(lambda n, h: r.mixed.at[n, pl.ds(64 * h, 64)], c.mixed_y)

    def share(ring, channel, *members):
        for n in members:
            for h in range(2):
                part = ring.piece(n, h)
                send(part, part, channel, 0, z * 8 + partner, tx)

    def to_plane_members(out, into, channel, n, first):
        own = PLANES[n] == 0

        @pl.loop(1 if own else 0, 8)
        def _(d):
            peer = (j + d) % 8
            send(out.at[first + peer], into.at[me], channel, 0, planes[n] * 8 + peer, tx)

        if own:
            into[me] = out[first + j]

    def to_group(out, into, channel):
        @pl.loop(1, 8)
        def _(d):
            peer = (j + d) % 8
            send(out.at[peer], into.at[j], channel, 0, z * 8 + peer, tx)

        into[j] = out[j]

    def across_planes(out, into, channel):
        @pl.loop(1, 8)
        def _(d):
            plane = (z + d) % 8
            send(out.at[plane], into.at[z], channel, 0, plane * 8 + j, tx)

        into[z] = out[z]

    def to_planes(src, into, channel):
        @pl.loop(1, 8)
        def _(d):
            send(src, into.at[z], channel, 0, ((z + d) % 8) * 8 + j, tx)

    eye = hot(iota((128, 128), 0) == iota((128, 128), 1), F32)
    loaded(r.routes, local.routes)
    loaded(r.route_weights, local.route_weights)
    routes = dot(eye, r.routes[...].astype(F32), 1, 1, precision=HIGHEST)
    route_weights = dot(eye, r.route_weights[...], 1, 1, precision=HIGHEST)
    expert = iota((128, 64), 1).astype(F32)
    route = [routes[:, 0:1], routes[:, 1:2]]
    named = [hot(route[n] == expert, F32) for n in range(2)]
    strict = iota((128, 128), 0) > iota((128, 128), 1)
    earlier = dot(hot(strict), (named[0] + named[1]).astype(BF16))
    slot = iota((128, 512), 1).astype(F32)
    loaded(r.cot, local.cot)
    cot = r.cot[...].astype(F32)
    scaled = []
    for n in range(2):
        rank = jnp.sum(named[n] * earlier, axis=1, keepdims=True)
        upper = jnp.where(rank >= 3.0, 1.0, 0.0)
        base = route[n] * 8.0
        r.hit_a[n] = hot(slot == base + rank)
        for m in range(3):
            place = jnp.where(rank - 3.0 * upper == float(m), base + 6.0 + upper, -1.0)
            r.hit_b[n, m] = hot(slot == place)
        scaled.append((route_weights[:, n : n + 1] * cot).astype(BF16))
    for m in range(3):
        lanes = slice(m * 128, (m + 1) * 128)
        total = dot(r.hit_a[0], scaled[0][:, lanes], 0, 0)
        total = total + dot(r.hit_a[1], scaled[1][:, lanes], 0, 0)
        total = total + dot(r.hit_b[0, m], scaled[0][:, 384:512], 0, 0)
        total = total + dot(r.hit_b[1, m], scaled[1][:, 384:512], 0, 0)
        r.pack_out[:, :, lanes] = total.reshape(64, 8, 128).astype(BF16)
    row, col = iota((128, 128), 0), iota((128, 128), 1)
    tri = hot(row >= col, F32)
    head_of = iota((16, 1024), 1) // 64 == iota((16, 1024), 0)
    loaded(r.log_decay, local.log_decay)
    loaded(r.v, local.v)
    loaded(r.k, local.k)
    log_decay = r.log_decay[...]
    cumulative = dot(tri, log_decay, 1, 1, precision=HIGHEST)
    r.c_col[...] = dot(cumulative, hot(iota((16, 128), 0) == iota((16, 128), 1), F32), precision=HIGHEST)
    r.c_row[...] = dot(log_decay, tri, 1, 1, precision=HIGHEST)
    r.c_exp[...] = dot(cumulative, hot(head_of, F32), precision=HIGHEST)
    c_exp = r.c_exp[...]
    r.from_start[...] = jnp.exp(c_exp)
    r.to_end[...] = jnp.exp(r.c_exp[127:128, :] - c_exp)
    r.v_end[0], r.v_end[1] = split(r.v[...].astype(F32) * r.to_end[...])
    for g in range(2):
        wide, k = slice(g * 512, (g + 1) * 512), r.k[:, g * 128 : (g + 1) * 128]
        own = dot(r.v_end[0, :, wide], k, 0, 0) + dot(r.v_end[1, :, wide], k, 0, 0)
        r.f_own[g * 4 : (g + 1) * 4] = own.reshape(4, 128, 128)
    total = dot(log_decay, jnp.ones((128, 128), F32), precision=HIGHEST)
    spread = hot(iota((64, 16), 0) // 4 == iota((64, 16), 1), F32)
    r.log_out[...] = dot(spread, total, precision=HIGHEST).reshape(8, 8, 128)
    place, packed = iota((384, 512), 0), iota((384, 512), 1)
    source, rank = place // 6, place % 6
    r.sel_a[...] = hot(packed == source * 8 + rank)
    for m in range(3):
        r.sel_b[m] = hot((packed == source * 8 + 6 + rank // 3) & (rank % 3 == m))

    lower = row >= col
    first = col < 64
    loaded(r.q, local.q)
    for g in range(2):
        r.qk[g] = dot(r.q[:, g * 128 : (g + 1) * 128], r.k[:, g * 128 : (g + 1) * 128], 1, 1)

    def masked_values(p):
        vp = r.v[:, pl.ds(pl.multiple_of(p * 128, 128), 128)].astype(F32)
        return jnp.concatenate(
            [jnp.where(first, vp, 0.0).astype(BF16), jnp.where(first, 0.0, vp).astype(BF16)], axis=0
        )

    @pl.loop(0, 8)
    def _(p):
        off = pl.multiple_of(p * 128, 128)
        qk = r.qk[p // 4]
        c_pair = r.c_exp[:, pl.ds(off, 128)]
        for n in range(2):
            down = jnp.minimum(c_pair[:, 64 * n : 64 * n + 1] - r.c_row[pl.ds(2 * p + n, 1), :], 0.0)
            decay = jnp.where(lower, jnp.exp(down), 0.0)
            r.decay[p, :, n * 128 : (n + 1) * 128] = decay
            lanes = slice(n * 128, (n + 1) * 128)
            r.score[0, p, :, lanes], r.score[1, p, :, lanes] = split(qk * decay)
        values = masked_values(p)
        r.y[:, pl.ds(off, 128)] = dot(r.score[0, p], values) + dot(r.score[1, p], values)

    pl.semaphore_wait(barrier, 66)
    for n in range(8):
        channel = c.dispatch if n < 3 else c.dispatch_near
        to_plane_members(r.pack_out, r.pack_in, channel, n, planes[n] * 8)
    loaded(r.full.at[tx], local.rows)
    rows_ring.start()
    to_group(r.f_own, r.f_in, c.f_j)
    to_group(r.log_out, r.log_in, c.f_jlog)
    rows_ring.step()
    loaded(r.weight.at[z, j], local.out_weight)
    to_planes(r.weight.at[z, j], r.weight.at[:, j], c.weight_z)

    def factor(log):
        e = jnp.exp(log)
        return jnp.concatenate(
            [jnp.broadcast_to(e[0:1], (64, 128)), jnp.broadcast_to(e[4:5], (64, 128))], axis=0
        )

    def carry_group(states, run_ref, reverse):
        run, log = jnp.zeros((128, 128), F32), jnp.zeros((8, 128), F32)
        for i in reversed(range(8)) if reverse else range(8):
            r.before[i] = run
            r.log_before[i] = log
            run = factor(r.log_in[i]) * run + states[i].astype(F32)
            log = log + r.log_in[i]
        run_ref[...] = run.reshape(run_ref.shape)
        return log

    def scan_planes(planes_in, scan):
        run = jnp.zeros((16, 128), F32)
        for i in reversed(range(8)):
            scan[i] = run
            run = jnp.exp(r.log_z[i, pl.ds(4 * (z // 4), 1), :]) * run + planes_in[i]

    def carry_planes(planes, back):
        run = jnp.zeros((128, 128), F32)
        for i in range(8):
            run = jnp.where(i < z, factor(r.log_z[i]) * run + planes[i], run)
        back_to_group(run, back)

    def back_to_group(run, back):
        for i in range(8):
            back[i] = (r.before[i] + factor(r.log_before[i]) * run).astype(back.dtype)

    def unpack(group, lanes, first, last):
        start, _, end = group
        for n in range(first // 8, last // 8):
            r.pack_sorted[n * 8 : (n + 1) * 8] = r.pack_in[pl.ds(planes[n] * 8, 8)]
        packed = r.pack_sorted[lanes.start // 8 : lanes.stop // 8].reshape(lanes.stop - lanes.start, 384)
        r.arr[tx, start:end, 0:384] = dot(r.sel_a[start:end, lanes], packed).astype(BF16)
        tail = dot(r.sel_b[0, start:end, lanes], packed[:, 0:128])
        tail = tail + dot(r.sel_b[1, start:end, lanes], packed[:, 128:256])
        tail = tail + dot(r.sel_b[2, start:end, lanes], packed[:, 256:384])
        r.arr[tx, start:end, 384:512] = tail.astype(BF16)

    r.pack_sorted[24:32] = jnp.zeros((8, 8, 384), BF16)
    got(r.pack_in.at[pl.ds(0, 24)], c.dispatch)
    unpack(FAR, slice(0, 256), 0, 24)
    far_ring.start()
    got(r.pack_in.at[pl.ds(0, 39)], c.dispatch_near)
    unpack(NEAR, slice(128, 512), 24, 64)
    far_ring.step()
    near_ring.start()

    got(r.f_in.at[pl.ds(0, 7)], c.f_j)
    got(r.log_in.at[pl.ds(0, 7)], c.f_jlog)
    r.log_run[...] = carry_group(r.f_in, r.f_run, False)
    r.log_z[z] = r.log_run[...]
    r.f_z[z] = r.f_run[...]
    to_planes(r.f_run, r.f_z, c.f_z)
    to_planes(r.log_run, r.log_z, c.f_zlog)


    rows_ring.near()
    rows_ring.far()
    loaded(r.w_gate, local.w_gate)
    loaded(r.w_up, local.w_up)
    loaded(r.w_down, local.w_down)
    gate_pre, up_pre = jnp.zeros((384, 256), F32), jnp.zeros((384, 256), F32)
    for t in range(4):
        gate_pre = gate_pre + dot(r.full[t], r.w_gate[t * 512 : (t + 1) * 512, :])
    r.gate_pre[...] = gate_pre
    for t in range(4):
        up_pre = up_pre + dot(r.full[t], r.w_up[t * 512 : (t + 1) * 512, :])
    r.up_pre[...] = up_pre
    gate_pre = r.gate_pre[...]
    r.hidden[...] = (gate_pre * sigmoid(gate_pre) * up_pre).astype(BF16)

    def hidden_part(t, group):
        lanes = pl.ds(pl.multiple_of(t * 512, 512), 512)
        return dot(r.arr[t, group[0] : group[2]], r.w_down[:, lanes], 1, 1)

    def hidden_grads(group):
        start, _, end = group
        hidden_grad = r.hidden_grad[start:end] + hidden_part(opp, group)
        gate_pre = r.gate_pre[start:end]
        gate_sig = sigmoid(gate_pre)
        slope = gate_sig * (1.0 + gate_pre * (1.0 - gate_sig))
        r.gate_grad[start:end] = (hidden_grad * r.up_pre[start:end] * slope).astype(BF16)
        r.up_grad[start:end] = (hidden_grad * (gate_pre * gate_sig)).astype(BF16)

    def row_part(t, start, end):
        rows = pl.ds(pl.multiple_of(t * 512, 512), 512)
        part = dot(r.gate_grad[start:end], r.w_gate[rows, :], 1, 1)
        return part + dot(r.up_grad[start:end], r.w_up[rows, :], 1, 1)

    def half_send(source, target, channel, n, start, end, side):
        part = pl.ds(start, end - start)
        send(source.at[part], target.at[part], channel, n, me, side)

    def scatter_parts(group):
        start, _, end = group
        r.rs_opp[start:end] = row_part(opp, start, end).astype(BF16)
        r.rs_own_r[start:end] = row_part(right, start, end)
        r.rs_own_l[start:end] = row_part(left, start, end)

    def scatter_start(group, channel):
        start, middle, end = group
        half_send(r.rs_opp, r.rs_half_l, channel, 0, start, middle, right)
        half_send(r.rs_opp, r.rs_half_r, channel, 1, middle, end, left)
        r.rs_right[middle:end] = r.rs_own_r[middle:end].astype(BF16)
        half_send(r.rs_right, r.rs_in_l, channel, 2, middle, end, right)
        r.rs_left[start:middle] = r.rs_own_l[start:middle].astype(BF16)
        half_send(r.rs_left, r.rs_in_r, channel, 3, start, middle, left)

    def scatter_step(group, channel):
        start, middle, end = group
        got(r.rs_half_l.at[pl.ds(start, middle - start)], channel, 0)
        total = r.rs_own_r[start:middle] + r.rs_half_l[start:middle].astype(F32)
        r.rs_right[start:middle] = total.astype(BF16)
        half_send(r.rs_right, r.rs_in_l, channel, 4, start, middle, right)
        got(r.rs_half_r.at[pl.ds(middle, end - middle)], channel, 1)
        total = r.rs_own_l[middle:end] + r.rs_half_r[middle:end].astype(F32)
        r.rs_left[middle:end] = total.astype(BF16)
        half_send(r.rs_left, r.rs_in_r, channel, 5, middle, end, left)

    def scatter_end(group, channel):
        start, middle, end = group
        top, bottom = pl.ds(start, middle - start), pl.ds(middle, end - middle)
        got(r.rs_in_l.at[bottom], channel, 2)
        got(r.rs_in_r.at[top], channel, 3)
        got(r.rs_in_l.at[top], channel, 4)
        got(r.rs_in_r.at[bottom], channel, 5)
        total = r.rs_own[start:end] + r.rs_in_l[start:end].astype(F32)
        return (total + r.rs_in_r[start:end].astype(F32)).astype(BF16)

    def scatter_sent(group, channel):
        start, middle, end = group
        top, bottom = pl.ds(start, middle - start), pl.ds(middle, end - middle)
        for n, part in enumerate((top, bottom, bottom, top, top, bottom)):
            sent(r.rs_half_l.at[part], channel, n)

    def pack_rows(summed, group, lanes, first, last):
        start, _, end = group
        skip = first * 8 - lanes.start
        for m in range(3):
            part = slice(m * 128, (m + 1) * 128)
            total = dot(r.sel_a[start:end, lanes], summed[:, part], 0, 0)
            total = total + dot(r.sel_b[m, start:end, lanes], summed[:, 384:512], 0, 0)
            total = total[skip : skip + (last - first) * 8].reshape(last - first, 8, 128)
            r.ret_out[first:last, :, part] = total.astype(BF16)

    r.hidden_grad[0:144] = hidden_part(tx, FAR)
    far_ring.near()
    r.hidden_grad[0:144] += hidden_part(left, FAR)
    r.hidden_grad[0:144] += hidden_part(right, FAR)
    far_ring.far()
    hidden_grads(FAR)
    scatter_parts(FAR)
    scatter_start(FAR, c.scatter)
    near_ring.step()
    r.hidden_grad[144:384] = hidden_part(tx, NEAR)
    scatter_step(FAR, c.scatter)

    got(r.weight.at[pl.ds(0, 7), 0], c.weight_z)
    weight_ring.first()
    share(weight_ring, c.weight_c, j)
    weight_ring.second()

    near_ring.near()
    r.hidden_grad[144:384] += hidden_part(left, NEAR)
    r.hidden_grad[144:384] += hidden_part(right, NEAR)
    near_ring.far()
    hidden_grads(NEAR)
    scatter_parts(NEAR)
    scatter_start(NEAR, c.scatter_near)
    r.rs_own[...] = row_part(tx, 0, 384)
    summed = scatter_end(FAR, c.scatter)
    pack_rows(summed, FAR, slice(0, 256), 0, 24)
    for n in range(3):
        to_plane_members(r.ret_out, r.ret_in, c.back, n, n * 8)

    got(r.f_z.at[pl.ds(0, 7)], c.f_z)
    got(r.log_z.at[pl.ds(0, 7)], c.f_zlog)
    carry_planes(r.f_z, r.f_back)
    to_group(r.f_back, r.state, c.f_back)
    scatter_step(NEAR, c.scatter_near)

    @pl.loop(0, 4)
    def _(t):
        rows = pl.ds(pl.multiple_of(t * 512, 512), 512)
        r.g_gate[rows, :] = dot(r.full[t], r.gate_grad[...], 0, 0).astype(BF16)
        r.g_up[rows, :] = dot(r.full[t], r.up_grad[...], 0, 0).astype(BF16)
        r.g_down[:, rows] = dot(r.hidden[...], r.arr[t], 0, 0).astype(BF16)


    summed = scatter_end(NEAR, c.scatter_near)
    pack_rows(summed, NEAR, slice(128, 512), 24, 64)
    for n in range(3, 8):
        to_plane_members(r.ret_out, r.ret_in, c.back, n, n * 8)
    weight_ring.step()
    weight_ring.near()
    share(weight_ring, c.weight_c, weight_ring.left, weight_ring.right)

    got(r.state.at[pl.ds(0, 7)], c.f_back)
    for g in range(2):
        lanes = slice(g * 512, (g + 1) * 512)
        state = r.state[g * 4 : (g + 1) * 4].reshape(512, 128)
        r.carried[:, lanes] = dot(r.q[:, g * 128 : (g + 1) * 128], state, 1, 1) * r.from_start[:, lanes]
    y = r.y[...] + r.carried[...]
    r.y[...] = y
    loaded(r.gate, local.gate)
    gate = r.gate[...].astype(F32)
    r.mixed[j] = (y * (gate * sigmoid(gate))).astype(BF16)
    got(r.ret_in.at[pl.ds(0, 63)], c.back)
    packed_back = r.ret_in[...].reshape(512, 384)
    picked = dot(r.hit_a[0] + r.hit_a[1], packed_back)
    tail = dot(r.hit_b[0, 0] + r.hit_b[1, 0], packed_back[:, 0:128])
    tail = tail + dot(r.hit_b[0, 1] + r.hit_b[1, 1], packed_back[:, 128:256])
    tail = tail + dot(r.hit_b[0, 2] + r.hit_b[1, 2], packed_back[:, 256:384])
    picked = jnp.concatenate([picked, tail], axis=1)
    residual = r.cot[...].astype(F32) + picked
    r.resid[tx] = residual.astype(BF16)
    residual_ring.start()

    r.res_t[...] = dot(r.resid[tx], eye.astype(BF16), 0, 0).reshape(2, 8, 32, 128).astype(BF16)

    @pl.loop(1, 8)
    def _(d):
        peer = (j + d) % 8
        send(r.res_t.at[:, peer], r.res_in.at[tx, j], c.gow_j, 0, z * 8 + peer, tx)

    r.res_in[tx, j] = r.res_t[:, j]
    r.g_res[...] = residual

    mixed_ring.start()
    share(mixed_ring, c.mixed_c, j)

    weight_ring.far()
    share(weight_ring, c.weight_c, weight_ring.opp)

    got(r.weight.at[:, pl.ds(0, 4)], c.weight_c)

    def mixed_grad_part(t, lanes):
        w = r.weight[pl.ds(2 * t, 2), :, :, lanes].reshape(512, 256)
        return dot(r.resid[t], w)

    residual_ring.near()
    for n in range(4):
        lanes = slice(n * 256, (n + 1) * 256)
        grad = mixed_grad_part(tx, lanes) + mixed_grad_part(left, lanes)
        r.mixed_grad[:, lanes] = grad + mixed_grad_part(right, lanes)
    got(r.res_in.at[tx, pl.ds(0, 7)], c.gow_j)
    columns_ring.start()
    mixed_ring.step()
    residual_ring.far()

    for n in range(4):
        lanes = slice(n * 256, (n + 1) * 256)
        grad = r.mixed_grad[:, lanes] + mixed_grad_part(opp, lanes)
        gate = r.gate[:, lanes].astype(F32)
        sig = sigmoid(gate)
        r.g_gate_in[:, lanes] = grad * r.y[:, lanes] * (sig * (1.0 + gate * (1.0 - sig)))
        dy = grad * (gate * sig)
        r.dy[:, lanes] = dy
        high, low = split(dy * r.from_start[:, lanes])
        r.dy_start[:, lanes] = high
        q = r.q[:, (n // 2) * 128 : (n // 2 + 1) * 128]
        reached = dot(high, q, 0, 0) + dot(low, q, 0, 0)
        r.b_own[2 * n : 2 * n + 2] = reached.reshape(2, 128, 128)
        for peer in (2 * n, 2 * n + 1):

            @pl.when(j != peer)
            def _():
                send(r.b_own.at[peer], r.b_in.at[j], c.b_j, 0, z * 8 + peer, tx)


    r.b_in[j] = r.b_own[j]

    mixed_ring.near()
    share(mixed_ring, c.mixed_c, mixed_ring.left, mixed_ring.right)

    got(r.b_in.at[pl.ds(0, 7)], c.b_j)
    carry_group(r.b_in, r.b_run, True)
    across_planes(r.b_run, r.b_z, c.b_z)
    to_group(r.before, r.b_group, c.b_group)
    to_group(r.log_before, r.b_log, c.b_log)
    mixed_ring.far()
    share(mixed_ring, c.mixed_c, mixed_ring.opp)

    columns_ring.near()
    columns_ring.far()
    got(r.mixed.at[pl.ds(0, 4)], c.mixed_c)

    @pl.loop(0, 4)
    def _(n):
        lanes = pl.ds(pl.multiple_of(n * 256, 256), 256)
        part = jnp.zeros((256, 256), F32)
        for i in range(8):
            part = part + dot(r.res_in[:, i].reshape(256, 128), r.mixed[i, :, lanes])
        part = part.reshape(8, 32, 256)
        r.gow_part[:, :, lanes] = part
        r.gow_out[:, :, lanes] = part.astype(BF16)

    def gow_send(*distances):
        for d in distances:
            plane = (z + d) % 8
            send(r.gow_out.at[plane], r.gow_in.at[z], c.gow_z, 0, plane * 8 + j, tx)


    got(r.b_z.at[pl.ds(0, 7)], c.b_z)
    scan_planes(r.b_z, r.b_scan)
    across_planes(r.b_scan, r.b_pre, c.b_pre)
    gow_send(3, 5, 4, 2, 6, 1, 7)

    got(r.b_pre.at[pl.ds(0, 7)], c.b_pre)
    r.b_plane[...] = r.b_pre[...].reshape(128, 128).astype(BF16)

    @pl.loop(1, 8)
    def _(d):
        send(r.b_plane, r.b_planes.at[j], c.b_back, 0, z * 8 + (j + d) % 8, tx)

    r.b_planes[j] = r.b_plane[...]

    r.row_col[...] = jnp.zeros((128, 128), F32)
    r.dqk[...] = jnp.zeros((2, 128, 128), F32)

    @pl.loop(0, 8)
    def _(p):
        off = pl.multiple_of(p * 128, 128)
        g = p // 4
        qk = r.qk[g]
        dy = r.dy[:, pl.ds(off, 128)]
        part = dot(dy.astype(BF16), masked_values(p), 1, 1) * r.decay[p]
        r.dqk[g] += part[:, 0:128] + part[:, 128:256]
        total = r.row_col[...]
        dv = jnp.zeros((128, 128), F32)
        for n in range(2):
            lanes = slice(n * 128, (n + 1) * 128)
            weighed = (part[:, lanes] * qk).astype(BF16)
            head = hot(col == 2 * p + n)
            total = total + dot(weighed, head) - dot(weighed, head, 0, 0)
            own = jnp.where(first, dy, 0.0) if n == 0 else jnp.where(first, 0.0, dy)
            dv = dv + dot(r.score[0, p, :, lanes], own.astype(BF16), 0, 0)
        r.row_col[...] = total
        r.dv[:, pl.ds(off, 128)] = dv

    by_head = hot(iota((1024, 128), 0) // 64 == iota((1024, 128), 1))
    r.row_col[...] += fine_dot(r.dy[...] * r.carried[...], by_head)
    for g in range(2):
        state = r.state[g * 4 : (g + 1) * 4].reshape(512, 128)
        r.dq[:, g * 128 : (g + 1) * 128] = dot(r.dy_start[:, g * 512 : (g + 1) * 512], state)

    for g in range(2):
        lanes = slice(g * 128, (g + 1) * 128)
        r.g_q[:, lanes] = r.dq[:, lanes] + dot(r.dqk[g].astype(BF16), r.k[:, lanes])


    got(r.b_group.at[pl.ds(0, 7)], c.b_group)
    got(r.b_log.at[pl.ds(0, 7)], c.b_log)
    for i in range(8):
        r.carry[i] = factor(r.b_log[i])
    got(r.b_planes.at[pl.ds(0, 7)], c.b_back)
    for i in range(8):
        r.dstate[i] = r.b_group[i] + r.carry[i] * r.b_planes[i].astype(F32)
    for g in range(2):
        lanes, wide = slice(g * 128, (g + 1) * 128), slice(g * 512, (g + 1) * 512)
        dstate, low = split(r.dstate[g * 4 : (g + 1) * 4].reshape(512, 128))
        k = r.k[:, lanes]
        through = (dot(k, dstate, 1, 1) + dot(k, low, 1, 1)) * r.to_end[:, wide]
        r.carried[:, wide] = through
        r.g_v[:, wide] = r.dv[:, wide] + through
        r.g_k[:, lanes] = dot(r.dqk[g].astype(BF16), r.q[:, lanes], 0, 0) + dot(r.v_end[0, :, wide], dstate)
    added = fine_dot(r.v[...].astype(F32) * r.carried[...], by_head)
    high, low = split((r.dstate[...] * r.state[...].astype(F32)).reshape(1024, 128))
    both = dot(by_head, high, 0, 0) + dot(by_head, low, 0, 0)
    kept = dot(jnp.ones((128, 128), F32), both, 1, 1, precision=HIGHEST)
    kept = kept * jnp.exp(r.c_col[127:128, :])
    upper = hot(row <= col, F32)
    below = hot(row > col, F32)
    grad = dot(upper, r.row_col[...], precision=HIGHEST) + dot(below, added, precision=HIGHEST) + kept
    r.g_decay[...] = dot(eye[0:16], grad, 1, 1, precision=HIGHEST)

    got(r.gow_in.at[pl.ds(0, 7)], c.gow_z)
    total = r.gow_part[z]
    for d in range(1, 8):
        total = total + r.gow_in[(z + d) % 8].astype(F32)
    r.g_out[...] = total

    for ring in (rows_ring, far_ring, near_ring, residual_ring, columns_ring, weight_ring, mixed_ring):
        ring.sent()
    sent(r.pack_out.at[pl.ds(0, 24)], c.dispatch)
    sent(r.pack_out.at[pl.ds(0, 39)], c.dispatch_near)
    sent(r.ret_out.at[pl.ds(0, 63)], c.back)
    scatter_sent(FAR, c.scatter)
    scatter_sent(NEAR, c.scatter_near)
    sent(r.weight.at[pl.ds(0, 7), 0], c.weight_z)
    sent(r.weight.at[:, pl.ds(0, 4)], c.weight_c)
    sent(r.mixed.at[pl.ds(0, 4)], c.mixed_c)
    sent(r.res_in.at[tx, pl.ds(0, 7)], c.gow_j)
    sent(r.gow_out.at[pl.ds(0, 7)], c.gow_z)
    for channel in (c.f_j, c.f_z, c.b_j, c.b_group):
        sent(r.f_in.at[pl.ds(0, 7)], channel)
    sent(r.b_planes.at[pl.ds(0, 7)], c.b_back)
    sent(r.state.at[pl.ds(0, 7)], c.f_back)
    sent(r.b_z.at[pl.ds(0, 7)], c.b_z)
    sent(r.b_z.at[pl.ds(0, 7)], c.b_pre)
    for channel in (c.f_jlog, c.f_zlog, c.b_log):
        sent(r.log_in.at[pl.ds(0, 7)], channel)


def shards(
    out_cotangent,
    routes,
    route_weights,
    expert_rows,
    w_gate,
    w_up,
    w_down,
    out_weight,
    values,
    keys,
    queries,
    log_decay,
    gate_input,
):
    arrays = [jax.ShapeDtypeStruct(shape, dtype) for shape, dtype in OUTPUTS.values()]
    scratch = [pltpu.VMEM(shape, dtype) for shape, dtype in BUFFERS.values()]
    for n in CHANNELS.values():
        scratch += [pltpu.SemaphoreType.DMA((n,))] * 2
    scratch += [pltpu.SemaphoreType.DMA((len(INPUTS),))]
    arguments = (
        out_cotangent,
        routes.T,
        route_weights.T,
        expert_rows[0],
        w_gate[0],
        w_up[0],
        w_down[0],
        out_weight,
        values,
        keys,
        queries,
        log_decay.T,
        gate_input,
    )
    outs = pl.pallas_call(
        kernel,
        out_shape=arrays,
        in_specs=[pl.BlockSpec(memory_space=pltpu.HBM)] * len(INPUTS),
        out_specs=[pl.BlockSpec(memory_space=pltpu.VMEM)] * len(OUTPUTS),
        scratch_shapes=scratch,
        compiler_params=pltpu.CompilerParams(
            has_side_effects=True, collective_id=0, vmem_limit_bytes=50000000
        ),
        name="layer_backward",
    )(*[pltpu.with_memory_space_constraint(value, pltpu.HBM) for value in arguments])
    outs = pl.pallas_call(
        publish,
        out_shape=arrays,
        in_specs=[pl.BlockSpec(memory_space=pltpu.VMEM)] * len(OUTPUTS),
        out_specs=[pl.BlockSpec(memory_space=pltpu.HBM)] * len(OUTPUTS),
        scratch_shapes=[pltpu.SemaphoreType.DMA((len(OUTPUTS),))],
        compiler_params=pltpu.CompilerParams(vmem_limit_bytes=8_000_000),
        name="publish",
    )(*outs)
    outs = list(outs)
    outs[8] = outs[8].T
    return (outs[0][None], outs[1][None], outs[2][None]) + tuple(outs[3:])


def solution(mesh):
    sp, both = P("sp", None), P("sp", "tp")
    columns, hidden = P("sp", None, "tp"), P("sp", "tp", None)
    in_specs = (sp, sp, sp, columns, columns, columns, hidden) + (both,) * 6
    out_specs = (columns, columns, hidden) + (both,) * 7
    return jax.shard_map(
        shards, mesh=mesh, in_specs=in_specs, out_specs=out_specs, check_vma=False
    )
```

```python
import jax
import jax.numpy as jnp
from jax import lax
from jax.experimental import pallas as pl
from jax.experimental.pallas import tpu as pltpu
from jax.sharding import PartitionSpec as P

MESH = pl.DeviceIdType.MESH
F32, BF16 = jnp.float32, jnp.bfloat16
HIGHEST = lax.Precision.HIGHEST

BUFFERS = dict(
    cot=((128, 512), BF16),
    routes=((2, 128), jnp.int32),
    route_weights=((2, 128), F32),
    w_gate=((2048, 256), BF16),
    w_up=((2048, 256), BF16),
    w_down=((256, 2048), BF16),
    v=((128, 1024), BF16),
    k=((128, 256), BF16),
    q=((128, 256), BF16),
    log_decay=((16, 128), F32),
    gate=((128, 1024), BF16),
    pack_out=((64, 8, 384), BF16),
    pack_in=((64, 8, 384), BF16),
    pack_sorted=((64, 8, 384), BF16),
    ret_out=((64, 8, 384), BF16),
    ret_in=((64, 8, 384), BF16),
    hit_a=((2, 128, 512), BF16),
    hit_b=((2, 3, 128, 512), BF16),
    sel_a=((384, 512), BF16),
    sel_b=((3, 384, 512), BF16),
    arr=((4, 384, 512), BF16),
    full=((4, 384, 512), BF16),
    gate_pre=((384, 256), F32),
    up_pre=((384, 256), F32),
    hidden_grad=((384, 256), F32),
    hidden=((384, 256), BF16),
    gate_grad=((384, 256), BF16),
    up_grad=((384, 256), BF16),
    rs_opp=((384, 512), BF16),
    rs_right=((384, 512), BF16),
    rs_left=((384, 512), BF16),
    rs_half_l=((384, 512), BF16),
    rs_half_r=((384, 512), BF16),
    rs_in_l=((384, 512), BF16),
    rs_in_r=((384, 512), BF16),
    rs_own=((384, 512), F32),
    rs_own_l=((384, 512), F32),
    rs_own_r=((384, 512), F32),
    resid=((4, 128, 512), BF16),
    res_t=((2, 8, 32, 128), BF16),
    res_in=((4, 8, 2, 32, 128), BF16),
    weight=((8, 8, 32, 1024), BF16),
    mixed=((8, 128, 1024), BF16),
    gow_part=((8, 32, 1024), F32),
    gow_out=((8, 32, 1024), BF16),
    gow_in=((8, 32, 1024), BF16),
    c_exp=((128, 1024), F32),
    to_end=((128, 1024), F32),
    from_start=((128, 1024), F32),
    c_row=((16, 128), F32),
    c_col=((128, 128), F32),
    v_end=((2, 128, 1024), BF16),
    qk=((2, 128, 128), F32),
    decay=((8, 128, 256), F32),
    score=((2, 8, 128, 256), BF16),
    y=((128, 1024), F32),
    carried=((128, 1024), F32),
    dy=((128, 1024), F32),
    mixed_grad=((128, 1024), F32),
    dy_start=((128, 1024), BF16),
    dv=((128, 1024), F32),
    dqk=((2, 128, 128), F32),
    row_col=((128, 128), F32),
    dq=((128, 256), F32),
    log_out=((8, 8, 128), F32),
    log_in=((8, 8, 128), F32),
    log_run=((8, 128), F32),
    log_z=((8, 8, 128), F32),
    log_before=((8, 8, 128), F32),
    before=((8, 128, 128), F32),
    f_own=((8, 128, 128), F32),
    f_in=((8, 128, 128), F32),
    f_run=((128, 128), F32),
    f_z=((8, 128, 128), F32),
    f_back=((8, 128, 128), BF16),
    state=((8, 128, 128), BF16),
    b_own=((8, 128, 128), F32),
    b_in=((8, 128, 128), F32),
    b_run=((8, 16, 128), F32),
    b_z=((8, 16, 128), F32),
    b_scan=((8, 16, 128), F32),
    b_pre=((8, 16, 128), F32),
    b_plane=((128, 128), BF16),
    b_planes=((8, 128, 128), BF16),
    b_group=((8, 128, 128), F32),
    b_log=((8, 8, 128), F32),
    dstate=((8, 128, 128), F32),
    carry=((8, 128, 128), F32),
)
CHANNELS = dict(
    rows=6,
    arrived=6,
    arrived_near=6,
    residual=3,
    dispatch=1,
    dispatch_near=1,
    back=1,
    scatter=6,
    scatter_near=6,
    weight_z=1,
    weight_y=6,
    weight_c=1,
    mixed_y=6,
    mixed_c=1,
    gow_j=1,
    columns=3,
    gow_z=1,
    f_j=1,
    f_jlog=1,
    f_z=1,
    f_zlog=1,
    f_back=1,
    b_j=1,
    b_z=1,
    b_pre=1,
    b_back=1,
    b_group=1,
    b_log=1,
)
INPUTS = dict(
    h_cot=((128, 2048), BF16),
    h_routes=((2, 128), jnp.int32),
    h_route_weights=((2, 128), F32),
    h_rows=((384, 512), BF16),
    h_w_gate=((2048, 256), BF16),
    h_w_up=((2048, 256), BF16),
    h_w_down=((256, 2048), BF16),
    h_out_weight=((32, 1024), BF16),
    h_v=((128, 1024), BF16),
    h_k=((128, 256), BF16),
    h_q=((128, 256), BF16),
    h_log_decay=((16, 128), F32),
    h_gate=((128, 1024), BF16),
)
OUTPUTS = dict(
    g_gate=((2048, 256), BF16),
    g_up=((2048, 256), BF16),
    g_down=((256, 2048), BF16),
    g_out=((32, 1024), F32),
    g_res=((128, 512), F32),
    g_v=((128, 1024), F32),
    g_k=((128, 256), F32),
    g_q=((128, 256), F32),
    g_decay=((16, 128), F32),
    g_gate_in=((128, 1024), F32),
)


PLANES = (4, 3, 5, 2, 6, 1, 7, 0)
FAR, NEAR = (0, 80, 144), (144, 256, 384)


class Refs:
    pass


def dot(a, b, ca=1, cb=0, precision=None):
    return lax.dot_general(
        a, b, (((ca,), (cb,)), ((), ())), precision=precision, preferred_element_type=F32
    )


def iota(shape, dim):
    return lax.broadcasted_iota(jnp.int32, shape, dim)


def hot(cond, dtype=BF16):
    return jnp.where(cond, 1.0, 0.0).astype(dtype)


def split(x):
    high = x.astype(BF16)
    return high, (x - high.astype(F32)).astype(BF16)


def fine_dot(a, b, ca=1, cb=0):
    high, low = split(a)
    return dot(high, b, ca, cb) + dot(low, b, ca, cb)


def sigmoid(x):
    return 1.0 / (1.0 + jnp.exp(-x))


def publish(*refs):
    n = len(OUTPUTS)
    sources, targets, sems = refs[:n], refs[n : 2 * n], refs[2 * n]
    stores = [pltpu.make_async_copy(sources[i], targets[i], sems.at[i]) for i in range(n)]
    for store in stores:
        store.start()
    for store in stores:
        store.wait()


def kernel(*refs):
    r, c, local = Refs(), Refs(), Refs()
    names = list(INPUTS) + list(OUTPUTS) + list(BUFFERS)
    for name, ref in zip(names, refs):
        setattr(r, name, ref)
    at = len(names)
    for name in CHANNELS:
        setattr(c, name, (refs[at], refs[at + 1]))
        at += 2
    in_sems = refs[at]
    for i, name in enumerate(INPUTS):
        setattr(local, name[2:], in_sems.at[i])

    me, tx = lax.axis_index("sp"), lax.axis_index("tp")
    z, j = me // 8, me % 8
    partner = j + 1 - 2 * (j % 2)
    right, left, opp = (tx + 1) % 4, (tx + 3) % 4, (tx + 2) % 4
    column = pl.multiple_of(tx * 512, 512)
    planes = [(z + d) % 8 for d in PLANES]

    barrier = pltpu.get_barrier_semaphore()

    @pl.loop(1, 64)
    def _(d):
        peer = (me + d) % 64
        pl.semaphore_signal(barrier, inc=1, device_id=(peer, tx), device_id_type=MESH)

    for side in (right, left, opp):
        pl.semaphore_signal(barrier, inc=1, device_id=(me, side), device_id_type=MESH)

    loads = dict(
        routes=(r.h_routes, r.routes),
        route_weights=(r.h_route_weights, r.route_weights),
        cot=(r.h_cot.at[:, pl.ds(column, 512)], r.cot),
        log_decay=(r.h_log_decay, r.log_decay),
        k=(r.h_k, r.k),
        v=(r.h_v, r.v),
        out_weight=(r.h_out_weight, r.weight.at[z, j]),
        q=(r.h_q, r.q),
        w_gate=(r.h_w_gate, r.w_gate),
        w_up=(r.h_w_up, r.w_up),
        w_down=(r.h_w_down, r.w_down),
        gate=(r.h_gate, r.gate),
    )
    for name, (source, target) in loads.items():
        pltpu.make_async_copy(source, target, getattr(local, name)).start()

    for n in range(8):
        source = r.h_rows.at[pl.ds(pl.multiple_of(planes[n] * 48, 16), 48)]
        pltpu.make_async_copy(source, r.full.at[tx, pl.ds(n * 48, 48)], local.rows).start()

    def loaded(target, sem):
        pltpu.make_async_copy(target, target, sem).wait()

    def send(src, dst, channel, n, sp, tp):
        out_sem, in_sem = channel
        pltpu.make_async_remote_copy(
            src_ref=src,
            dst_ref=dst,
            send_sem=out_sem.at[n],
            recv_sem=in_sem.at[n],
            device_id=(sp, tp),
            device_id_type=MESH,
        ).start()

    def got(ref, channel, n=0):
        pltpu.make_async_copy(ref, ref, channel[1].at[n]).wait()

    def sent(ref, channel, n=0):
        pltpu.make_async_copy(ref, ref, channel[0].at[n]).wait()

    class Ring:
        def __init__(self, piece, channel, members, targets):
            self.piece, self.channel = piece, channel
            self.mine, self.right, self.left, self.opp = members
            self.to_right, self.to_left = targets

        def go(self, n, h, sem, target):
            part = self.piece(n, h)
            send(part, part, self.channel, sem, *target)

        def start(self):
            self.first()
            self.second()

        def first(self):
            self.go(self.mine, 0, 0, self.to_right)
            self.go(self.mine, 1, 2, self.to_left)

        def second(self):
            self.go(self.mine, 1, 1, self.to_right)
            self.go(self.mine, 0, 3, self.to_left)

        def step(self):
            got(self.piece(self.left, 0), self.channel, 0)
            self.go(self.left, 0, 4, self.to_right)
            got(self.piece(self.right, 1), self.channel, 2)
            self.go(self.right, 1, 5, self.to_left)

        def near(self):
            got(self.piece(self.left, 1), self.channel, 1)
            got(self.piece(self.right, 0), self.channel, 3)

        def far(self):
            got(self.piece(self.opp, 0), self.channel, 4)
            got(self.piece(self.opp, 1), self.channel, 5)

        def sent(self):
            for sem, n, h in ((0, self.mine, 0), (1, self.mine, 1), (2, self.mine, 1), (3, self.mine, 0)):
                sent(self.piece(n, h), self.channel, sem)
            sent(self.piece(self.left, 0), self.channel, 4)
            sent(self.piece(self.right, 1), self.channel, 5)

    def tp_ring(buf, channel, group=None):
        start, middle, end = group or (0, buf.shape[1] // 2, buf.shape[1])
        parts = (pl.ds(start, middle - start), pl.ds(middle, end - middle))
        piece = lambda n, h: buf.at[n, parts[h]]
        return Ring(piece, channel, (tx, right, left, opp), ((me, right), (me, left)))

    class Direct:
        def __init__(self, buf, channel):
            self.buf, self.channel = buf, channel

        def start(self):
            for n, side in enumerate((right, left, opp)):
                send(self.buf.at[tx], self.buf.at[tx], self.channel, n, me, side)

        def near(self):
            got(self.buf.at[left], self.channel, 0)
            got(self.buf.at[right], self.channel, 1)

        def far(self):
            got(self.buf.at[opp], self.channel, 2)

        def sent(self):
            for n in range(3):
                sent(self.buf.at[tx], self.channel, n)

    def y_ring(piece, channel):
        members = (j, (j + 2) % 8, (j + 6) % 8, (j + 4) % 8)
        return Ring(piece, channel, members, ((z * 8 + members[1], tx), (z * 8 + members[2], tx)))

    rows_ring = tp_ring(r.full, c.rows)
    far_ring = tp_ring(r.arr, c.arrived, FAR)
    near_ring = tp_ring(r.arr, c.arrived_near, NEAR)
    residual_ring = Direct(r.resid, c.residual)
    columns_ring = Direct(r.res_in, c.columns)

    weight_ring = y_ring(lambda n, h: r.weight.at[pl.ds(4 * h, 4), n], c.weight_y)
    mixed_ring = y_ring(lambda n, h: r.mixed.at[n, pl.ds(64 * h, 64)], c.mixed_y)

    def share(ring, channel, *members):
        for n in members:
            for h in range(2):
                part = ring.piece(n, h)
                send(part, part, channel, 0, z * 8 + partner, tx)

    def to_plane_members(out, into, channel, n, first):
        own = PLANES[n] == 0

        @pl.loop(1 if own else 0, 8)
        def _(d):
            peer = (j + d) % 8
            send(out.at[first + peer], into.at[me], channel, 0, planes[n] * 8 + peer, tx)

        if own:
            into[me] = out[first + j]

    def to_group(out, into, channel):
        @pl.loop(1, 8)
        def _(d):
            peer = (j + d) % 8
            send(out.at[peer], into.at[j], channel, 0, z * 8 + peer, tx)

        into[j] = out[j]

    def across_planes(out, into, channel):
        @pl.loop(1, 8)
        def _(d):
            plane = (z + d) % 8
            send(out.at[plane], into.at[z], channel, 0, plane * 8 + j, tx)

        into[z] = out[z]

    def to_planes(src, into, channel):
        @pl.loop(1, 8)
        def _(d):
            send(src, into.at[z], channel, 0, ((z + d) % 8) * 8 + j, tx)

    eye = hot(iota((128, 128), 0) == iota((128, 128), 1), F32)
    loaded(r.routes, local.routes)
    loaded(r.route_weights, local.route_weights)
    routes = dot(eye, r.routes[...].astype(F32), 1, 1, precision=HIGHEST)
    route_weights = dot(eye, r.route_weights[...], 1, 1, precision=HIGHEST)
    expert = iota((128, 64), 1).astype(F32)
    route = [routes[:, 0:1], routes[:, 1:2]]
    named = [hot(route[n] == expert, F32) for n in range(2)]
    strict = iota((128, 128), 0) > iota((128, 128), 1)
    earlier = dot(hot(strict), (named[0] + named[1]).astype(BF16))
    slot = iota((128, 512), 1).astype(F32)
    loaded(r.cot, local.cot)
    cot = r.cot[...].astype(F32)
    scaled = []
    for n in range(2):
        rank = jnp.sum(named[n] * earlier, axis=1, keepdims=True)
        upper = jnp.where(rank >= 3.0, 1.0, 0.0)
        base = route[n] * 8.0
        r.hit_a[n] = hot(slot == base + rank)
        for m in range(3):
            place = jnp.where(rank - 3.0 * upper == float(m), base + 6.0 + upper, -1.0)
            r.hit_b[n, m] = hot(slot == place)
        scaled.append((route_weights[:, n : n + 1] * cot).astype(BF16))
    for m in range(3):
        lanes = slice(m * 128, (m + 1) * 128)
        total = dot(r.hit_a[0], scaled[0][:, lanes], 0, 0)
        total = total + dot(r.hit_a[1], scaled[1][:, lanes], 0, 0)
        total = total + dot(r.hit_b[0, m], scaled[0][:, 384:512], 0, 0)
        total = total + dot(r.hit_b[1, m], scaled[1][:, 384:512], 0, 0)
        r.pack_out[:, :, lanes] = total.reshape(64, 8, 128).astype(BF16)
    row, col = iota((128, 128), 0), iota((128, 128), 1)
    tri = hot(row >= col, F32)
    head_of = iota((16, 1024), 1) // 64 == iota((16, 1024), 0)
    loaded(r.log_decay, local.log_decay)
    loaded(r.v, local.v)
    loaded(r.k, local.k)
    log_decay = r.log_decay[...]
    cumulative = dot(tri, log_decay, 1, 1, precision=HIGHEST)
    r.c_col[...] = dot(cumulative, hot(iota((16, 128), 0) == iota((16, 128), 1), F32), precision=HIGHEST)
    r.c_row[...] = dot(log_decay, tri, 1, 1, precision=HIGHEST)
    r.c_exp[...] = dot(cumulative, hot(head_of, F32), precision=HIGHEST)
    c_exp = r.c_exp[...]
    r.from_start[...] = jnp.exp(c_exp)
    r.to_end[...] = jnp.exp(r.c_exp[127:128, :] - c_exp)
    r.v_end[0], r.v_end[1] = split(r.v[...].astype(F32) * r.to_end[...])
    for g in range(2):
        wide, k = slice(g * 512, (g + 1) * 512), r.k[:, g * 128 : (g + 1) * 128]
        own = dot(r.v_end[0, :, wide], k, 0, 0) + dot(r.v_end[1, :, wide], k, 0, 0)
        r.f_own[g * 4 : (g + 1) * 4] = own.reshape(4, 128, 128)
    total = dot(log_decay, jnp.ones((128, 128), F32), precision=HIGHEST)
    spread = hot(iota((64, 16), 0) // 4 == iota((64, 16), 1), F32)
    r.log_out[...] = dot(spread, total, precision=HIGHEST).reshape(8, 8, 128)
    place, packed = iota((384, 512), 0), iota((384, 512), 1)
    source, rank = place // 6, place % 6
    r.sel_a[...] = hot(packed == source * 8 + rank)
    for m in range(3):
        r.sel_b[m] = hot((packed == source * 8 + 6 + rank // 3) & (rank % 3 == m))

    lower = row >= col
    first = col < 64
    loaded(r.q, local.q)
    for g in range(2):
        r.qk[g] = dot(r.q[:, g * 128 : (g + 1) * 128], r.k[:, g * 128 : (g + 1) * 128], 1, 1)

    def masked_values(p):
        vp = r.v[:, pl.ds(pl.multiple_of(p * 128, 128), 128)].astype(F32)
        return jnp.concatenate(
            [jnp.where(first, vp, 0.0).astype(BF16), jnp.where(first, 0.0, vp).astype(BF16)], axis=0
        )

    @pl.loop(0, 8)
    def _(p):
        off = pl.multiple_of(p * 128, 128)
        qk = r.qk[p // 4]
        c_pair = r.c_exp[:, pl.ds(off, 128)]
        for n in range(2):
            down = jnp.minimum(c_pair[:, 64 * n : 64 * n + 1] - r.c_row[pl.ds(2 * p + n, 1), :], 0.0)
            decay = jnp.where(lower, jnp.exp(down), 0.0)
            r.decay[p, :, n * 128 : (n + 1) * 128] = decay
            lanes = slice(n * 128, (n + 1) * 128)
            r.score[0, p, :, lanes], r.score[1, p, :, lanes] = split(qk * decay)
        values = masked_values(p)
        r.y[:, pl.ds(off, 128)] = dot(r.score[0, p], values) + dot(r.score[1, p], values)

    pl.semaphore_wait(barrier, 66)
    for n in range(8):
        channel = c.dispatch if n < 3 else c.dispatch_near
        to_plane_members(r.pack_out, r.pack_in, channel, n, planes[n] * 8)
    loaded(r.full.at[tx], local.rows)
    rows_ring.start()
    to_group(r.f_own, r.f_in, c.f_j)
    to_group(r.log_out, r.log_in, c.f_jlog)
    rows_ring.step()
    loaded(r.weight.at[z, j], local.out_weight)
    to_planes(r.weight.at[z, j], r.weight.at[:, j], c.weight_z)

    def factor(log):
        e = jnp.exp(log)
        return jnp.concatenate(
            [jnp.broadcast_to(e[0:1], (64, 128)), jnp.broadcast_to(e[4:5], (64, 128))], axis=0
        )

    def carry_group(states, run_ref, reverse):
        run, log = jnp.zeros((128, 128), F32), jnp.zeros((8, 128), F32)
        for i in reversed(range(8)) if reverse else range(8):
            r.before[i] = run
            r.log_before[i] = log
            run = factor(r.log_in[i]) * run + states[i].astype(F32)
            log = log + r.log_in[i]
        run_ref[...] = run.reshape(run_ref.shape)
        return log

    def scan_planes(planes_in, scan):
        run = jnp.zeros((16, 128), F32)
        for i in reversed(range(8)):
            scan[i] = run
            run = jnp.exp(r.log_z[i, pl.ds(4 * (z // 4), 1), :]) * run + planes_in[i]

    def carry_planes(planes, back):
        run = jnp.zeros((128, 128), F32)
        for i in range(8):
            run = jnp.where(i < z, factor(r.log_z[i]) * run + planes[i], run)
        back_to_group(run, back)

    def back_to_group(run, back):
        for i in range(8):
            back[i] = (r.before[i] + factor(r.log_before[i]) * run).astype(back.dtype)

    def unpack(group, lanes, first, last):
        start, _, end = group
        for n in range(first // 8, last // 8):
            r.pack_sorted[n * 8 : (n + 1) * 8] = r.pack_in[pl.ds(planes[n] * 8, 8)]
        packed = r.pack_sorted[lanes.start // 8 : lanes.stop // 8].reshape(lanes.stop - lanes.start, 384)
        r.arr[tx, start:end, 0:384] = dot(r.sel_a[start:end, lanes], packed).astype(BF16)
        tail = dot(r.sel_b[0, start:end, lanes], packed[:, 0:128])
        tail = tail + dot(r.sel_b[1, start:end, lanes], packed[:, 128:256])
        tail = tail + dot(r.sel_b[2, start:end, lanes], packed[:, 256:384])
        r.arr[tx, start:end, 384:512] = tail.astype(BF16)

    r.pack_sorted[24:32] = jnp.zeros((8, 8, 384), BF16)
    got(r.pack_in.at[pl.ds(0, 24)], c.dispatch)
    unpack(FAR, slice(0, 256), 0, 24)
    far_ring.start()
    got(r.pack_in.at[pl.ds(0, 39)], c.dispatch_near)
    unpack(NEAR, slice(128, 512), 24, 64)
    far_ring.step()
    near_ring.start()

    got(r.f_in.at[pl.ds(0, 7)], c.f_j)
    got(r.log_in.at[pl.ds(0, 7)], c.f_jlog)
    r.log_run[...] = carry_group(r.f_in, r.f_run, False)
    r.log_z[z] = r.log_run[...]
    r.f_z[z] = r.f_run[...]
    to_planes(r.f_run, r.f_z, c.f_z)
    to_planes(r.log_run, r.log_z, c.f_zlog)


    rows_ring.near()
    rows_ring.far()
    loaded(r.w_gate, local.w_gate)
    loaded(r.w_up, local.w_up)
    loaded(r.w_down, local.w_down)
    gate_pre, up_pre = jnp.zeros((384, 256), F32), jnp.zeros((384, 256), F32)
    for t in range(4):
        gate_pre = gate_pre + dot(r.full[t], r.w_gate[t * 512 : (t + 1) * 512, :])
    r.gate_pre[...] = gate_pre
    for t in range(4):
        up_pre = up_pre + dot(r.full[t], r.w_up[t * 512 : (t + 1) * 512, :])
    r.up_pre[...] = up_pre
    gate_pre = r.gate_pre[...]
    r.hidden[...] = (gate_pre * sigmoid(gate_pre) * up_pre).astype(BF16)

    def hidden_part(t, group):
        lanes = pl.ds(pl.multiple_of(t * 512, 512), 512)
        return dot(r.arr[t, group[0] : group[2]], r.w_down[:, lanes], 1, 1)

    def hidden_grads(group):
        start, _, end = group
        hidden_grad = r.hidden_grad[start:end] + hidden_part(opp, group)
        gate_pre = r.gate_pre[start:end]
        gate_sig = sigmoid(gate_pre)
        slope = gate_sig * (1.0 + gate_pre * (1.0 - gate_sig))
        r.gate_grad[start:end] = (hidden_grad * r.up_pre[start:end] * slope).astype(BF16)
        r.up_grad[start:end] = (hidden_grad * (gate_pre * gate_sig)).astype(BF16)

    def row_part(t, start, end):
        rows = pl.ds(pl.multiple_of(t * 512, 512), 512)
        part = dot(r.gate_grad[start:end], r.w_gate[rows, :], 1, 1)
        return part + dot(r.up_grad[start:end], r.w_up[rows, :], 1, 1)

    def half_send(source, target, channel, n, start, end, side):
        part = pl.ds(start, end - start)
        send(source.at[part], target.at[part], channel, n, me, side)

    def scatter_parts(group):
        start, _, end = group
        r.rs_opp[start:end] = row_part(opp, start, end).astype(BF16)
        r.rs_own_r[start:end] = row_part(right, start, end)
        r.rs_own_l[start:end] = row_part(left, start, end)

    def scatter_start(group, channel):
        start, middle, end = group
        half_send(r.rs_opp, r.rs_half_l, channel, 0, start, middle, right)
        half_send(r.rs_opp, r.rs_half_r, channel, 1, middle, end, left)
        r.rs_right[middle:end] = r.rs_own_r[middle:end].astype(BF16)
        half_send(r.rs_right, r.rs_in_l, channel, 2, middle, end, right)
        r.rs_left[start:middle] = r.rs_own_l[start:middle].astype(BF16)
        half_send(r.rs_left, r.rs_in_r, channel, 3, start, middle, left)

    def scatter_step(group, channel):
        start, middle, end = group
        got(r.rs_half_l.at[pl.ds(start, middle - start)], channel, 0)
        total = r.rs_own_r[start:middle] + r.rs_half_l[start:middle].astype(F32)
        r.rs_right[start:middle] = total.astype(BF16)
        half_send(r.rs_right, r.rs_in_l, channel, 4, start, middle, right)
        got(r.rs_half_r.at[pl.ds(middle, end - middle)], channel, 1)
        total = r.rs_own_l[middle:end] + r.rs_half_r[middle:end].astype(F32)
        r.rs_left[middle:end] = total.astype(BF16)
        half_send(r.rs_left, r.rs_in_r, channel, 5, middle, end, left)

    def scatter_end(group, channel):
        start, middle, end = group
        top, bottom = pl.ds(start, middle - start), pl.ds(middle, end - middle)
        got(r.rs_in_l.at[bottom], channel, 2)
        got(r.rs_in_r.at[top], channel, 3)
        got(r.rs_in_l.at[top], channel, 4)
        got(r.rs_in_r.at[bottom], channel, 5)
        total = r.rs_own[start:end] + r.rs_in_l[start:end].astype(F32)
        return (total + r.rs_in_r[start:end].astype(F32)).astype(BF16)

    def scatter_sent(group, channel):
        start, middle, end = group
        top, bottom = pl.ds(start, middle - start), pl.ds(middle, end - middle)
        for n, part in enumerate((top, bottom, bottom, top, top, bottom)):
            sent(r.rs_half_l.at[part], channel, n)

    def pack_rows(summed, group, lanes, first, last):
        start, _, end = group
        skip = first * 8 - lanes.start
        for m in range(3):
            part = slice(m * 128, (m + 1) * 128)
            total = dot(r.sel_a[start:end, lanes], summed[:, part], 0, 0)
            total = total + dot(r.sel_b[m, start:end, lanes], summed[:, 384:512], 0, 0)
            total = total[skip : skip + (last - first) * 8].reshape(last - first, 8, 128)
            r.ret_out[first:last, :, part] = total.astype(BF16)

    r.hidden_grad[0:144] = hidden_part(tx, FAR)
    far_ring.near()
    r.hidden_grad[0:144] += hidden_part(left, FAR)
    r.hidden_grad[0:144] += hidden_part(right, FAR)
    far_ring.far()
    hidden_grads(FAR)
    scatter_parts(FAR)
    scatter_start(FAR, c.scatter)
    near_ring.step()
    r.hidden_grad[144:384] = hidden_part(tx, NEAR)
    scatter_step(FAR, c.scatter)

    got(r.weight.at[pl.ds(0, 7), 0], c.weight_z)
    weight_ring.first()
    share(weight_ring, c.weight_c, j)
    weight_ring.second()

    near_ring.near()
    r.hidden_grad[144:384] += hidden_part(left, NEAR)
    r.hidden_grad[144:384] += hidden_part(right, NEAR)
    near_ring.far()
    hidden_grads(NEAR)
    scatter_parts(NEAR)
    scatter_start(NEAR, c.scatter_near)
    r.rs_own[...] = row_part(tx, 0, 384)
    summed = scatter_end(FAR, c.scatter)
    pack_rows(summed, FAR, slice(0, 256), 0, 24)
    for n in range(3):
        to_plane_members(r.ret_out, r.ret_in, c.back, n, n * 8)

    got(r.f_z.at[pl.ds(0, 7)], c.f_z)
    got(r.log_z.at[pl.ds(0, 7)], c.f_zlog)
    carry_planes(r.f_z, r.f_back)
    to_group(r.f_back, r.state, c.f_back)
    scatter_step(NEAR, c.scatter_near)

    @pl.loop(0, 4)
    def _(t):
        rows = pl.ds(pl.multiple_of(t * 512, 512), 512)
        r.g_gate[rows, :] = dot(r.full[t], r.gate_grad[...], 0, 0).astype(BF16)
        r.g_up[rows, :] = dot(r.full[t], r.up_grad[...], 0, 0).astype(BF16)
        r.g_down[:, rows] = dot(r.hidden[...], r.arr[t], 0, 0).astype(BF16)


    summed = scatter_end(NEAR, c.scatter_near)
    pack_rows(summed, NEAR, slice(128, 512), 24, 64)
    for n in range(3, 8):
        to_plane_members(r.ret_out, r.ret_in, c.back, n, n * 8)
    weight_ring.step()
    weight_ring.near()
    share(weight_ring, c.weight_c, weight_ring.left, weight_ring.right)

    got(r.state.at[pl.ds(0, 7)], c.f_back)
    for g in range(2):
        lanes = slice(g * 512, (g + 1) * 512)
        state = r.state[g * 4 : (g + 1) * 4].reshape(512, 128)
        r.carried[:, lanes] = dot(r.q[:, g * 128 : (g + 1) * 128], state, 1, 1) * r.from_start[:, lanes]
    y = r.y[...] + r.carried[...]
    r.y[...] = y
    loaded(r.gate, local.gate)
    gate = r.gate[...].astype(F32)
    r.mixed[j] = (y * (gate * sigmoid(gate))).astype(BF16)
    got(r.ret_in.at[pl.ds(0, 63)], c.back)
    packed_back = r.ret_in[...].reshape(512, 384)
    picked = dot(r.hit_a[0] + r.hit_a[1], packed_back)
    tail = dot(r.hit_b[0, 0] + r.hit_b[1, 0], packed_back[:, 0:128])
    tail = tail + dot(r.hit_b[0, 1] + r.hit_b[1, 1], packed_back[:, 128:256])
    tail = tail + dot(r.hit_b[0, 2] + r.hit_b[1, 2], packed_back[:, 256:384])
    picked = jnp.concatenate([picked, tail], axis=1)
    residual = r.cot[...].astype(F32) + picked
    r.resid[tx] = residual.astype(BF16)
    residual_ring.start()

    r.res_t[...] = dot(r.resid[tx], eye.astype(BF16), 0, 0).reshape(2, 8, 32, 128).astype(BF16)

    @pl.loop(1, 8)
    def _(d):
        peer = (j + d) % 8
        send(r.res_t.at[:, peer], r.res_in.at[tx, j], c.gow_j, 0, z * 8 + peer, tx)

    r.res_in[tx, j] = r.res_t[:, j]
    r.g_res[...] = residual

    mixed_ring.start()
    share(mixed_ring, c.mixed_c, j)

    weight_ring.far()
    share(weight_ring, c.weight_c, weight_ring.opp)

    got(r.weight.at[:, pl.ds(0, 4)], c.weight_c)

    def mixed_grad_part(t, lanes):
        w = r.weight[pl.ds(2 * t, 2), :, :, lanes].reshape(512, 256)
        return dot(r.resid[t], w)

    residual_ring.near()
    for n in range(4):
        lanes = slice(n * 256, (n + 1) * 256)
        grad = mixed_grad_part(tx, lanes) + mixed_grad_part(left, lanes)
        r.mixed_grad[:, lanes] = grad + mixed_grad_part(right, lanes)
    got(r.res_in.at[tx, pl.ds(0, 7)], c.gow_j)
    columns_ring.start()
    mixed_ring.step()
    residual_ring.far()

    for n in range(4):
        lanes = slice(n * 256, (n + 1) * 256)
        grad = r.mixed_grad[:, lanes] + mixed_grad_part(opp, lanes)
        gate = r.gate[:, lanes].astype(F32)
        sig = sigmoid(gate)
        r.g_gate_in[:, lanes] = grad * r.y[:, lanes] * (sig * (1.0 + gate * (1.0 - sig)))
        dy = grad * (gate * sig)
        r.dy[:, lanes] = dy
        high, low = split(dy * r.from_start[:, lanes])
        r.dy_start[:, lanes] = high
        q = r.q[:, (n // 2) * 128 : (n // 2 + 1) * 128]
        reached = dot(high, q, 0, 0) + dot(low, q, 0, 0)
        r.b_own[2 * n : 2 * n + 2] = reached.reshape(2, 128, 128)
        for peer in (2 * n, 2 * n + 1):

            @pl.when(j != peer)
            def _():
                send(r.b_own.at[peer], r.b_in.at[j], c.b_j, 0, z * 8 + peer, tx)


    r.b_in[j] = r.b_own[j]

    got(r.b_in.at[pl.ds(0, 7)], c.b_j)
    carry_group(r.b_in, r.b_run, True)
    across_planes(r.b_run, r.b_z, c.b_z)
    to_group(r.before, r.b_group, c.b_group)
    to_group(r.log_before, r.b_log, c.b_log)
    mixed_ring.near()
    mixed_ring.far()
    share(mixed_ring, c.mixed_c, mixed_ring.left, mixed_ring.right, mixed_ring.opp)

    columns_ring.near()
    columns_ring.far()
    got(r.mixed.at[pl.ds(0, 4)], c.mixed_c)

    @pl.loop(0, 4)
    def _(n):
        lanes = pl.ds(pl.multiple_of(n * 256, 256), 256)
        part = jnp.zeros((256, 256), F32)
        for i in range(8):
            part = part + dot(r.res_in[:, i].reshape(256, 128), r.mixed[i, :, lanes])
        part = part.reshape(8, 32, 256)
        r.gow_part[:, :, lanes] = part
        r.gow_out[:, :, lanes] = part.astype(BF16)

    def gow_send(*distances):
        for d in distances:
            plane = (z + d) % 8
            send(r.gow_out.at[plane], r.gow_in.at[z], c.gow_z, 0, plane * 8 + j, tx)


    got(r.b_z.at[pl.ds(0, 7)], c.b_z)
    scan_planes(r.b_z, r.b_scan)
    across_planes(r.b_scan, r.b_pre, c.b_pre)
    gow_send(3, 5, 4, 2, 6, 1, 7)

    got(r.b_pre.at[pl.ds(0, 7)], c.b_pre)
    r.b_plane[...] = r.b_pre[...].reshape(128, 128).astype(BF16)

    @pl.loop(1, 8)
    def _(d):
        send(r.b_plane, r.b_planes.at[j], c.b_back, 0, z * 8 + (j + d) % 8, tx)

    r.b_planes[j] = r.b_plane[...]

    r.row_col[...] = jnp.zeros((128, 128), F32)
    r.dqk[...] = jnp.zeros((2, 128, 128), F32)

    @pl.loop(0, 8)
    def _(p):
        off = pl.multiple_of(p * 128, 128)
        g = p // 4
        qk = r.qk[g]
        dy = r.dy[:, pl.ds(off, 128)]
        part = dot(dy.astype(BF16), masked_values(p), 1, 1) * r.decay[p]
        r.dqk[g] += part[:, 0:128] + part[:, 128:256]
        total = r.row_col[...]
        dv = jnp.zeros((128, 128), F32)
        for n in range(2):
            lanes = slice(n * 128, (n + 1) * 128)
            weighed = (part[:, lanes] * qk).astype(BF16)
            head = hot(col == 2 * p + n)
            total = total + dot(weighed, head) - dot(weighed, head, 0, 0)
            own = jnp.where(first, dy, 0.0) if n == 0 else jnp.where(first, 0.0, dy)
            dv = dv + dot(r.score[0, p, :, lanes], own.astype(BF16), 0, 0)
        r.row_col[...] = total
        r.dv[:, pl.ds(off, 128)] = dv

    by_head = hot(iota((1024, 128), 0) // 64 == iota((1024, 128), 1))
    r.row_col[...] += fine_dot(r.dy[...] * r.carried[...], by_head)
    for g in range(2):
        state = r.state[g * 4 : (g + 1) * 4].reshape(512, 128)
        r.dq[:, g * 128 : (g + 1) * 128] = dot(r.dy_start[:, g * 512 : (g + 1) * 512], state)

    for g in range(2):
        lanes = slice(g * 128, (g + 1) * 128)
        r.g_q[:, lanes] = r.dq[:, lanes] + dot(r.dqk[g].astype(BF16), r.k[:, lanes])


    got(r.b_group.at[pl.ds(0, 7)], c.b_group)
    got(r.b_log.at[pl.ds(0, 7)], c.b_log)
    for i in range(8):
        r.carry[i] = factor(r.b_log[i])
    got(r.b_planes.at[pl.ds(0, 7)], c.b_back)
    for i in range(8):
        r.dstate[i] = r.b_group[i] + r.carry[i] * r.b_planes[i].astype(F32)
    for g in range(2):
        lanes, wide = slice(g * 128, (g + 1) * 128), slice(g * 512, (g + 1) * 512)
        dstate, low = split(r.dstate[g * 4 : (g + 1) * 4].reshape(512, 128))
        k = r.k[:, lanes]
        through = (dot(k, dstate, 1, 1) + dot(k, low, 1, 1)) * r.to_end[:, wide]
        r.carried[:, wide] = through
        r.g_v[:, wide] = r.dv[:, wide] + through
        r.g_k[:, lanes] = dot(r.dqk[g].astype(BF16), r.q[:, lanes], 0, 0) + dot(r.v_end[0, :, wide], dstate)
    added = fine_dot(r.v[...].astype(F32) * r.carried[...], by_head)
    high, low = split((r.dstate[...] * r.state[...].astype(F32)).reshape(1024, 128))
    both = dot(by_head, high, 0, 0) + dot(by_head, low, 0, 0)
    kept = dot(jnp.ones((128, 128), F32), both, 1, 1, precision=HIGHEST)
    kept = kept * jnp.exp(r.c_col[127:128, :])
    upper = hot(row <= col, F32)
    below = hot(row > col, F32)
    grad = dot(upper, r.row_col[...], precision=HIGHEST) + dot(below, added, precision=HIGHEST) + kept
    r.g_decay[...] = dot(eye[0:16], grad, 1, 1, precision=HIGHEST)

    got(r.gow_in.at[pl.ds(0, 7)], c.gow_z)
    total = r.gow_part[z]
    for d in range(1, 8):
        total = total + r.gow_in[(z + d) % 8].astype(F32)
    r.g_out[...] = total

    for ring in (rows_ring, far_ring, near_ring, residual_ring, columns_ring, weight_ring, mixed_ring):
        ring.sent()
    sent(r.pack_out.at[pl.ds(0, 24)], c.dispatch)
    sent(r.pack_out.at[pl.ds(0, 39)], c.dispatch_near)
    sent(r.ret_out.at[pl.ds(0, 63)], c.back)
    scatter_sent(FAR, c.scatter)
    scatter_sent(NEAR, c.scatter_near)
    sent(r.weight.at[pl.ds(0, 7), 0], c.weight_z)
    sent(r.weight.at[:, pl.ds(0, 4)], c.weight_c)
    sent(r.mixed.at[pl.ds(0, 4)], c.mixed_c)
    sent(r.res_in.at[tx, pl.ds(0, 7)], c.gow_j)
    sent(r.gow_out.at[pl.ds(0, 7)], c.gow_z)
    for channel in (c.f_j, c.f_z, c.b_j, c.b_group):
        sent(r.f_in.at[pl.ds(0, 7)], channel)
    sent(r.b_planes.at[pl.ds(0, 7)], c.b_back)
    sent(r.state.at[pl.ds(0, 7)], c.f_back)
    sent(r.b_z.at[pl.ds(0, 7)], c.b_z)
    sent(r.b_z.at[pl.ds(0, 7)], c.b_pre)
    for channel in (c.f_jlog, c.f_zlog, c.b_log):
        sent(r.log_in.at[pl.ds(0, 7)], channel)


def shards(
    out_cotangent,
    routes,
    route_weights,
    expert_rows,
    w_gate,
    w_up,
    w_down,
    out_weight,
    values,
    keys,
    queries,
    log_decay,
    gate_input,
):
    arrays = [jax.ShapeDtypeStruct(shape, dtype) for shape, dtype in OUTPUTS.values()]
    scratch = [pltpu.VMEM(shape, dtype) for shape, dtype in BUFFERS.values()]
    for n in CHANNELS.values():
        scratch += [pltpu.SemaphoreType.DMA((n,))] * 2
    scratch += [pltpu.SemaphoreType.DMA((len(INPUTS),))]
    arguments = (
        out_cotangent,
        routes.T,
        route_weights.T,
        expert_rows[0],
        w_gate[0],
        w_up[0],
        w_down[0],
        out_weight,
        values,
        keys,
        queries,
        log_decay.T,
        gate_input,
    )
    outs = pl.pallas_call(
        kernel,
        out_shape=arrays,
        in_specs=[pl.BlockSpec(memory_space=pltpu.HBM)] * len(INPUTS),
        out_specs=[pl.BlockSpec(memory_space=pltpu.VMEM)] * len(OUTPUTS),
        scratch_shapes=scratch,
        compiler_params=pltpu.CompilerParams(
            has_side_effects=True, collective_id=0, vmem_limit_bytes=50000000
        ),
        name="layer_backward",
    )(*[pltpu.with_memory_space_constraint(value, pltpu.HBM) for value in arguments])
    outs = pl.pallas_call(
        publish,
        out_shape=arrays,
        in_specs=[pl.BlockSpec(memory_space=pltpu.VMEM)] * len(OUTPUTS),
        out_specs=[pl.BlockSpec(memory_space=pltpu.HBM)] * len(OUTPUTS),
        scratch_shapes=[pltpu.SemaphoreType.DMA((len(OUTPUTS),))],
        compiler_params=pltpu.CompilerParams(vmem_limit_bytes=8_000_000),
        name="publish",
    )(*outs)
    outs = list(outs)
    outs[8] = outs[8].T
    return (outs[0][None], outs[1][None], outs[2][None]) + tuple(outs[3:])


def solution(mesh):
    sp, both = P("sp", None), P("sp", "tp")
    columns, hidden = P("sp", None, "tp"), P("sp", "tp", None)
    in_specs = (sp, sp, sp, columns, columns, columns, hidden) + (both,) * 6
    out_specs = (columns, columns, hidden) + (both,) * 7
    return jax.shard_map(
        shards, mesh=mesh, in_specs=in_specs, out_specs=out_specs, check_vma=False
    )
```

```python
import jax
import jax.numpy as jnp
from jax import lax
from jax.experimental import pallas as pl
from jax.experimental.pallas import tpu as pltpu
from jax.sharding import PartitionSpec as P

MESH = pl.DeviceIdType.MESH
F32, BF16 = jnp.float32, jnp.bfloat16
HIGHEST = lax.Precision.HIGHEST

BUFFERS = dict(
    cot=((128, 512), BF16),
    routes=((2, 128), jnp.int32),
    route_weights=((2, 128), F32),
    w_gate=((2048, 256), BF16),
    w_up=((2048, 256), BF16),
    w_down=((256, 2048), BF16),
    v=((128, 1024), BF16),
    k=((128, 256), BF16),
    q=((128, 256), BF16),
    log_decay=((16, 128), F32),
    gate=((128, 1024), BF16),
    pack_out=((64, 8, 384), BF16),
    pack_in=((64, 8, 384), BF16),
    pack_sorted=((64, 8, 384), BF16),
    ret_out=((64, 8, 384), BF16),
    ret_in=((64, 8, 384), BF16),
    hit_a=((2, 128, 512), BF16),
    hit_b=((2, 3, 128, 512), BF16),
    sel_a=((384, 512), BF16),
    sel_b=((3, 384, 512), BF16),
    arr=((4, 384, 512), BF16),
    full=((4, 384, 512), BF16),
    gate_pre=((384, 256), F32),
    up_pre=((384, 256), F32),
    hidden_grad=((384, 256), F32),
    hidden=((384, 256), BF16),
    gate_grad=((384, 256), BF16),
    up_grad=((384, 256), BF16),
    rs_opp=((384, 512), BF16),
    rs_right=((384, 512), BF16),
    rs_left=((384, 512), BF16),
    rs_half_l=((384, 512), BF16),
    rs_half_r=((384, 512), BF16),
    rs_in_l=((384, 512), BF16),
    rs_in_r=((384, 512), BF16),
    rs_own=((384, 512), F32),
    rs_own_l=((384, 512), F32),
    rs_own_r=((384, 512), F32),
    resid=((4, 128, 512), BF16),
    res_t=((2, 8, 32, 128), BF16),
    res_in=((4, 8, 2, 32, 128), BF16),
    weight=((8, 8, 32, 1024), BF16),
    mixed=((8, 128, 1024), BF16),
    gow_part=((8, 32, 1024), F32),
    gow_out=((8, 32, 1024), BF16),
    gow_in=((8, 32, 1024), BF16),
    c_exp=((128, 1024), F32),
    to_end=((128, 1024), F32),
    from_start=((128, 1024), F32),
    c_row=((16, 128), F32),
    c_col=((128, 128), F32),
    v_end=((2, 128, 1024), BF16),
    qk=((2, 128, 128), F32),
    decay=((8, 128, 256), F32),
    score=((2, 8, 128, 256), BF16),
    y=((128, 1024), F32),
    carried=((128, 1024), F32),
    dy=((128, 1024), F32),
    mixed_grad=((128, 1024), F32),
    dy_start=((128, 1024), BF16),
    dv=((128, 1024), F32),
    dqk=((2, 128, 128), F32),
    row_col=((128, 128), F32),
    dq=((128, 256), F32),
    log_out=((8, 8, 128), F32),
    log_in=((8, 8, 128), F32),
    log_run=((8, 128), F32),
    log_z=((8, 8, 128), F32),
    log_before=((8, 8, 128), F32),
    before=((8, 128, 128), F32),
    f_own=((8, 128, 128), F32),
    f_in=((8, 128, 128), F32),
    f_run=((128, 128), F32),
    f_z=((8, 128, 128), F32),
    f_back=((8, 128, 128), BF16),
    state=((8, 128, 128), BF16),
    b_own=((8, 128, 128), F32),
    b_in=((8, 128, 128), F32),
    b_run=((8, 16, 128), F32),
    b_z=((8, 16, 128), F32),
    b_scan=((8, 16, 128), F32),
    b_pre=((8, 16, 128), F32),
    b_plane=((128, 128), BF16),
    b_planes=((8, 128, 128), BF16),
    b_group=((8, 128, 128), F32),
    b_log=((8, 8, 128), F32),
    dstate=((8, 128, 128), F32),
    carry=((8, 128, 128), F32),
)
CHANNELS = dict(
    rows=6,
    arrived=6,
    arrived_near=6,
    residual=3,
    dispatch=1,
    dispatch_near=1,
    back=1,
    scatter=6,
    scatter_near=6,
    weight_z=1,
    weight_y=6,
    weight_c=1,
    mixed_y=6,
    mixed_c=1,
    gow_j=1,
    columns=3,
    gow_z=1,
    f_j=1,
    f_jlog=1,
    f_z=1,
    f_zlog=1,
    f_back=1,
    b_j=1,
    b_z=1,
    b_pre=1,
    b_back=1,
    b_group=1,
    b_log=1,
)
INPUTS = dict(
    h_cot=((128, 2048), BF16),
    h_routes=((2, 128), jnp.int32),
    h_route_weights=((2, 128), F32),
    h_rows=((384, 512), BF16),
    h_w_gate=((2048, 256), BF16),
    h_w_up=((2048, 256), BF16),
    h_w_down=((256, 2048), BF16),
    h_out_weight=((32, 1024), BF16),
    h_v=((128, 1024), BF16),
    h_k=((128, 256), BF16),
    h_q=((128, 256), BF16),
    h_log_decay=((16, 128), F32),
    h_gate=((128, 1024), BF16),
)
OUTPUTS = dict(
    g_gate=((2048, 256), BF16),
    g_up=((2048, 256), BF16),
    g_down=((256, 2048), BF16),
    g_out=((32, 1024), F32),
    g_res=((128, 512), F32),
    g_v=((128, 1024), F32),
    g_k=((128, 256), F32),
    g_q=((128, 256), F32),
    g_decay=((16, 128), F32),
    g_gate_in=((128, 1024), F32),
)


PLANES = (4, 3, 5, 2, 6, 1, 7, 0)
FAR, NEAR = (0, 80, 144), (144, 256, 384)


class Refs:
    pass


def dot(a, b, ca=1, cb=0, precision=None):
    return lax.dot_general(
        a, b, (((ca,), (cb,)), ((), ())), precision=precision, preferred_element_type=F32
    )


def iota(shape, dim):
    return lax.broadcasted_iota(jnp.int32, shape, dim)


def hot(cond, dtype=BF16):
    return jnp.where(cond, 1.0, 0.0).astype(dtype)


def split(x):
    high = x.astype(BF16)
    return high, (x - high.astype(F32)).astype(BF16)


def fine_dot(a, b, ca=1, cb=0):
    high, low = split(a)
    return dot(high, b, ca, cb) + dot(low, b, ca, cb)


def sigmoid(x):
    return 1.0 / (1.0 + jnp.exp(-x))


def publish(*refs):
    n = len(OUTPUTS)
    sources, targets, sems = refs[:n], refs[n : 2 * n], refs[2 * n]
    stores = [pltpu.make_async_copy(sources[i], targets[i], sems.at[i]) for i in range(n)]
    for store in stores:
        store.start()
    for store in stores:
        store.wait()


def kernel(*refs):
    r, c, local = Refs(), Refs(), Refs()
    names = list(INPUTS) + list(OUTPUTS) + list(BUFFERS)
    for name, ref in zip(names, refs):
        setattr(r, name, ref)
    at = len(names)
    for name in CHANNELS:
        setattr(c, name, (refs[at], refs[at + 1]))
        at += 2
    in_sems = refs[at]
    for i, name in enumerate(INPUTS):
        setattr(local, name[2:], in_sems.at[i])

    me, tx = lax.axis_index("sp"), lax.axis_index("tp")
    z, j = me // 8, me % 8
    partner = j + 1 - 2 * (j % 2)
    right, left, opp = (tx + 1) % 4, (tx + 3) % 4, (tx + 2) % 4
    column = pl.multiple_of(tx * 512, 512)
    planes = [(z + d) % 8 for d in PLANES]

    barrier = pltpu.get_barrier_semaphore()

    @pl.loop(0, 63)
    def _(n):
        away = (n // 2 + 1) * (1 - 2 * (n % 2))
        peer = (me + 32 + away * (1 - n // 62)) % 64
        pl.semaphore_signal(barrier, inc=1, device_id=(peer, tx), device_id_type=MESH)

    for side in (right, left, opp):
        pl.semaphore_signal(barrier, inc=1, device_id=(me, side), device_id_type=MESH)

    loads = dict(
        routes=(r.h_routes, r.routes),
        route_weights=(r.h_route_weights, r.route_weights),
        cot=(r.h_cot.at[:, pl.ds(column, 512)], r.cot),
        log_decay=(r.h_log_decay, r.log_decay),
        k=(r.h_k, r.k),
        v=(r.h_v, r.v),
        out_weight=(r.h_out_weight, r.weight.at[z, j]),
        q=(r.h_q, r.q),
        w_gate=(r.h_w_gate, r.w_gate),
        w_up=(r.h_w_up, r.w_up),
        w_down=(r.h_w_down, r.w_down),
        gate=(r.h_gate, r.gate),
    )
    for name, (source, target) in loads.items():
        pltpu.make_async_copy(source, target, getattr(local, name)).start()

    for n in range(8):
        source = r.h_rows.at[pl.ds(pl.multiple_of(planes[n] * 48, 16), 48)]
        pltpu.make_async_copy(source, r.full.at[tx, pl.ds(n * 48, 48)], local.rows).start()

    def loaded(target, sem):
        pltpu.make_async_copy(target, target, sem).wait()

    def send(src, dst, channel, n, sp, tp):
        out_sem, in_sem = channel
        pltpu.make_async_remote_copy(
            src_ref=src,
            dst_ref=dst,
            send_sem=out_sem.at[n],
            recv_sem=in_sem.at[n],
            device_id=(sp, tp),
            device_id_type=MESH,
        ).start()

    def got(ref, channel, n=0):
        pltpu.make_async_copy(ref, ref, channel[1].at[n]).wait()

    def sent(ref, channel, n=0):
        pltpu.make_async_copy(ref, ref, channel[0].at[n]).wait()

    class Ring:
        def __init__(self, piece, channel, members, targets):
            self.piece, self.channel = piece, channel
            self.mine, self.right, self.left, self.opp = members
            self.to_right, self.to_left = targets

        def go(self, n, h, sem, target):
            part = self.piece(n, h)
            send(part, part, self.channel, sem, *target)

        def start(self):
            self.first()
            self.second()

        def first(self):
            self.go(self.mine, 0, 0, self.to_right)
            self.go(self.mine, 1, 2, self.to_left)

        def second(self):
            self.go(self.mine, 1, 1, self.to_right)
            self.go(self.mine, 0, 3, self.to_left)

        def step(self):
            got(self.piece(self.left, 0), self.channel, 0)
            self.go(self.left, 0, 4, self.to_right)
            got(self.piece(self.right, 1), self.channel, 2)
            self.go(self.right, 1, 5, self.to_left)

        def near(self):
            got(self.piece(self.left, 1), self.channel, 1)
            got(self.piece(self.right, 0), self.channel, 3)

        def far(self):
            got(self.piece(self.opp, 0), self.channel, 4)
            got(self.piece(self.opp, 1), self.channel, 5)

        def sent(self):
            for sem, n, h in ((0, self.mine, 0), (1, self.mine, 1), (2, self.mine, 1), (3, self.mine, 0)):
                sent(self.piece(n, h), self.channel, sem)
            sent(self.piece(self.left, 0), self.channel, 4)
            sent(self.piece(self.right, 1), self.channel, 5)

    def tp_ring(buf, channel, group=None):
        start, middle, end = group or (0, buf.shape[1] // 2, buf.shape[1])
        parts = (pl.ds(start, middle - start), pl.ds(middle, end - middle))
        piece = lambda n, h: buf.at[n, parts[h]]
        return Ring(piece, channel, (tx, right, left, opp), ((me, right), (me, left)))

    class Direct:
        def __init__(self, buf, channel):
            self.buf, self.channel = buf, channel

        def start(self):
            for n, side in enumerate((right, left, opp)):
                send(self.buf.at[tx], self.buf.at[tx], self.channel, n, me, side)

        def near(self):
            got(self.buf.at[left], self.channel, 0)
            got(self.buf.at[right], self.channel, 1)

        def far(self):
            got(self.buf.at[opp], self.channel, 2)

        def sent(self):
            for n in range(3):
                sent(self.buf.at[tx], self.channel, n)

    def y_ring(piece, channel):
        members = (j, (j + 2) % 8, (j + 6) % 8, (j + 4) % 8)
        return Ring(piece, channel, members, ((z * 8 + members[1], tx), (z * 8 + members[2], tx)))

    rows_ring = tp_ring(r.full, c.rows)
    far_ring = tp_ring(r.arr, c.arrived, FAR)
    near_ring = tp_ring(r.arr, c.arrived_near, NEAR)
    residual_ring = Direct(r.resid, c.residual)
    columns_ring = Direct(r.res_in, c.columns)

    weight_ring = y_ring(lambda n, h: r.weight.at[pl.ds(4 * h, 4), n], c.weight_y)
    mixed_ring = y_ring(lambda n, h: r.mixed.at[n, pl.ds(64 * h, 64)], c.mixed_y)

    def share(ring, channel, *members):
        for n in members:
            for h in range(2):
                part = ring.piece(n, h)
                send(part, part, channel, 0, z * 8 + partner, tx)

    def to_plane_members(out, into, channel, n, first):
        own = PLANES[n] == 0

        @pl.loop(1 if own else 0, 8)
        def _(d):
            peer = (j + d) % 8
            send(out.at[first + peer], into.at[me], channel, 0, planes[n] * 8 + peer, tx)

        if own:
            into[me] = out[first + j]

    def to_group(out, into, channel):
        @pl.loop(1, 8)
        def _(d):
            peer = (j + d) % 8
            send(out.at[peer], into.at[j], channel, 0, z * 8 + peer, tx)

        into[j] = out[j]

    def across_planes(out, into, channel):
        @pl.loop(1, 8)
        def _(d):
            plane = (z + d) % 8
            send(out.at[plane], into.at[z], channel, 0, plane * 8 + j, tx)

        into[z] = out[z]

    def to_planes(src, into, channel):
        @pl.loop(1, 8)
        def _(d):
            send(src, into.at[z], channel, 0, ((z + d) % 8) * 8 + j, tx)

    eye = hot(iota((128, 128), 0) == iota((128, 128), 1), F32)
    loaded(r.routes, local.routes)
    loaded(r.route_weights, local.route_weights)
    routes = dot(eye, r.routes[...].astype(F32), 1, 1, precision=HIGHEST)
    route_weights = dot(eye, r.route_weights[...], 1, 1, precision=HIGHEST)
    expert = iota((128, 64), 1).astype(F32)
    route = [routes[:, 0:1], routes[:, 1:2]]
    named = [hot(route[n] == expert, F32) for n in range(2)]
    strict = iota((128, 128), 0) > iota((128, 128), 1)
    earlier = dot(hot(strict), (named[0] + named[1]).astype(BF16))
    slot = iota((128, 512), 1).astype(F32)
    loaded(r.cot, local.cot)
    cot = r.cot[...].astype(F32)
    scaled = []
    for n in range(2):
        rank = jnp.sum(named[n] * earlier, axis=1, keepdims=True)
        upper = jnp.where(rank >= 3.0, 1.0, 0.0)
        base = route[n] * 8.0
        r.hit_a[n] = hot(slot == base + rank)
        for m in range(3):
            place = jnp.where(rank - 3.0 * upper == float(m), base + 6.0 + upper, -1.0)
            r.hit_b[n, m] = hot(slot == place)
        scaled.append((route_weights[:, n : n + 1] * cot).astype(BF16))
    for m in range(3):
        lanes = slice(m * 128, (m + 1) * 128)
        total = dot(r.hit_a[0], scaled[0][:, lanes], 0, 0)
        total = total + dot(r.hit_a[1], scaled[1][:, lanes], 0, 0)
        total = total + dot(r.hit_b[0, m], scaled[0][:, 384:512], 0, 0)
        total = total + dot(r.hit_b[1, m], scaled[1][:, 384:512], 0, 0)
        r.pack_out[:, :, lanes] = total.reshape(64, 8, 128).astype(BF16)
    row, col = iota((128, 128), 0), iota((128, 128), 1)
    tri = hot(row >= col, F32)
    head_of = iota((16, 1024), 1) // 64 == iota((16, 1024), 0)
    loaded(r.log_decay, local.log_decay)
    loaded(r.v, local.v)
    loaded(r.k, local.k)
    log_decay = r.log_decay[...]
    cumulative = dot(tri, log_decay, 1, 1, precision=HIGHEST)
    r.c_col[...] = dot(cumulative, hot(iota((16, 128), 0) == iota((16, 128), 1), F32), precision=HIGHEST)
    r.c_row[...] = dot(log_decay, tri, 1, 1, precision=HIGHEST)
    r.c_exp[...] = dot(cumulative, hot(head_of, F32), precision=HIGHEST)
    c_exp = r.c_exp[...]
    r.from_start[...] = jnp.exp(c_exp)
    r.to_end[...] = jnp.exp(r.c_exp[127:128, :] - c_exp)
    r.v_end[0], r.v_end[1] = split(r.v[...].astype(F32) * r.to_end[...])
    for g in range(2):
        wide, k = slice(g * 512, (g + 1) * 512), r.k[:, g * 128 : (g + 1) * 128]
        own = dot(r.v_end[0, :, wide], k, 0, 0) + dot(r.v_end[1, :, wide], k, 0, 0)
        r.f_own[g * 4 : (g + 1) * 4] = own.reshape(4, 128, 128)
    total = dot(log_decay, jnp.ones((128, 128), F32), precision=HIGHEST)
    spread = hot(iota((64, 16), 0) // 4 == iota((64, 16), 1), F32)
    r.log_out[...] = dot(spread, total, precision=HIGHEST).reshape(8, 8, 128)
    place, packed = iota((384, 512), 0), iota((384, 512), 1)
    source, rank = place // 6, place % 6
    r.sel_a[...] = hot(packed == source * 8 + rank)
    for m in range(3):
        r.sel_b[m] = hot((packed == source * 8 + 6 + rank // 3) & (rank % 3 == m))

    lower = row >= col
    first = col < 64
    loaded(r.q, local.q)
    for g in range(2):
        r.qk[g] = dot(r.q[:, g * 128 : (g + 1) * 128], r.k[:, g * 128 : (g + 1) * 128], 1, 1)

    def masked_values(p):
        vp = r.v[:, pl.ds(pl.multiple_of(p * 128, 128), 128)].astype(F32)
        return jnp.concatenate(
            [jnp.where(first, vp, 0.0).astype(BF16), jnp.where(first, 0.0, vp).astype(BF16)], axis=0
        )

    @pl.loop(0, 8)
    def _(p):
        off = pl.multiple_of(p * 128, 128)
        qk = r.qk[p // 4]
        c_pair = r.c_exp[:, pl.ds(off, 128)]
        for n in range(2):
            down = jnp.minimum(c_pair[:, 64 * n : 64 * n + 1] - r.c_row[pl.ds(2 * p + n, 1), :], 0.0)
            decay = jnp.where(lower, jnp.exp(down), 0.0)
            r.decay[p, :, n * 128 : (n + 1) * 128] = decay
            lanes = slice(n * 128, (n + 1) * 128)
            r.score[0, p, :, lanes], r.score[1, p, :, lanes] = split(qk * decay)
        values = masked_values(p)
        r.y[:, pl.ds(off, 128)] = dot(r.score[0, p], values) + dot(r.score[1, p], values)

    pl.semaphore_wait(barrier, 66)
    for n in range(8):
        channel = c.dispatch if n < 3 else c.dispatch_near
        to_plane_members(r.pack_out, r.pack_in, channel, n, planes[n] * 8)
    loaded(r.full.at[tx], local.rows)
    rows_ring.start()
    to_group(r.f_own, r.f_in, c.f_j)
    to_group(r.log_out, r.log_in, c.f_jlog)
    rows_ring.step()
    loaded(r.weight.at[z, j], local.out_weight)
    to_planes(r.weight.at[z, j], r.weight.at[:, j], c.weight_z)

    def factor(log):
        e = jnp.exp(log)
        return jnp.concatenate(
            [jnp.broadcast_to(e[0:1], (64, 128)), jnp.broadcast_to(e[4:5], (64, 128))], axis=0
        )

    def carry_group(states, run_ref, reverse):
        run, log = jnp.zeros((128, 128), F32), jnp.zeros((8, 128), F32)
        for i in reversed(range(8)) if reverse else range(8):
            r.before[i] = run
            r.log_before[i] = log
            run = factor(r.log_in[i]) * run + states[i].astype(F32)
            log = log + r.log_in[i]
        run_ref[...] = run.reshape(run_ref.shape)
        return log

    def scan_planes(planes_in, scan):
        run = jnp.zeros((16, 128), F32)
        for i in reversed(range(8)):
            scan[i] = run
            run = jnp.exp(r.log_z[i, pl.ds(4 * (z // 4), 1), :]) * run + planes_in[i]

    def carry_planes(planes, back):
        run = jnp.zeros((128, 128), F32)
        for i in range(8):
            run = jnp.where(i < z, factor(r.log_z[i]) * run + planes[i], run)
        back_to_group(run, back)

    def back_to_group(run, back):
        for i in range(8):
            back[i] = (r.before[i] + factor(r.log_before[i]) * run).astype(back.dtype)

    def unpack(group, lanes, first, last):
        start, _, end = group
        for n in range(first // 8, last // 8):
            r.pack_sorted[n * 8 : (n + 1) * 8] = r.pack_in[pl.ds(planes[n] * 8, 8)]
        packed = r.pack_sorted[lanes.start // 8 : lanes.stop // 8].reshape(lanes.stop - lanes.start, 384)
        r.arr[tx, start:end, 0:384] = dot(r.sel_a[start:end, lanes], packed).astype(BF16)
        tail = dot(r.sel_b[0, start:end, lanes], packed[:, 0:128])
        tail = tail + dot(r.sel_b[1, start:end, lanes], packed[:, 128:256])
        tail = tail + dot(r.sel_b[2, start:end, lanes], packed[:, 256:384])
        r.arr[tx, start:end, 384:512] = tail.astype(BF16)

    r.pack_sorted[24:32] = jnp.zeros((8, 8, 384), BF16)
    got(r.pack_in.at[pl.ds(0, 24)], c.dispatch)
    unpack(FAR, slice(0, 256), 0, 24)
    far_ring.start()
    got(r.pack_in.at[pl.ds(0, 39)], c.dispatch_near)
    unpack(NEAR, slice(128, 512), 24, 64)
    far_ring.step()
    near_ring.start()

    got(r.f_in.at[pl.ds(0, 7)], c.f_j)
    got(r.log_in.at[pl.ds(0, 7)], c.f_jlog)
    r.log_run[...] = carry_group(r.f_in, r.f_run, False)
    r.log_z[z] = r.log_run[...]
    r.f_z[z] = r.f_run[...]
    to_planes(r.f_run, r.f_z, c.f_z)
    to_planes(r.log_run, r.log_z, c.f_zlog)


    rows_ring.near()
    rows_ring.far()
    loaded(r.w_gate, local.w_gate)
    loaded(r.w_up, local.w_up)
    loaded(r.w_down, local.w_down)
    gate_pre, up_pre = jnp.zeros((384, 256), F32), jnp.zeros((384, 256), F32)
    for t in range(4):
        gate_pre = gate_pre + dot(r.full[t], r.w_gate[t * 512 : (t + 1) * 512, :])
    r.gate_pre[...] = gate_pre
    for t in range(4):
        up_pre = up_pre + dot(r.full[t], r.w_up[t * 512 : (t + 1) * 512, :])
    r.up_pre[...] = up_pre
    gate_pre = r.gate_pre[...]
    r.hidden[...] = (gate_pre * sigmoid(gate_pre) * up_pre).astype(BF16)

    def hidden_part(t, group):
        lanes = pl.ds(pl.multiple_of(t * 512, 512), 512)
        return dot(r.arr[t, group[0] : group[2]], r.w_down[:, lanes], 1, 1)

    def hidden_grads(group):
        start, _, end = group
        hidden_grad = r.hidden_grad[start:end] + hidden_part(opp, group)
        gate_pre = r.gate_pre[start:end]
        gate_sig = sigmoid(gate_pre)
        slope = gate_sig * (1.0 + gate_pre * (1.0 - gate_sig))
        r.gate_grad[start:end] = (hidden_grad * r.up_pre[start:end] * slope).astype(BF16)
        r.up_grad[start:end] = (hidden_grad * (gate_pre * gate_sig)).astype(BF16)

    def row_part(t, start, end):
        rows = pl.ds(pl.multiple_of(t * 512, 512), 512)
        part = dot(r.gate_grad[start:end], r.w_gate[rows, :], 1, 1)
        return part + dot(r.up_grad[start:end], r.w_up[rows, :], 1, 1)

    def half_send(source, target, channel, n, start, end, side):
        part = pl.ds(start, end - start)
        send(source.at[part], target.at[part], channel, n, me, side)

    def scatter_parts(group):
        start, _, end = group
        r.rs_opp[start:end] = row_part(opp, start, end).astype(BF16)
        r.rs_own_r[start:end] = row_part(right, start, end)
        r.rs_own_l[start:end] = row_part(left, start, end)

    def scatter_start(group, channel):
        start, middle, end = group
        half_send(r.rs_opp, r.rs_half_l, channel, 0, start, middle, right)
        half_send(r.rs_opp, r.rs_half_r, channel, 1, middle, end, left)
        r.rs_right[middle:end] = r.rs_own_r[middle:end].astype(BF16)
        half_send(r.rs_right, r.rs_in_l, channel, 2, middle, end, right)
        r.rs_left[start:middle] = r.rs_own_l[start:middle].astype(BF16)
        half_send(r.rs_left, r.rs_in_r, channel, 3, start, middle, left)

    def scatter_step(group, channel):
        start, middle, end = group
        got(r.rs_half_l.at[pl.ds(start, middle - start)], channel, 0)
        total = r.rs_own_r[start:middle] + r.rs_half_l[start:middle].astype(F32)
        r.rs_right[start:middle] = total.astype(BF16)
        half_send(r.rs_right, r.rs_in_l, channel, 4, start, middle, right)
        got(r.rs_half_r.at[pl.ds(middle, end - middle)], channel, 1)
        total = r.rs_own_l[middle:end] + r.rs_half_r[middle:end].astype(F32)
        r.rs_left[middle:end] = total.astype(BF16)
        half_send(r.rs_left, r.rs_in_r, channel, 5, middle, end, left)

    def scatter_end(group, channel):
        start, middle, end = group
        top, bottom = pl.ds(start, middle - start), pl.ds(middle, end - middle)
        got(r.rs_in_l.at[bottom], channel, 2)
        got(r.rs_in_r.at[top], channel, 3)
        got(r.rs_in_l.at[top], channel, 4)
        got(r.rs_in_r.at[bottom], channel, 5)
        total = r.rs_own[start:end] + r.rs_in_l[start:end].astype(F32)
        return (total + r.rs_in_r[start:end].astype(F32)).astype(BF16)

    def scatter_sent(group, channel):
        start, middle, end = group
        top, bottom = pl.ds(start, middle - start), pl.ds(middle, end - middle)
        for n, part in enumerate((top, bottom, bottom, top, top, bottom)):
            sent(r.rs_half_l.at[part], channel, n)

    def pack_rows(summed, group, lanes, first, last):
        start, _, end = group
        skip = first * 8 - lanes.start
        for m in range(3):
            part = slice(m * 128, (m + 1) * 128)
            total = dot(r.sel_a[start:end, lanes], summed[:, part], 0, 0)
            total = total + dot(r.sel_b[m, start:end, lanes], summed[:, 384:512], 0, 0)
            total = total[skip : skip + (last - first) * 8].reshape(last - first, 8, 128)
            r.ret_out[first:last, :, part] = total.astype(BF16)

    r.hidden_grad[0:144] = hidden_part(tx, FAR)
    far_ring.near()
    r.hidden_grad[0:144] += hidden_part(left, FAR)
    r.hidden_grad[0:144] += hidden_part(right, FAR)
    far_ring.far()
    hidden_grads(FAR)
    scatter_parts(FAR)
    scatter_start(FAR, c.scatter)
    near_ring.step()
    r.hidden_grad[144:384] = hidden_part(tx, NEAR)
    scatter_step(FAR, c.scatter)

    got(r.weight.at[pl.ds(0, 7), 0], c.weight_z)
    weight_ring.first()
    share(weight_ring, c.weight_c, j)
    weight_ring.second()

    near_ring.near()
    r.hidden_grad[144:384] += hidden_part(left, NEAR)
    r.hidden_grad[144:384] += hidden_part(right, NEAR)
    near_ring.far()
    hidden_grads(NEAR)
    scatter_parts(NEAR)
    scatter_start(NEAR, c.scatter_near)
    r.rs_own[...] = row_part(tx, 0, 384)
    summed = scatter_end(FAR, c.scatter)
    pack_rows(summed, FAR, slice(0, 256), 0, 24)
    for n in range(3):
        to_plane_members(r.ret_out, r.ret_in, c.back, n, n * 8)

    got(r.f_z.at[pl.ds(0, 7)], c.f_z)
    got(r.log_z.at[pl.ds(0, 7)], c.f_zlog)
    carry_planes(r.f_z, r.f_back)
    to_group(r.f_back, r.state, c.f_back)
    scatter_step(NEAR, c.scatter_near)

    @pl.loop(0, 4)
    def _(t):
        rows = pl.ds(pl.multiple_of(t * 512, 512), 512)
        r.g_gate[rows, :] = dot(r.full[t], r.gate_grad[...], 0, 0).astype(BF16)
        r.g_up[rows, :] = dot(r.full[t], r.up_grad[...], 0, 0).astype(BF16)
        r.g_down[:, rows] = dot(r.hidden[...], r.arr[t], 0, 0).astype(BF16)


    summed = scatter_end(NEAR, c.scatter_near)
    pack_rows(summed, NEAR, slice(128, 512), 24, 64)
    for n in range(3, 8):
        to_plane_members(r.ret_out, r.ret_in, c.back, n, n * 8)
    weight_ring.step()
    weight_ring.near()
    share(weight_ring, c.weight_c, weight_ring.left, weight_ring.right)

    got(r.state.at[pl.ds(0, 7)], c.f_back)
    for g in range(2):
        lanes = slice(g * 512, (g + 1) * 512)
        state = r.state[g * 4 : (g + 1) * 4].reshape(512, 128)
        r.carried[:, lanes] = dot(r.q[:, g * 128 : (g + 1) * 128], state, 1, 1) * r.from_start[:, lanes]
    y = r.y[...] + r.carried[...]
    r.y[...] = y
    loaded(r.gate, local.gate)
    gate = r.gate[...].astype(F32)
    r.mixed[j] = (y * (gate * sigmoid(gate))).astype(BF16)
    got(r.ret_in.at[pl.ds(0, 63)], c.back)
    packed_back = r.ret_in[...].reshape(512, 384)
    picked = dot(r.hit_a[0] + r.hit_a[1], packed_back)
    tail = dot(r.hit_b[0, 0] + r.hit_b[1, 0], packed_back[:, 0:128])
    tail = tail + dot(r.hit_b[0, 1] + r.hit_b[1, 1], packed_back[:, 128:256])
    tail = tail + dot(r.hit_b[0, 2] + r.hit_b[1, 2], packed_back[:, 256:384])
    picked = jnp.concatenate([picked, tail], axis=1)
    residual = r.cot[...].astype(F32) + picked
    r.resid[tx] = residual.astype(BF16)
    residual_ring.start()

    r.res_t[...] = dot(r.resid[tx], eye.astype(BF16), 0, 0).reshape(2, 8, 32, 128).astype(BF16)

    @pl.loop(1, 8)
    def _(d):
        peer = (j + d) % 8
        send(r.res_t.at[:, peer], r.res_in.at[tx, j], c.gow_j, 0, z * 8 + peer, tx)

    r.res_in[tx, j] = r.res_t[:, j]
    r.g_res[...] = residual

    mixed_ring.start()
    share(mixed_ring, c.mixed_c, j)

    weight_ring.far()
    share(weight_ring, c.weight_c, weight_ring.opp)

    got(r.weight.at[:, pl.ds(0, 4)], c.weight_c)

    def mixed_grad_part(t, lanes):
        w = r.weight[pl.ds(2 * t, 2), :, :, lanes].reshape(512, 256)
        return dot(r.resid[t], w)

    residual_ring.near()
    for n in range(4):
        lanes = slice(n * 256, (n + 1) * 256)
        grad = mixed_grad_part(tx, lanes) + mixed_grad_part(left, lanes)
        r.mixed_grad[:, lanes] = grad + mixed_grad_part(right, lanes)
    got(r.res_in.at[tx, pl.ds(0, 7)], c.gow_j)
    columns_ring.start()
    mixed_ring.step()
    residual_ring.far()

    for n in range(4):
        lanes = slice(n * 256, (n + 1) * 256)
        grad = r.mixed_grad[:, lanes] + mixed_grad_part(opp, lanes)
        gate = r.gate[:, lanes].astype(F32)
        sig = sigmoid(gate)
        r.g_gate_in[:, lanes] = grad * r.y[:, lanes] * (sig * (1.0 + gate * (1.0 - sig)))
        dy = grad * (gate * sig)
        r.dy[:, lanes] = dy
        high, low = split(dy * r.from_start[:, lanes])
        r.dy_start[:, lanes] = high
        q = r.q[:, (n // 2) * 128 : (n // 2 + 1) * 128]
        reached = dot(high, q, 0, 0) + dot(low, q, 0, 0)
        r.b_own[2 * n : 2 * n + 2] = reached.reshape(2, 128, 128)
        for peer in (2 * n, 2 * n + 1):

            @pl.when(j != peer)
            def _():
                send(r.b_own.at[peer], r.b_in.at[j], c.b_j, 0, z * 8 + peer, tx)


    r.b_in[j] = r.b_own[j]

    got(r.b_in.at[pl.ds(0, 7)], c.b_j)
    carry_group(r.b_in, r.b_run, True)
    across_planes(r.b_run, r.b_z, c.b_z)
    to_group(r.before, r.b_group, c.b_group)
    to_group(r.log_before, r.b_log, c.b_log)
    mixed_ring.near()
    mixed_ring.far()
    share(mixed_ring, c.mixed_c, mixed_ring.left, mixed_ring.right, mixed_ring.opp)

    columns_ring.near()
    columns_ring.far()
    got(r.mixed.at[pl.ds(0, 4)], c.mixed_c)

    @pl.loop(0, 4)
    def _(n):
        lanes = pl.ds(pl.multiple_of(n * 256, 256), 256)
        part = jnp.zeros((256, 256), F32)
        for i in range(8):
            part = part + dot(r.res_in[:, i].reshape(256, 128), r.mixed[i, :, lanes])
        part = part.reshape(8, 32, 256)
        r.gow_part[:, :, lanes] = part
        r.gow_out[:, :, lanes] = part.astype(BF16)

    def gow_send(*distances):
        for d in distances:
            plane = (z + d) % 8
            send(r.gow_out.at[plane], r.gow_in.at[z], c.gow_z, 0, plane * 8 + j, tx)


    got(r.b_z.at[pl.ds(0, 7)], c.b_z)
    scan_planes(r.b_z, r.b_scan)
    across_planes(r.b_scan, r.b_pre, c.b_pre)
    gow_send(3, 5, 4, 2, 6, 1, 7)

    got(r.b_pre.at[pl.ds(0, 7)], c.b_pre)
    r.b_plane[...] = r.b_pre[...].reshape(128, 128).astype(BF16)

    @pl.loop(1, 8)
    def _(d):
        send(r.b_plane, r.b_planes.at[j], c.b_back, 0, z * 8 + (j + d) % 8, tx)

    r.b_planes[j] = r.b_plane[...]

    r.row_col[...] = jnp.zeros((128, 128), F32)
    r.dqk[...] = jnp.zeros((2, 128, 128), F32)

    @pl.loop(0, 8)
    def _(p):
        off = pl.multiple_of(p * 128, 128)
        g = p // 4
        qk = r.qk[g]
        dy = r.dy[:, pl.ds(off, 128)]
        part = dot(dy.astype(BF16), masked_values(p), 1, 1) * r.decay[p]
        r.dqk[g] += part[:, 0:128] + part[:, 128:256]
        total = r.row_col[...]
        dv = jnp.zeros((128, 128), F32)
        for n in range(2):
            lanes = slice(n * 128, (n + 1) * 128)
            weighed = (part[:, lanes] * qk).astype(BF16)
            head = hot(col == 2 * p + n)
            total = total + dot(weighed, head) - dot(weighed, head, 0, 0)
            own = jnp.where(first, dy, 0.0) if n == 0 else jnp.where(first, 0.0, dy)
            dv = dv + dot(r.score[0, p, :, lanes], own.astype(BF16), 0, 0)
        r.row_col[...] = total
        r.dv[:, pl.ds(off, 128)] = dv

    by_head = hot(iota((1024, 128), 0) // 64 == iota((1024, 128), 1))
    r.row_col[...] += fine_dot(r.dy[...] * r.carried[...], by_head)
    for g in range(2):
        state = r.state[g * 4 : (g + 1) * 4].reshape(512, 128)
        r.dq[:, g * 128 : (g + 1) * 128] = dot(r.dy_start[:, g * 512 : (g + 1) * 512], state)

    for g in range(2):
        lanes = slice(g * 128, (g + 1) * 128)
        r.g_q[:, lanes] = r.dq[:, lanes] + dot(r.dqk[g].astype(BF16), r.k[:, lanes])


    got(r.b_group.at[pl.ds(0, 7)], c.b_group)
    got(r.b_log.at[pl.ds(0, 7)], c.b_log)
    for i in range(8):
        r.carry[i] = factor(r.b_log[i])
    got(r.b_planes.at[pl.ds(0, 7)], c.b_back)
    for i in range(8):
        r.dstate[i] = r.b_group[i] + r.carry[i] * r.b_planes[i].astype(F32)
    for g in range(2):
        lanes, wide = slice(g * 128, (g + 1) * 128), slice(g * 512, (g + 1) * 512)
        dstate, low = split(r.dstate[g * 4 : (g + 1) * 4].reshape(512, 128))
        k = r.k[:, lanes]
        through = (dot(k, dstate, 1, 1) + dot(k, low, 1, 1)) * r.to_end[:, wide]
        r.carried[:, wide] = through
        r.g_v[:, wide] = r.dv[:, wide] + through
        r.g_k[:, lanes] = dot(r.dqk[g].astype(BF16), r.q[:, lanes], 0, 0) + dot(r.v_end[0, :, wide], dstate)
    added = fine_dot(r.v[...].astype(F32) * r.carried[...], by_head)
    high, low = split((r.dstate[...] * r.state[...].astype(F32)).reshape(1024, 128))
    both = dot(by_head, high, 0, 0) + dot(by_head, low, 0, 0)
    kept = dot(jnp.ones((128, 128), F32), both, 1, 1, precision=HIGHEST)
    kept = kept * jnp.exp(r.c_col[127:128, :])
    upper = hot(row <= col, F32)
    below = hot(row > col, F32)
    grad = dot(upper, r.row_col[...], precision=HIGHEST) + dot(below, added, precision=HIGHEST) + kept
    r.g_decay[...] = dot(eye[0:16], grad, 1, 1, precision=HIGHEST)

    got(r.gow_in.at[pl.ds(0, 7)], c.gow_z)
    total = r.gow_part[z]
    for d in range(1, 8):
        total = total + r.gow_in[(z + d) % 8].astype(F32)
    r.g_out[...] = total

    for ring in (rows_ring, far_ring, near_ring, residual_ring, columns_ring, weight_ring, mixed_ring):
        ring.sent()
    sent(r.pack_out.at[pl.ds(0, 24)], c.dispatch)
    sent(r.pack_out.at[pl.ds(0, 39)], c.dispatch_near)
    sent(r.ret_out.at[pl.ds(0, 63)], c.back)
    scatter_sent(FAR, c.scatter)
    scatter_sent(NEAR, c.scatter_near)
    sent(r.weight.at[pl.ds(0, 7), 0], c.weight_z)
    sent(r.weight.at[:, pl.ds(0, 4)], c.weight_c)
    sent(r.mixed.at[pl.ds(0, 4)], c.mixed_c)
    sent(r.res_in.at[tx, pl.ds(0, 7)], c.gow_j)
    sent(r.gow_out.at[pl.ds(0, 7)], c.gow_z)
    for channel in (c.f_j, c.f_z, c.b_j, c.b_group):
        sent(r.f_in.at[pl.ds(0, 7)], channel)
    sent(r.b_planes.at[pl.ds(0, 7)], c.b_back)
    sent(r.state.at[pl.ds(0, 7)], c.f_back)
    sent(r.b_z.at[pl.ds(0, 7)], c.b_z)
    sent(r.b_z.at[pl.ds(0, 7)], c.b_pre)
    for channel in (c.f_jlog, c.f_zlog, c.b_log):
        sent(r.log_in.at[pl.ds(0, 7)], channel)


def shards(
    out_cotangent,
    routes,
    route_weights,
    expert_rows,
    w_gate,
    w_up,
    w_down,
    out_weight,
    values,
    keys,
    queries,
    log_decay,
    gate_input,
):
    arrays = [jax.ShapeDtypeStruct(shape, dtype) for shape, dtype in OUTPUTS.values()]
    scratch = [pltpu.VMEM(shape, dtype) for shape, dtype in BUFFERS.values()]
    for n in CHANNELS.values():
        scratch += [pltpu.SemaphoreType.DMA((n,))] * 2
    scratch += [pltpu.SemaphoreType.DMA((len(INPUTS),))]
    arguments = (
        out_cotangent,
        routes.T,
        route_weights.T,
        expert_rows[0],
        w_gate[0],
        w_up[0],
        w_down[0],
        out_weight,
        values,
        keys,
        queries,
        log_decay.T,
        gate_input,
    )
    outs = pl.pallas_call(
        kernel,
        out_shape=arrays,
        in_specs=[pl.BlockSpec(memory_space=pltpu.HBM)] * len(INPUTS),
        out_specs=[pl.BlockSpec(memory_space=pltpu.VMEM)] * len(OUTPUTS),
        scratch_shapes=scratch,
        compiler_params=pltpu.CompilerParams(
            has_side_effects=True, collective_id=0, vmem_limit_bytes=50000000
        ),
        name="layer_backward",
    )(*[pltpu.with_memory_space_constraint(value, pltpu.HBM) for value in arguments])
    outs = pl.pallas_call(
        publish,
        out_shape=arrays,
        in_specs=[pl.BlockSpec(memory_space=pltpu.VMEM)] * len(OUTPUTS),
        out_specs=[pl.BlockSpec(memory_space=pltpu.HBM)] * len(OUTPUTS),
        scratch_shapes=[pltpu.SemaphoreType.DMA((len(OUTPUTS),))],
        compiler_params=pltpu.CompilerParams(vmem_limit_bytes=8_000_000),
        name="publish",
    )(*outs)
    outs = list(outs)
    outs[8] = outs[8].T
    return (outs[0][None], outs[1][None], outs[2][None]) + tuple(outs[3:])


def solution(mesh):
    sp, both = P("sp", None), P("sp", "tp")
    columns, hidden = P("sp", None, "tp"), P("sp", "tp", None)
    in_specs = (sp, sp, sp, columns, columns, columns, hidden) + (both,) * 6
    out_specs = (columns, columns, hidden) + (both,) * 7
    return jax.shard_map(
        shards, mesh=mesh, in_specs=in_specs, out_specs=out_specs, check_vma=False
    )
```
